32 devices in a mesh: fs: 4 (over y, x), tp: 8 (over z, core).
Axes of the slice: x: 2, y: 2, z: 4, core: 2. Of those that a mesh axis runs over, the one named last changes fastest.
Arguments:
- tokens: bfloat16 [4096, 2048], P(('fs', 'tp')), may hold values from -6 to 6
- up_weight: bfloat16 [2048, 4096], P('fs', 'tp'), may hold values from -0.125 to 0.125
- down_weight: bfloat16 [4096, 2048], P('tp', 'fs'), may hold values from -0.09375 to 0.09375
- cotangent: bfloat16 [4096, 2048], P(('fs', 'tp')), may hold values from -6 to 6
Outputs:
- input_grad: bfloat16 [4096, 2048], P(('fs', 'tp'))
- up_grad: float32 [2048, 4096], P('fs', 'tp')
- down_grad: float32 [4096, 2048], P('tp', 'fs')
The draws below stay inside these ranges and needn't reach their ends.
All inputs are finite; a program needn't handle non-finite values.
Results may differ from the reference program's by a relative error of at most 0.018.
Values may be sent and summed in bfloat16 or wider, within the bound.
A program may use at most 128 MiB of HBM per device.

```python
import jax
import jax.numpy as jnp
from jax import lax

D = 2048
FF = 4096
TOKENS = 4096
N_TP = 8


def spiked(entries, own_key, source, target, blocks, factor):
    owner, partner = [(jnp.arange(entries.shape[dim]) // (entries.shape[dim] // blocks)).reshape([-1 if axis == dim else 1 for axis in range(entries.ndim)]) for dim in (source, target)]
    chosen = jax.random.permutation(own_key, blocks)[partner]
    strong = (owner == chosen) | (owner == (partner + blocks // 2) % blocks)
    return jnp.where(strong, factor * entries, entries)


def levels(own_key, dims, pieces, low, high):
    loudness = 1.0
    for axis_at, parts in pieces:
        heights = jax.random.uniform(jax.random.fold_in(jax.random.fold_in(own_key, 6), axis_at), (parts,), jnp.float32, low / len(pieces), high / len(pieces))
        loudness = loudness * jnp.repeat(jnp.exp(heights), dims[axis_at] // parts).reshape((-1,) + (1,) * (len(dims) - 1 - axis_at))
    return loudness


def bell_draw(key, shape, spread, reach, split=(), kind=jnp.bfloat16):
    level = levels(key, shape, split, -0.22, 0.18) if split else 1.0
    drawn = jax.random.normal(key, shape, jnp.float32) * spread * level
    return jnp.minimum(jnp.maximum(drawn, -reach), reach).astype(kind)


def gaussian_with(rng, dims, spread, bound, pieces, heavy, held_as=jnp.bfloat16):
    values = spread * jax.random.normal(rng, dims, jnp.float32)
    if pieces:
        values = values * levels(rng, dims, pieces, -0.22, 0.18)
    return jnp.clip(spiked(values, jax.random.fold_in(rng, 3), *heavy), -bound, bound).astype(held_as)


def setup_inputs(seed: int = 0) -> dict:
    key_list = jax.random.split(jax.random.key(seed), 5)
    return {
        "tokens": bell_draw(key_list[0], (TOKENS, D), 1.0, 6.0, ((0, 32),)),
        "up_weight": bell_draw(key_list[1], (D, FF), D ** -0.5, 0.125, ((0, 4), (1, 8))),
        "down_weight": bell_draw(key_list[2], (FF, D), FF ** -0.5, 0.09375, ((0, 8), (1, 4))),
        "cotangent": gaussian_with(key_list[3], (TOKENS, D), 1.0, 6.0, ((0, 32),), (0, 1, 32, 2.75)),
    }


def reference(tokens, up_weight, down_weight, cotangent):
    pre = jnp.dot(tokens, up_weight, preferred_element_type=jnp.float32)
    active = jnp.maximum(pre, 0.0)
    hidden = (active * active).astype(jnp.bfloat16)
    dhidden = jnp.dot(cotangent, down_weight.T, preferred_element_type=jnp.float32)
    dpre = (2.0 * active * dhidden).astype(jnp.bfloat16)
    factor = 1.0 / jnp.sqrt(jnp.float32(TOKENS))
    down_grad = jnp.dot(hidden.T, cotangent, preferred_element_type=jnp.float32) * factor
    up_grad = jnp.dot(tokens.T, dpre, preferred_element_type=jnp.float32) * factor
    width = FF // N_TP

    def add_block(index, total):
        start = (index * width).astype(jnp.int32)
        cols = lax.dynamic_slice_in_dim(dpre, start, width, 1)
        right = lax.dynamic_slice_in_dim(up_weight, start, width, 1)
        part = jnp.dot(cols, right.T, preferred_element_type=jnp.float32).astype(jnp.bfloat16)
        part = lax.optimization_barrier(part)
        return total + part.astype(jnp.float32)
    total = lax.fori_loop(jnp.int32(0), jnp.int32(N_TP), add_block, jnp.zeros((TOKENS, D), jnp.float32))
    return (total.astype(jnp.bfloat16), up_grad, down_grad)
```

```python
import functools

import jax
import jax.numpy as jnp
from jax import lax
from jax.experimental import pallas as pl
from jax.experimental.pallas import tpu as pltpu
from jax.sharding import PartitionSpec as P

MESH = pl.DeviceIdType.MESH
BF16 = jnp.bfloat16
F32 = jnp.float32


def ring_index(p):
    q, b = p // 2, p % 2
    return 2 * q + b + (q % 2) * (1 - 2 * b)


def dot(a, b, ca, cb):
    return lax.dot_general(a, b, (((ca,), (cb,)), ((), ())), preferred_element_type=F32)


def kernel(
    nfs, nz, factor,
    tok_in, up_in, down_in, cot_in,
    dx_out, ug_out, dg_out,
    tok, cot, up, down, hid, dpre,
    dx_own, dx_send, dx_recv, dr_send, dr_recv,
    ug_own, dg_own, ug_send, ug_recv, dg_send, dg_recv,
    local_sem, zs, zr, ps, pr, ws, wr, gs, gr, xs, xr, rs, rr,
):
    fs, tp = lax.axis_index("fs"), lax.axis_index("tp")
    rows, width = tok_in.shape
    h = rows // 2
    block = 4 * h
    dl = up_in.shape[0]
    fl = up_in.shape[1]
    z, core = tp // 2, tp % 2
    pos = ring_index(fs)
    fwd = (fs, ((z + 1) % nz) * 2 + core)
    bwd = (fs, ((z + nz - 1) % nz) * 2 + core)
    mate = (fs, 2 * z + 1 - core)
    cw = (ring_index((pos + 1) % nfs), tp)
    ccw = (ring_index((pos + nfs - 1) % nfs), tp)

    def cols(o):
        return pl.ds(pl.multiple_of(o * dl, dl), dl)

    locals_ = [
        pltpu.make_async_copy(tok_in, tok.at[pl.ds(0, rows)], local_sem.at[0]),
        pltpu.make_async_copy(up_in, up.at[cols(fs)], local_sem.at[1]),
        pltpu.make_async_copy(down_in, down.at[:, cols(fs)], local_sem.at[2]),
        pltpu.make_async_copy(cot_in, cot.at[pl.ds(0, rows)], local_sem.at[3]),
    ]
    for c in locals_:
        c.start()
    barrier = pltpu.get_barrier_semaphore()
    peers = (fwd, bwd, mate, cw, ccw)
    for peer in peers:
        pl.semaphore_signal(barrier, inc=1, device_id=peer, device_id_type=MESH)
    pl.semaphore_wait(barrier, len(peers))
    for c in locals_:
        c.wait()

    sends = []

    def remote(src, dst, s, r, peer):
        c = pltpu.make_async_remote_copy(
            src_ref=src, dst_ref=dst, send_sem=s, recv_sem=r, device_id=peer, device_id_type=MESH
        )
        c.start()
        sends.append(c)
        return c

    bufs = (tok, cot)

    def z_send(k, a):
        out = []
        for d, peer in enumerate((fwd, bwd)):
            out.append(remote(
                bufs[a].at[pl.ds(k * block + d * h, h)],
                bufs[a].at[pl.ds((k + 1) * block + d * h, h)],
                zs.at[k, d, a], zr.at[k, d, a], peer,
            ))
        return out

    def mate_send(k, a):
        return remote(
            bufs[a].at[pl.ds(k * block, 2 * h)],
            bufs[a].at[pl.ds(k * block + 2 * h, 2 * h)],
            ps.at[k, a], pr.at[k, a], mate,
        )

    def w_send(k, half):
        a = ring_index((pos + nfs - k) % nfs)
        b = ring_index((pos + k) % nfs)
        n = dl // 2
        piece = up.at[pl.ds(pl.multiple_of(a * dl + half * n, n), n)]
        m = fl // 2
        other = down.at[pl.ds(half * m, m), cols(b)]
        return [
            remote(piece, piece, ws.at[k, half, 0], wr.at[k, half, 0], cw),
            remote(other, other, ws.at[k, half, 1], wr.at[k, half, 1], ccw),
        ]

    z_copy, w_copy, mate_copy = {}, {}, {}
    for a in range(2):
        z_copy[0, a] = z_send(0, a)
        w_copy[0, a] = w_send(0, a)
    for a in range(2):
        mate_copy[0, a] = mate_send(0, a)

    def hidden_block(s):
        here = pl.ds(s * block, block)
        active = jnp.maximum(dot(tok[here, :], up[...], 1, 0), 0.0)
        hid[here, :] = (active * active).astype(BF16)
        dh = dot(cot[here, :], down[...], 1, 1)
        dpre[here, :] = (2.0 * active * dh).astype(BF16)

    pair_copy = {}

    def dx_block(s):
        here = pl.ds(s * block, block)

        def tile(j, carry):
            c = cols(j)
            part = dot(dpre[here, :], up[c, :], 1, 1)
            dx_own[s, :, c] = part[: 2 * h]
            dx_send[s, :, c] = part[2 * h :].astype(BF16)
            return carry

        lax.fori_loop(0, nfs, tile, 0)
        pair_copy[s] = remote(dx_send.at[s], dx_recv.at[s], xs.at[s], xr.at[s], mate)

    x_copy = {}

    def x_step(r):
        s = r + 1 if r < nz - 1 else 0
        pair_copy[s].wait_recv()
        for d, peer in enumerate((fwd, bwd)):
            here = pl.ds(d * h, h)
            if r > 0:
                x_copy[r - 1, d].wait_recv()
            total = dx_own[s, here, :] + dx_recv[s, here, :].astype(F32)
            if r > 0:
                total = total + dr_recv[r - 1, here, :].astype(F32)
            if r < nz - 1:
                dr_send[r, here, :] = total.astype(BF16)
                x_copy[r, d] = remote(
                    dr_send.at[r, here], dr_recv.at[r, here], rs.at[r, d], rr.at[r, d], peer
                )
            else:
                dx_out[here, :] = total.astype(BF16)

    events = []
    for k in range(nfs - 1):
        for half in range(2):
            events.append(((2 * k + half + 1) * 1.5 / (nfs - 1), 1, k, half))
    for k in range(nz - 1):
        for a in range(2):
            events.append(((2 * k + a + 1) * 3.0 / (nz - 1), 0, k, a))
    events.sort()
    weights_left = 2 * (nfs - 1)
    ready = [0]

    def settle(s):
        for a in range(2):
            mate_copy[s, a].wait_recv()
        hidden_block(s)
        if s < nz - 1:
            dx_block(s)

    for _, kind, k, a in events:
        if kind == 1:
            for c in w_copy[k, a]:
                c.wait_recv()
            if k + 1 < nfs - 1:
                w_copy[k + 1, a] = w_send(k + 1, a)
            weights_left -= 1
        else:
            for c in z_copy[k, a]:
                c.wait_recv()
            if k + 1 < nz - 1:
                z_copy[k + 1, a] = z_send(k + 1, a)
            mate_copy[k + 1, a] = mate_send(k + 1, a)
            if a == 1:
                ready.append(k + 1)
        if weights_left == 0 and (kind, k) != (0, nz - 2):
            for s in ready:
                settle(s)
            ready = []
    for s in ready[:-1]:
        settle(s)
    x_step(0)
    settle(ready[-1])

    def up_term(r):
        o = ring_index((pos + nfs - r - 1) % nfs)
        return dot(tok[:, cols(o)], dpre[...], 0, 0)

    def down_term(r):
        o = ring_index((pos + r + 1) % nfs)
        return dot(hid[...], cot[:, cols(o)], 0, 0)

    g_copy = {}

    def g_send(r, half, which):
        n, m = dl // 2, fl // 2
        a, b = pl.ds(half * n, n), pl.ds(half * m, m)
        if which == 0:
            g_copy[r, half, 0] = remote(
                ug_send.at[r, a], ug_recv.at[r, a], gs.at[r, half, 0], gr.at[r, half, 0], cw
            )
        else:
            g_copy[r, half, 1] = remote(
                dg_send.at[r, b], dg_recv.at[r, b], gs.at[r, half, 1], gr.at[r, half, 1], ccw
            )

    def g_terms(r):
        ug_own[...] = up_term(r)
        dg_own[...] = down_term(r)

    def g_first():
        ug_send[0] = up_term(0).astype(BF16)
        for half in range(2):
            g_send(0, half, 0)
        dg_send[0] = down_term(0).astype(BF16)
        for half in range(2):
            g_send(0, half, 1)
        g_terms(1)

    def g_step(r, half):
        n, m = dl // 2, fl // 2
        a, b = pl.ds(half * n, n), pl.ds(half * m, m)
        g_copy[r - 1, half, 0].wait_recv()
        gu = ug_own[a, :] + ug_recv[r - 1, a, :].astype(F32)
        if r < nfs - 1:
            ug_send[r, a, :] = gu.astype(BF16)
            g_send(r, half, 0)
        else:
            ug_out[a, :] = gu * factor
        g_copy[r - 1, half, 1].wait_recv()
        gd = dg_own[b, :] + dg_recv[r - 1, b, :].astype(F32)
        if r < nfs - 1:
            dg_send[r, b, :] = gd.astype(BF16)
            g_send(r, half, 1)
        else:
            dg_out[b, :] = gd * factor

    g_first()
    dx_block(nz - 1)
    for r in range(1, max(nfs, nz)):
        if r < nfs:
            g_step(r, 0)
        if r < nz:
            x_step(r)
        if r < nfs:
            g_step(r, 1)
            if r < nfs - 1:
                g_terms(r + 1)
    for c in sends:
        c.wait_send()


def shards(nfs, ntp, tokens, up_weight, down_weight, cotangent):
    rows, width = tokens.shape
    dl, fl = up_weight.shape
    nz = ntp // 2
    whole = rows * ntp
    factor = 1.0 / (whole * nfs) ** 0.5
    dma = pltpu.SemaphoreType.DMA
    any_space = pl.BlockSpec(memory_space=pl.ANY)
    vmem = pl.BlockSpec(memory_space=pltpu.VMEM)
    return pl.pallas_call(
        functools.partial(kernel, nfs, nz, factor),
        out_shape=(
            jax.ShapeDtypeStruct((rows, width), BF16),
            jax.ShapeDtypeStruct((dl, fl), F32),
            jax.ShapeDtypeStruct((fl, dl), F32),
        ),
        in_specs=[any_space] * 4,
        out_specs=(vmem, vmem, vmem),
        scratch_shapes=[
            pltpu.VMEM((whole, width), BF16),
            pltpu.VMEM((whole, width), BF16),
            pltpu.VMEM((width, fl), BF16),
            pltpu.VMEM((fl, width), BF16),
            pltpu.VMEM((whole, fl), BF16),
            pltpu.VMEM((whole, fl), BF16),
            pltpu.VMEM((nz, rows, width), F32),
            pltpu.VMEM((nz, rows, width), BF16),
            pltpu.VMEM((nz, rows, width), BF16),
            pltpu.VMEM((nz - 1, rows, width), BF16),
            pltpu.VMEM((nz - 1, rows, width), BF16),
            pltpu.VMEM((dl, fl), F32),
            pltpu.VMEM((fl, dl), F32),
            pltpu.VMEM((nfs - 1, dl, fl), BF16),
            pltpu.VMEM((nfs - 1, dl, fl), BF16),
            pltpu.VMEM((nfs - 1, fl, dl), BF16),
            pltpu.VMEM((nfs - 1, fl, dl), BF16),
            dma((4,)),
            dma((nz - 1, 2, 2)), dma((nz - 1, 2, 2)),
            dma((nz, 2)), dma((nz, 2)),
            dma((nfs - 1, 2, 2)), dma((nfs - 1, 2, 2)),
            dma((nfs - 1, 2, 2)), dma((nfs - 1, 2, 2)),
            dma((nz,)), dma((nz,)),
            dma((nz - 1, 2)), dma((nz - 1, 2)),
        ],
        compiler_params=pltpu.CompilerParams(
            collective_id=0, has_side_effects=True, vmem_limit_bytes=67_000_000
        ),
    )(tokens, up_weight, down_weight, cotangent)


def grid_kernel(
    factor,
    tok_in, up_in, down_in, cot_in,
    dx_out, ug_out, dg_out,
    tok, cot, up, down, up_home, down_home, hid, dpre, ug_acc, dg_acc,
    gx_send, gx_recv, gz_send, gz_recv, gy_send, gm_send, gf_recv,
    dx_own, dxm_send, dxm_recv, dxz_send, dxz_recv, dxy_send, dxy_recv,
    local_sem, fys, fyr, fms, fmr, fzs, fzr, fxs, fxr,
    tzs, tzr, tys, tyr, tms, tmr,
    gxs, gxr, gzs, gzr, gys, gms, gfr,
    ms, mr, dzs, dzr, dys, dyr,
):
    fs, tp = lax.axis_index("fs"), lax.axis_index("tp")
    rows, width = tok_in.shape
    dl, fl = up_in.shape
    unit, hr, hd, hf = 2 * rows, rows // 2, dl // 2, fl // 2
    x, y, z, c = fs % 2, fs // 2, tp // 2, tp % 2
    p = z % 2
    first = c == p
    second = c != p
    home = c == y
    away = c != y
    over = 2 * (1 - y) + x
    mate = (fs, 2 * z + 1 - c)
    xn = (2 * y + 1 - x, tp)
    yn = (over, tp)
    zn = (fs, 2 * (z + 1 - 2 * p) + c)
    zf = (fs, 2 * ((z + 2) % 4) + c)

    def cols(o):
        return pl.ds(pl.multiple_of(o * dl, dl), dl)

    own = jnp.logical_and(home, first)
    locals_ = [
        (pltpu.make_async_copy(up_in, up.at[cols(fs)], local_sem.at[0]), own),
        (pltpu.make_async_copy(down_in, down.at[:, cols(fs)], local_sem.at[1]), own),
        (pltpu.make_async_copy(up_in, up_home, local_sem.at[2]), jnp.logical_not(own)),
        (pltpu.make_async_copy(down_in, down_home, local_sem.at[3]), jnp.logical_not(own)),
        (pltpu.make_async_copy(tok_in, tok.at[pl.ds(0, rows)], local_sem.at[4]), None),
        (pltpu.make_async_copy(cot_in, cot.at[pl.ds(0, rows)], local_sem.at[5]), None),
    ]

    def when(cond, f):
        if cond is None:
            f()
        else:
            pl.when(cond)(f)

    for cp, cond in locals_:
        when(cond, lambda cp=cp: cp.start())
    barrier = pltpu.get_barrier_semaphore()
    peers = (mate, xn, yn, (over, 2 * z + 1 - c), zn, zf)
    for peer in peers:
        pl.semaphore_signal(barrier, inc=1, device_id=peer, device_id_type=MESH)
    pl.semaphore_wait(barrier, len(peers))
    for cp, cond in locals_:
        when(cond, lambda cp=cp: cp.wait())

    sends = []

    def remote(src, dst, s, r, peer, cond=None):
        cp = pltpu.make_async_remote_copy(
            src_ref=src, dst_ref=dst, send_sem=s, recv_sem=r, device_id=peer, device_id_type=MESH
        )
        sends.append((cp, cond))
        return cp

    def piece(o, q):
        if q < 2:
            return up.at[pl.ds(pl.multiple_of(o * dl + q * hd, hd), hd)]
        return down.at[pl.ds((q - 2) * hf, hf), cols(o)]

    def home_piece(q):
        if q < 2:
            return up_home.at[pl.ds(q * hd, hd)]
        return down_home.at[pl.ds((q - 2) * hf, hf)]

    bufs = (tok, cot)

    def rows_of(j, u, shift=0):
        return bufs[j % 2].at[pl.ds(u * unit + shift + (j // 2) * hr, hr)]

    Q = range(4)
    to_half = jnp.logical_and(home, second)
    fy = [remote(home_piece(q), piece(fs, q), fys.at[q], fyr.at[q], (over, 2 * z + p), away) for q in Q]
    fm = [remote(home_piece(q), piece(fs, q), fms.at[q], fmr.at[q], mate, to_half) for q in Q]
    fz = [[remote(piece(o, q), piece(o, q), fzs.at[i, q], fzr.at[i, q], zn, first) for q in Q]
          for i, o in enumerate((fs, over))]
    fx = [[remote(piece(o, q), piece(o, q), fxs.at[i, q], fxr.at[i, q], xn) for q in Q]
          for i, o in enumerate((fs, over))]
    tz = [remote(rows_of(j, 0), rows_of(j, 1), tzs.at[j], tzr.at[j], zf) for j in Q]
    ty = [[remote(rows_of(j, u), rows_of(j, u + 2), tys.at[u, j], tyr.at[u, j], yn) for j in Q]
          for u in range(2)]
    tm = [[remote(rows_of(j, u), rows_of(j, u, rows), tms.at[u, j], tmr.at[u, j], mate) for j in Q]
          for u in range(4)]

    @pl.when(away)
    def _():
        for q in Q:
            fy[q].start()

    @pl.when(to_half)
    def _():
        for q in Q:
            fm[q].start()

    @pl.when(second)
    def _():
        for j in Q:
            tz[j].start()

    for j in Q:
        ty[0][j].start()
    for j in Q:
        tm[0][j].start()

    @pl.when(first)
    def _():
        for q in Q:
            pl.when(away)(lambda q=q: fm[q].wait_recv())
            fz[0][q].start()
            fx[0][q].start()
        for q in Q:
            fy[q].wait_recv()
            fz[1][q].start()
            fx[1][q].start()
        for j in Q:
            tz[j].start()
        for j in Q:
            ty[0][j].wait_recv()
            tm[2][j].start()
        for j in Q:
            tz[j].wait_recv()
            ty[1][j].start()
            tm[1][j].start()

    @pl.when(second)
    def _():
        for q in Q:
            fz[0][q].wait_recv()
            fx[0][q].start()
            tz[q].wait_recv()
            ty[1][q].start()
            tm[1][q].start()
        for q in Q:
            fz[1][q].wait_recv()
            fx[1][q].start()
        for j in Q:
            ty[0][j].wait_recv()
            tm[2][j].start()

    def hidden_block(u):
        here = pl.ds(u * unit, unit)
        active = jnp.maximum(dot(tok[here, :], up[...], 1, 0), 0.0)
        hid[here, :] = (active * active).astype(BF16)
        dh = dot(cot[here, :], down[...], 1, 1)
        dpre[here, :] = (2.0 * active * dh).astype(BF16)

    dxm = [remote(dxm_send.at[u], dxm_recv.at[u], ms.at[u], mr.at[u], mate) for u in range(4)]

    def dx_block(u):
        here = pl.ds(u * unit, unit)

        def tile(j, carry):
            o = cols(j)
            part = dot(dpre[here, :], up[o, :], 1, 1)
            dx_own[u, :, o] = part[:rows]
            dxm_send[u, :, o] = part[rows:].astype(BF16)
            return carry

        lax.fori_loop(0, 4, tile, 0)
        dxm[u].start()

    def relay(j):
        ty[1][j].wait_recv()
        tm[3][j].start()

    dxz = [remote(dxz_send.at[i], dxz_recv.at[i], dzs.at[i], dzr.at[i], zf) for i in range(2)]
    dxy = remote(dxy_send, dxy_recv, dys.at[0], dyr.at[0], yn)

    def dx_sum(u):
        dxm[u].wait_recv()
        return dx_own[u] + dxm_recv[u].astype(F32)

    def dx_far(i):
        dxz_send[i] = dx_sum(2 * i + 1).astype(BF16)
        dxz[i].start()

    for q in Q:
        fx[0][q].wait_recv()
        fx[1][q].wait_recv()
    for j in Q:
        tm[0][j].wait_recv()
    hidden_block(0)
    for j in Q:
        tm[2][j].wait_recv()
    hidden_block(2)
    for j in Q:
        tm[1][j].wait_recv()
    hidden_block(1)
    dx_block(1)
    relay(0)
    early = pl.ds(0, 3 * unit)
    last = pl.ds(3 * unit, unit)

    def ug_early(o, carry):
        ug_acc[cols(o), :] = dot(tok[early, cols(o)], dpre[early, :], 0, 0)
        return carry

    def dg_early(o, carry):
        dg_acc[:, cols(o)] = dot(hid[early, :], cot[early, cols(o)], 0, 0)
        return carry

    lax.fori_loop(0, 4, ug_early, 0)
    relay(1)
    dx_far(0)
    lax.fori_loop(0, 4, dg_early, 0)
    relay(2)
    relay(3)
    for j in Q:
        tm[3][j].wait_recv()
    hidden_block(3)

    def ug_val(o):
        return ug_acc[cols(o), :] + dot(tok[last, cols(o)], dpre[last, :], 0, 0)

    def dg_val(o):
        return dg_acc[:, cols(o)] + dot(hid[last, :], cot[last, cols(o)], 0, 0)

    o_xy = 2 * (1 - y) + 1 - x
    o_x = 2 * y + 1 - x
    o_y = over
    o_me = fs
    gx = [remote(gx_send.at[i], gx_recv.at[i], gxs.at[i], gxr.at[i], xn, None if i < 6 else first)
          for i in range(8)]
    gz = [[remote(gz_send.at[i, s], gz_recv.at[i, s], gzs.at[i, s], gzr.at[i, s], zn, second)
           if s == 0 or i >= 6 else None for s in range(2)] for i in range(8)]

    def put_x(i, val, start=None):
        for h in range(2):
            gx_send[i + h] = val[h * hd : (h + 1) * hd].astype(BF16)
        when(start, lambda: [gx[i + h].start() for h in range(2)] and None)

    def put_z(s, o):
        val = dg_val(o)

        @pl.when(second)
        def _():
            for h in range(2):
                gz_send[6 + h, s] = val[h * hf : (h + 1) * hf].astype(BF16)
                gz[6 + h][s].start()

        @pl.when(first)
        def _():
            dg_acc[:, cols(o)] = val

    put_x(0, ug_val(o_xy))
    put_z(0, o_xy)
    put_x(2, ug_val(o_x))
    dx_block(3)
    put_z(1, o_y)
    put_x(4, dg_val(o_x), second)
    dx_far(1)
    ug_acc[cols(o_y), :] = ug_val(o_y)

    def acc_at(i):
        h = i % 2
        if i < 4:
            o = o_y if i < 2 else o_me
            return ug_acc[pl.ds(pl.multiple_of(o * dl + h * hd, hd), hd), :]
        o = o_me if i < 6 else o_y
        return dg_acc[pl.ds(h * hf, hf), cols(o)]

    gy = [remote(gy_send.at[k], gf_recv.at[k], gys.at[k], gfr.at[k], (over, 2 * z + y), first) for k in Q]
    to_mate = jnp.logical_and(first, away)
    gm = [remote(gm_send.at[k], gf_recv.at[k], gms.at[k], gfr.at[k], mate, to_mate) for k in Q]
    outs = (ug_out, dg_out)

    def finish(i, total):
        k = 2 * (i >= 4) + i % 2
        if i in (0, 1, 6, 7):
            gy_send[k] = total.astype(BF16)
            gy[k].start()
        else:
            n = total.shape[0]

            @pl.when(home)
            def _():
                outs[k // 2][pl.ds((k % 2) * n, n), :] = total * factor

            @pl.when(away)
            def _():
                gm_send[k] = total.astype(BF16)
                gm[k].start()

    @pl.when(first)
    def _():
        for h in range(2):
            gz[6 + h][0].wait_recv()
            total = dg_acc[pl.ds(h * hf, hf), cols(o_xy)] + gz_recv[6 + h, 0].astype(F32)
            gx_send[6 + h] = total.astype(BF16)
            gx[6 + h].start()
        gx[4].start()
        gx[5].start()

    def step(i):
        gx[i].wait_recv()

        @pl.when(second)
        def _():
            gz_send[i, 0] = (acc_at(i) + gx_recv[i].astype(F32)).astype(BF16)
            gz[i][0].start()

        @pl.when(first)
        def _():
            part = acc_at(i) + gx_recv[i].astype(F32)
            gz[i][0].wait_recv()
            finish(i, part + gz_recv[i, 0].astype(F32))

    step(0)
    ug_acc[cols(o_me), :] = ug_val(o_me)
    step(1)
    dg_acc[:, cols(o_me)] = dg_val(o_me)
    dx_block(2)
    dx_block(0)
    step(2)
    dxz[1].wait_recv()
    dxy_send[...] = (dx_sum(2) + dxz_recv[1].astype(F32)).astype(BF16)
    dxy.start()
    step(3)

    @pl.when(first)
    def _():
        for h in range(2):
            i = 6 + h
            gz[i][1].wait_recv()
            gx[i].wait_recv()
            finish(i, acc_at(i) + gz_recv[i, 1].astype(F32) + gx_recv[i].astype(F32))

    step(4)
    dxz[0].wait_recv()
    near = dx_sum(0) + dxz_recv[0].astype(F32)
    dxy.wait_recv()
    dx_out[...] = (near + dxy_recv[...].astype(F32)).astype(BF16)
    step(5)

    @pl.when(jnp.logical_not(own))
    def _():
        for k in Q:
            gy[k].wait_recv()
            n = gf_recv.shape[1]
            outs[k // 2][pl.ds((k % 2) * n, n), :] = gf_recv[k].astype(F32) * factor

    for cp, cond in sends:
        when(cond, lambda cp=cp: cp.wait_send())


def grid_shards(nfs, ntp, tokens, up_weight, down_weight, cotangent):
    rows, width = tokens.shape
    dl, fl = up_weight.shape
    factor = 1.0 / (rows * ntp * nfs) ** 0.5
    mine = 8 * rows
    hd = dl // 2
    dma = pltpu.SemaphoreType.DMA
    any_space = pl.BlockSpec(memory_space=pl.ANY)
    vmem = pl.BlockSpec(memory_space=pltpu.VMEM)
    V = pltpu.VMEM
    return pl.pallas_call(
        functools.partial(grid_kernel, factor),
        out_shape=(
            jax.ShapeDtypeStruct((rows, width), BF16),
            jax.ShapeDtypeStruct((dl, fl), F32),
            jax.ShapeDtypeStruct((fl, dl), F32),
        ),
        in_specs=[any_space] * 4,
        out_specs=(vmem, vmem, vmem),
        scratch_shapes=[
            V((mine, width), BF16), V((mine, width), BF16),
            V((width, fl), BF16), V((fl, width), BF16),
            V((dl, fl), BF16), V((fl, dl), BF16),
            V((mine, fl), BF16), V((mine, fl), BF16),
            V((width, fl), F32), V((fl, width), F32),
            V((8, hd, fl), BF16), V((8, hd, fl), BF16),
            V((8, 2, hd, fl), BF16), V((8, 2, hd, fl), BF16),
            V((4, hd, fl), BF16), V((4, hd, fl), BF16), V((4, hd, fl), BF16),
            V((4, rows, width), F32), V((4, rows, width), BF16), V((4, rows, width), BF16),
            V((2, rows, width), BF16), V((2, rows, width), BF16),
            V((rows, width), BF16), V((rows, width), BF16),
            dma((6,)), dma((4,)), dma((4,)), dma((4,)), dma((4,)),
            dma((2, 4)), dma((2, 4)), dma((2, 4)), dma((2, 4)),
            dma((4,)), dma((4,)), dma((2, 4)), dma((2, 4)), dma((4, 4)), dma((4, 4)),
            dma((8,)), dma((8,)), dma((8, 2)), dma((8, 2)), dma((4,)), dma((4,)), dma((4,)),
            dma((4,)), dma((4,)), dma((2,)), dma((2,)), dma((1,)), dma((1,)),
        ],
        compiler_params=pltpu.CompilerParams(
            collective_id=0, has_side_effects=True, vmem_limit_bytes=67_000_000
        ),
    )(tokens, up_weight, down_weight, cotangent)


def solution(mesh):
    placed = (P(("fs", "tp"), None), P("fs", "tp"), P("tp", "fs"), P(("fs", "tp"), None))
    fs, tp = mesh.shape["fs"], mesh.shape["tp"]
    body = grid_shards if (fs, tp) == (4, 8) else shards
    return jax.shard_map(
        functools.partial(body, mesh.shape["fs"], mesh.shape["tp"]),
        mesh=mesh,
        in_specs=placed,
        out_specs=(P(("fs", "tp"), None), P("fs", "tp"), P("tp", "fs")),
        check_vma=False,
    )
```

```python
import functools

import jax
import jax.numpy as jnp
from jax import lax
from jax.experimental import pallas as pl
from jax.experimental.pallas import tpu as pltpu
from jax.sharding import PartitionSpec as P

MESH = pl.DeviceIdType.MESH
BF16 = jnp.bfloat16
F32 = jnp.float32


def ring_index(p):
    q, b = p // 2, p % 2
    return 2 * q + b + (q % 2) * (1 - 2 * b)


def dot(a, b, ca, cb):
    return lax.dot_general(a, b, (((ca,), (cb,)), ((), ())), preferred_element_type=F32)


def kernel(
    nfs, nz, factor,
    tok_in, up_in, down_in, cot_in,
    dx_out, ug_out, dg_out,
    tok, cot, up, down, hid, dpre,
    dx_own, dx_send, dx_recv, dr_send, dr_recv,
    ug_own, dg_own, ug_send, ug_recv, dg_send, dg_recv,
    local_sem, zs, zr, ps, pr, ws, wr, gs, gr, xs, xr, rs, rr,
):
    fs, tp = lax.axis_index("fs"), lax.axis_index("tp")
    rows, width = tok_in.shape
    h = rows // 2
    block = 4 * h
    dl = up_in.shape[0]
    fl = up_in.shape[1]
    z, core = tp // 2, tp % 2
    pos = ring_index(fs)
    fwd = (fs, ((z + 1) % nz) * 2 + core)
    bwd = (fs, ((z + nz - 1) % nz) * 2 + core)
    mate = (fs, 2 * z + 1 - core)
    cw = (ring_index((pos + 1) % nfs), tp)
    ccw = (ring_index((pos + nfs - 1) % nfs), tp)

    def cols(o):
        return pl.ds(pl.multiple_of(o * dl, dl), dl)

    locals_ = [
        pltpu.make_async_copy(tok_in, tok.at[pl.ds(0, rows)], local_sem.at[0]),
        pltpu.make_async_copy(up_in, up.at[cols(fs)], local_sem.at[1]),
        pltpu.make_async_copy(down_in, down.at[:, cols(fs)], local_sem.at[2]),
        pltpu.make_async_copy(cot_in, cot.at[pl.ds(0, rows)], local_sem.at[3]),
    ]
    for c in locals_:
        c.start()
    barrier = pltpu.get_barrier_semaphore()
    peers = (fwd, bwd, mate, cw, ccw)
    for peer in peers:
        pl.semaphore_signal(barrier, inc=1, device_id=peer, device_id_type=MESH)
    pl.semaphore_wait(barrier, len(peers))
    for c in locals_:
        c.wait()

    sends = []

    def remote(src, dst, s, r, peer):
        c = pltpu.make_async_remote_copy(
            src_ref=src, dst_ref=dst, send_sem=s, recv_sem=r, device_id=peer, device_id_type=MESH
        )
        c.start()
        sends.append(c)
        return c

    bufs = (tok, cot)

    def z_send(k, a):
        out = []
        for d, peer in enumerate((fwd, bwd)):
            out.append(remote(
                bufs[a].at[pl.ds(k * block + d * h, h)],
                bufs[a].at[pl.ds((k + 1) * block + d * h, h)],
                zs.at[k, d, a], zr.at[k, d, a], peer,
            ))
        return out

    def mate_send(k, a):
        return remote(
            bufs[a].at[pl.ds(k * block, 2 * h)],
            bufs[a].at[pl.ds(k * block + 2 * h, 2 * h)],
            ps.at[k, a], pr.at[k, a], mate,
        )

    def w_send(k, half):
        a = ring_index((pos + nfs - k) % nfs)
        b = ring_index((pos + k) % nfs)
        n = dl // 2
        piece = up.at[pl.ds(pl.multiple_of(a * dl + half * n, n), n)]
        m = fl // 2
        other = down.at[pl.ds(half * m, m), cols(b)]
        return [
            remote(piece, piece, ws.at[k, half, 0], wr.at[k, half, 0], cw),
            remote(other, other, ws.at[k, half, 1], wr.at[k, half, 1], ccw),
        ]

    z_copy, w_copy, mate_copy = {}, {}, {}
    for a in range(2):
        z_copy[0, a] = z_send(0, a)
        w_copy[0, a] = w_send(0, a)
    for a in range(2):
        mate_copy[0, a] = mate_send(0, a)

    def hidden_block(s):
        here = pl.ds(s * block, block)
        active = jnp.maximum(dot(tok[here, :], up[...], 1, 0), 0.0)
        hid[here, :] = (active * active).astype(BF16)
        dh = dot(cot[here, :], down[...], 1, 1)
        dpre[here, :] = (2.0 * active * dh).astype(BF16)

    pair_copy = {}

    def dx_block(s):
        here = pl.ds(s * block, block)

        def tile(j, carry):
            c = cols(j)
            part = dot(dpre[here, :], up[c, :], 1, 1)
            dx_own[s, :, c] = part[: 2 * h]
            dx_send[s, :, c] = part[2 * h :].astype(BF16)
            return carry

        lax.fori_loop(0, nfs, tile, 0)
        pair_copy[s] = remote(dx_send.at[s], dx_recv.at[s], xs.at[s], xr.at[s], mate)

    x_copy = {}

    def x_step(r):
        s = r + 1 if r < nz - 1 else 0
        pair_copy[s].wait_recv()
        for d, peer in enumerate((fwd, bwd)):
            here = pl.ds(d * h, h)
            if r > 0:
                x_copy[r - 1, d].wait_recv()
            total = dx_own[s, here, :] + dx_recv[s, here, :].astype(F32)
            if r > 0:
                total = total + dr_recv[r - 1, here, :].astype(F32)
            if r < nz - 1:
                dr_send[r, here, :] = total.astype(BF16)
                x_copy[r, d] = remote(
                    dr_send.at[r, here], dr_recv.at[r, here], rs.at[r, d], rr.at[r, d], peer
                )
            else:
                dx_out[here, :] = total.astype(BF16)

    events = []
    for k in range(nfs - 1):
        for half in range(2):
            events.append(((2 * k + half + 1) * 1.5 / (nfs - 1), 1, k, half))
    for k in range(nz - 1):
        for a in range(2):
            events.append(((2 * k + a + 1) * 3.0 / (nz - 1), 0, k, a))
    events.sort()
    weights_left = 2 * (nfs - 1)
    ready = [0]

    def settle(s):
        for a in range(2):
            mate_copy[s, a].wait_recv()
        hidden_block(s)
        if s < nz - 1:
            dx_block(s)

    for _, kind, k, a in events:
        if kind == 1:
            for c in w_copy[k, a]:
                c.wait_recv()
            if k + 1 < nfs - 1:
                w_copy[k + 1, a] = w_send(k + 1, a)
            weights_left -= 1
        else:
            for c in z_copy[k, a]:
                c.wait_recv()
            if k + 1 < nz - 1:
                z_copy[k + 1, a] = z_send(k + 1, a)
            mate_copy[k + 1, a] = mate_send(k + 1, a)
            if a == 1:
                ready.append(k + 1)
        if weights_left == 0 and (kind, k) != (0, nz - 2):
            for s in ready:
                settle(s)
            ready = []
    for s in ready[:-1]:
        settle(s)
    x_step(0)
    settle(ready[-1])

    def up_term(r):
        o = ring_index((pos + nfs - r - 1) % nfs)
        return dot(tok[:, cols(o)], dpre[...], 0, 0)

    def down_term(r):
        o = ring_index((pos + r + 1) % nfs)
        return dot(hid[...], cot[:, cols(o)], 0, 0)

    g_copy = {}

    def g_send(r, half, which):
        n, m = dl // 2, fl // 2
        a, b = pl.ds(half * n, n), pl.ds(half * m, m)
        if which == 0:
            g_copy[r, half, 0] = remote(
                ug_send.at[r, a], ug_recv.at[r, a], gs.at[r, half, 0], gr.at[r, half, 0], cw
            )
        else:
            g_copy[r, half, 1] = remote(
                dg_send.at[r, b], dg_recv.at[r, b], gs.at[r, half, 1], gr.at[r, half, 1], ccw
            )

    def g_terms(r):
        ug_own[...] = up_term(r)
        dg_own[...] = down_term(r)

    def g_first():
        ug_send[0] = up_term(0).astype(BF16)
        for half in range(2):
            g_send(0, half, 0)
        dg_send[0] = down_term(0).astype(BF16)
        for half in range(2):
            g_send(0, half, 1)
        g_terms(1)

    def g_step(r, half):
        n, m = dl // 2, fl // 2
        a, b = pl.ds(half * n, n), pl.ds(half * m, m)
        g_copy[r - 1, half, 0].wait_recv()
        gu = ug_own[a, :] + ug_recv[r - 1, a, :].astype(F32)
        if r < nfs - 1:
            ug_send[r, a, :] = gu.astype(BF16)
            g_send(r, half, 0)
        else:
            ug_out[a, :] = gu * factor
        g_copy[r - 1, half, 1].wait_recv()
        gd = dg_own[b, :] + dg_recv[r - 1, b, :].astype(F32)
        if r < nfs - 1:
            dg_send[r, b, :] = gd.astype(BF16)
            g_send(r, half, 1)
        else:
            dg_out[b, :] = gd * factor

    g_first()
    dx_block(nz - 1)
    for r in range(1, max(nfs, nz)):
        if r < nfs:
            g_step(r, 0)
        if r < nz:
            x_step(r)
        if r < nfs:
            g_step(r, 1)
            if r < nfs - 1:
                g_terms(r + 1)
    for c in sends:
        c.wait_send()


def shards(nfs, ntp, tokens, up_weight, down_weight, cotangent):
    rows, width = tokens.shape
    dl, fl = up_weight.shape
    nz = ntp // 2
    whole = rows * ntp
    factor = 1.0 / (whole * nfs) ** 0.5
    dma = pltpu.SemaphoreType.DMA
    any_space = pl.BlockSpec(memory_space=pl.ANY)
    vmem = pl.BlockSpec(memory_space=pltpu.VMEM)
    return pl.pallas_call(
        functools.partial(kernel, nfs, nz, factor),
        out_shape=(
            jax.ShapeDtypeStruct((rows, width), BF16),
            jax.ShapeDtypeStruct((dl, fl), F32),
            jax.ShapeDtypeStruct((fl, dl), F32),
        ),
        in_specs=[any_space] * 4,
        out_specs=(vmem, vmem, vmem),
        scratch_shapes=[
            pltpu.VMEM((whole, width), BF16),
            pltpu.VMEM((whole, width), BF16),
            pltpu.VMEM((width, fl), BF16),
            pltpu.VMEM((fl, width), BF16),
            pltpu.VMEM((whole, fl), BF16),
            pltpu.VMEM((whole, fl), BF16),
            pltpu.VMEM((nz, rows, width), F32),
            pltpu.VMEM((nz, rows, width), BF16),
            pltpu.VMEM((nz, rows, width), BF16),
            pltpu.VMEM((nz - 1, rows, width), BF16),
            pltpu.VMEM((nz - 1, rows, width), BF16),
            pltpu.VMEM((dl, fl), F32),
            pltpu.VMEM((fl, dl), F32),
            pltpu.VMEM((nfs - 1, dl, fl), BF16),
            pltpu.VMEM((nfs - 1, dl, fl), BF16),
            pltpu.VMEM((nfs - 1, fl, dl), BF16),
            pltpu.VMEM((nfs - 1, fl, dl), BF16),
            dma((4,)),
            dma((nz - 1, 2, 2)), dma((nz - 1, 2, 2)),
            dma((nz, 2)), dma((nz, 2)),
            dma((nfs - 1, 2, 2)), dma((nfs - 1, 2, 2)),
            dma((nfs - 1, 2, 2)), dma((nfs - 1, 2, 2)),
            dma((nz,)), dma((nz,)),
            dma((nz - 1, 2)), dma((nz - 1, 2)),
        ],
        compiler_params=pltpu.CompilerParams(
            collective_id=0, has_side_effects=True, vmem_limit_bytes=67_000_000
        ),
    )(tokens, up_weight, down_weight, cotangent)


def line_kernel(
    factor, give,
    tok_in, up_in, down_in, cot_in,
    dx_out, ug_out, dg_out,
    tok, cot, up, down, up_give, down_give, hid, dpre, ug_acc, dg_acc,
    ug_send, ug_recv, dg_send, dg_recv, ug_back, dg_back, ug_home, dg_home,
    dx_own, dxm_send, dxm_recv, dxz_send, dxz_recv,
    local_sem, exs, exr, wxs, wxr, wys, wyr, ts, tr, tms, tmr,
    ms, mr, dzs, dzr, gs, gr, bs, br,
):
    fs, tp = lax.axis_index("fs"), lax.axis_index("tp")
    rows, width = tok_in.shape
    dl, fl = up_in.shape
    unit, hr, hd = 2 * rows, rows // 2, dl // 2
    x, y, z, c = fs % 2, fs // 2, tp // 2, tp % 2
    high = z // 2
    toward = 1 - 2 * high
    at_end = z % 3 == 0
    fx_, fy_, fd_ = 2 * y + 1 - x, 2 * (1 - y) + x, 2 * (1 - y) + 1 - x
    mate = (fs, 2 * z + 1 - c)
    xn, yn = (fx_, tp), (fy_, tp)
    inner = (fs, 2 * (z + toward) + c)
    outer = (fs, 2 * jnp.maximum(z - toward, 0) + c)
    across = (fs, 2 * (3 - z) + c)
    Q = range(4)

    def cols(o):
        return pl.ds(pl.multiple_of(o * dl, dl), dl)

    bufs = (tok, cot)

    def body(end):
        nf = fl - give if end else fl + give
        hf = nf // 2
        nown = fl - give if end else fl
        units = slice(0, nf)
        locals_ = [
            pltpu.make_async_copy(up_in.at[:, pl.ds(0, nown)], up.at[cols(fs), pl.ds(0, nown)], local_sem.at[0]),
            pltpu.make_async_copy(down_in.at[pl.ds(0, nown)], down.at[pl.ds(0, nown), cols(fs)], local_sem.at[1]),
            pltpu.make_async_copy(tok_in, tok.at[pl.ds(0, rows)], local_sem.at[2]),
            pltpu.make_async_copy(cot_in, cot.at[pl.ds(0, rows)], local_sem.at[3]),
        ]
        if end:
            locals_ += [
                pltpu.make_async_copy(up_in.at[:, pl.ds(nown, give)], up_give, local_sem.at[4]),
                pltpu.make_async_copy(down_in.at[pl.ds(nown, give)], down_give, local_sem.at[5]),
            ]
        for cp in locals_:
            cp.start()
        barrier = pltpu.get_barrier_semaphore()
        peers = (mate, xn, yn, inner, across) if end else (mate, xn, yn, inner, outer)
        for peer in peers:
            pl.semaphore_signal(barrier, inc=1, device_id=peer, device_id_type=MESH)
        pl.semaphore_wait(barrier, len(peers))
        for cp in locals_:
            cp.wait()

        sends = []

        def remote(src, dst, s, r, peer):
            return pltpu.make_async_remote_copy(
                src_ref=src, dst_ref=dst, send_sem=s, recv_sem=r, device_id=peer, device_id_type=MESH
            )

        def go(cp):
            cp.start()
            sends.append(cp)

        def piece(o, q):
            if q < 2:
                return up.at[pl.ds(pl.multiple_of(o * dl + q * hd, hd), hd), pl.ds(0, nown)]
            if q < 4:
                return down.at[pl.ds((q - 2) * (nown // 2), nown // 2), cols(o)]
            if q == 4:
                return up.at[cols(o), pl.ds(fl, give)]
            return down.at[pl.ds(fl, give), cols(o)]

        pieces = Q if end else range(6)
        wx = [[remote(piece(o, q), piece(o, q), wxs.at[i, q], wxr.at[i, q], xn) for q in pieces]
              for i, o in enumerate((fs, fy_))]
        wy = [[remote(piece(o, q), piece(o, q), wys.at[i, q], wyr.at[i, q], yn) for q in pieces]
              for i, o in enumerate((fs, fx_))]

        def rows_of(j, u, shift=0):
            return bufs[j % 2].at[pl.ds(u * unit + shift + (j // 2) * hr, hr)]

        def t_send(flow, j, u, v, peer):
            go(remote(rows_of(j, u), rows_of(j, v), ts.at[flow, j], tr.at[v, j], peer))

        def t_wait(u, j):
            remote(rows_of(j, u), rows_of(j, u), ts.at[0, j], tr.at[u, j], mate).wait_recv()

        tm = [[remote(rows_of(j, u), rows_of(j, u, rows), tms.at[u, j], tmr.at[u, j], mate) for j in Q]
              for u in range(4)]

        def w_got(q):
            wx[0][q].wait_recv()
            if q % 2 == 0:
                go(wy[1][q])
            wy[0][q].wait_recv()
            if q % 2:
                go(wx[1][q])

        ex = (remote(up_give, up.at[cols(fs), pl.ds(fl, give)], exs.at[0], exr.at[0], inner),
              remote(down_give, down.at[pl.ds(fl, give), cols(fs)], exs.at[1], exr.at[1], inner))

        def hidden_block(u):
            here = pl.ds(u * unit, unit)
            active = jnp.maximum(dot(tok[here, :], up[:, units], 1, 0), 0.0)
            hid[here, units] = (active * active).astype(BF16)
            dh = dot(cot[here, :], down[units, :], 1, 1)
            dpre[here, units] = (2.0 * active * dh).astype(BF16)

        dxm = [remote(dxm_send.at[u], dxm_recv.at[u], ms.at[u], mr.at[u], mate) for u in range(4)]

        def dx_block(u):
            here = pl.ds(u * unit, unit)

            def tile(j, carry):
                o = cols(j)
                part = dot(dpre[here, units], up[o, units], 1, 1)
                dx_own[u, :, o] = part[:rows]
                dxm_send[u, :, o] = part[rows:].astype(BF16)
                return carry

            lax.fori_loop(0, 4, tile, 0)
            go(dxm[u])

        def dx_sum(u):
            dxm[u].wait_recv()
            return dx_own[u] + dxm_recv[u].astype(F32)

        def z_wait(slot):
            remote(dxz_send.at[0], dxz_recv.at[slot], dzs.at[0], dzr.at[slot], mate).wait_recv()
            return dxz_recv[slot].astype(F32)

        def z_send(i, value, slot, peer):
            dxz_send[i] = value.astype(BF16)
            go(remote(dxz_send.at[i], dxz_recv.at[slot], dzs.at[i], dzr.at[slot], peer))

        def ready(u):
            for j in Q:
                tm[u][j].wait_recv()
            hidden_block(u)

        if end:
            for cp in ex:
                go(cp)
            for q in Q:
                go(wx[0][q])
                go(wy[0][q])
            for j in Q:
                t_send(0, j, 0, 1, inner)
            for j in Q:
                go(tm[0][j])
            for j in Q:
                w_got(j)
                t_wait(1, j)
                go(tm[1][j])
            for q in Q:
                (wy if q % 2 else wx)[1][q ^ 1].wait_recv()
            ready(0)
            ready(1)
            dx_block(1)
            t_wait(2, 0)
            go(tm[2][0])
            z_send(0, dx_sum(1), 0, inner)
            for j in (1, 2, 3):
                t_wait(2, j)
                go(tm[2][j])
            ready(2)
            dx_block(2)
            t_wait(3, 0)
            go(tm[3][0])
            z_send(1, dx_sum(2), 1, inner)
        else:
            for q in Q:
                go(wx[0][q])
                go(wy[0][q])
            for j in Q:
                t_send(0, j, 0, 1, outer)
                t_send(1, j, 0, 2, inner)
            for j in Q:
                go(tm[0][j])
            for i in range(2):
                ex[i].wait_recv()
                go(wx[0][4 + i])
                go(wy[0][4 + i])
            for j in Q:
                t_wait(1, j)
                t_send(2, j, 1, 3, inner)
                go(tm[1][j])
                t_wait(2, j)
                t_send(3, j, 2, 2, outer)
                go(tm[2][j])
                w_got(j)
            w_got(4)
            w_got(5)
            for j in (0, 1, 2):
                t_wait(3, j)
                t_send(4, j, 3, 3, outer)
                go(tm[3][j])
            for q in pieces:
                (wy if q % 2 else wx)[1][q ^ 1].wait_recv()
            ready(0)
            ready(1)
            t_wait(3, 3)
            t_send(4, 3, 3, 3, outer)
            go(tm[3][3])
            ready(2)

        early = pl.ds(0, 3 * unit)
        last = pl.ds(3 * unit, unit)

        def ug_early(o, carry):
            ug_acc[cols(o), units] = dot(tok[early, cols(o)], dpre[early, units], 0, 0)
            return carry

        def dg_early(o, carry):
            dg_acc[units, cols(o)] = dot(hid[early, units], cot[early, cols(o)], 0, 0)
            return carry

        if end:
            lax.fori_loop(0, 4, ug_early, 0)
            lax.fori_loop(0, 4, dg_early, 0)
            dx_block(0)
            for j in (1, 2, 3):
                t_wait(3, j)
                go(tm[3][j])
        ready(3)

        def buf(pair, k, q):
            up_buf, down_buf = pair
            if q < 2:
                return up_buf.at[k, q, :, pl.ds(0, nf)]
            return down_buf.at[k, q - 2, pl.ds(0, hf)]

        out_bufs, in_bufs = (ug_send, dg_send), (ug_recv, dg_recv)

        def g_copy(k, q):
            over_x = k == 1 or (k == 0 and q % 2 == 0)
            return remote(buf(out_bufs, k, q), buf(in_bufs, k, q), gs.at[k, q], gr.at[k, q], xn if over_x else yn)

        g = [[g_copy(k, q) for q in Q] for k in range(3)]

        def acc_of(o, q):
            if q < 2:
                return ug_acc, pl.ds(pl.multiple_of(o * dl + q * hd, hd), hd), units
            return dg_acc, pl.ds((q - 2) * hf, hf), cols(o)

        def g_put(k, q, value):
            dst = buf(out_bufs, k, q)
            dst[...] = value.astype(BF16)
            go(g[k][q])

        def terms(o, p):
            part = last if end else slice(None)
            if p == 0:
                val = dot(tok[part, cols(o)], dpre[part, units], 0, 0)
                if end:
                    val = val + ug_acc[cols(o), units]
                return val[:hd], val[hd:]
            val = dot(hid[part, units], cot[part, cols(o)], 0, 0)
            if end:
                val = val + dg_acc[units, cols(o)]
            return val[:hf], val[hf:]

        def keep(o, q, value):
            ref, a, b = acc_of(o, q)
            ref[a, b] = value

        for p in range(2):
            for h, v in enumerate(terms(fd_, p)):
                g_put(0, 2 * p + h, v)
        for p in range(2):
            even, odd = terms(fx_, p)
            g_put(1, 2 * p, even)
            keep(fx_, 2 * p + 1, odd)
            even, odd = terms(fy_, p)
            g_put(2, 2 * p + 1, odd)
            keep(fy_, 2 * p, even)
        dx_block(3)

        def pass_on(q):
            g[0][q].wait_recv()
            k, o = (1, fx_) if q % 2 else (2, fy_)
            ref, a, b = acc_of(o, q)
            g_put(k, q, ref[a, b] + buf(in_bufs, 0, q)[...].astype(F32))

        if not end:
            z_send(1, dx_sum(3), 3, inner)
        pass_on(0)
        pass_on(1)
        if end:
            z_send(2, dx_sum(3), 1, across)
        for p in range(2):
            for h, v in enumerate(terms(fs, p)):
                keep(fs, 2 * p + h, v)
        pass_on(2)
        pass_on(3)
        if not end:
            dx_block(2)
            dx_block(1)
            dx_block(0)
            z_send(0, dx_sum(2) + z_wait(1), 2, inner)
            z_send(2, dx_sum(1) + z_wait(3), 0, outer)

        back = (remote(ug_back, ug_home, bs.at[0], br.at[0], outer),
                remote(dg_back, dg_home, bs.at[1], br.at[1], outer))

        def finish(q):
            ref, a, b = acc_of(fs, q)
            total = ref[a, b]
            for k in (1, 2):
                g[k][q].wait_recv()
                total = total + buf(in_bufs, k, q)[...].astype(F32)
            if q < 2:
                r = pl.ds(q * hd, hd)
                ug_out[r, pl.ds(0, nown)] = total[:, :nown] * factor
                if not end:
                    ug_back[r, :] = total[:, nown:].astype(BF16)
            else:
                n = min(nown - (q - 2) * hf, hf)
                dg_out[pl.ds((q - 2) * hf, n), :] = total[:n] * factor
                if n < hf:
                    dg_back[...] = total[n:].astype(BF16)

        for q in (0, 1):
            finish(q)
        if not end:
            go(back[0])
        for q in (2, 3):
            finish(q)
        if not end:
            go(back[1])
            near = dx_sum(0) + z_wait(0)
            dx_out[...] = (near + z_wait(2)).astype(BF16)
        else:
            near = dx_sum(0) + z_wait(0)
            dx_out[...] = (near + z_wait(1)).astype(BF16)
            back[0].wait_recv()
            ug_out[:, pl.ds(nown, give)] = ug_home[...].astype(F32) * factor
            back[1].wait_recv()
            dg_out[pl.ds(nown, give), :] = dg_home[...].astype(F32) * factor
        for cp in sends:
            cp.wait_send()

    pl.when(at_end)(lambda: body(True))
    pl.when(jnp.logical_not(at_end))(lambda: body(False))


def put_out(n, *refs):
    copies = [pltpu.make_async_copy(refs[i], refs[n + i], refs[2 * n].at[i]) for i in range(n)]
    for cp in copies:
        cp.start()
    for cp in copies:
        cp.wait()


def line_shards(nfs, ntp, tokens, up_weight, down_weight, cotangent):
    rows, width = tokens.shape
    dl, fl = up_weight.shape
    factor = 1.0 / (rows * ntp * nfs) ** 0.5
    mine = ntp * rows
    give = fl // 4
    most = fl + give
    hd, hf = dl // 2, most // 2
    dma = pltpu.SemaphoreType.DMA
    any_space = pl.BlockSpec(memory_space=pl.ANY)
    vmem = pl.BlockSpec(memory_space=pltpu.VMEM)
    V = pltpu.VMEM
    results = pl.pallas_call(
        functools.partial(line_kernel, factor, give),
        out_shape=(V((rows, width), BF16), V((dl, fl), F32), V((fl, dl), F32)),
        in_specs=[any_space] * 4,
        out_specs=(vmem, vmem, vmem),
        scratch_shapes=[
            V((mine, width), BF16), V((mine, width), BF16),
            V((width, most), BF16), V((most, width), BF16),
            V((dl, give), BF16), V((give, dl), BF16),
            V((mine, most), BF16), V((mine, most), BF16),
            V((width, most), F32), V((most, width), F32),
            V((3, 2, hd, most), BF16), V((3, 2, hd, most), BF16),
            V((3, 2, hf, dl), BF16), V((3, 2, hf, dl), BF16),
            V((dl, give), BF16), V((give, dl), BF16), V((dl, give), BF16), V((give, dl), BF16),
            V((4, rows, width), F32), V((4, rows, width), BF16), V((4, rows, width), BF16),
            V((3, rows, width), BF16), V((4, rows, width), BF16),
            dma((6,)), dma((2,)), dma((2,)), dma((2, 6)), dma((2, 6)), dma((2, 6)), dma((2, 6)),
            dma((5, 4)), dma((4, 4)), dma((4, 4)), dma((4, 4)),
            dma((4,)), dma((4,)), dma((3,)), dma((4,)), dma((3, 4)), dma((3, 4)), dma((2,)), dma((2,)),
        ],
        compiler_params=pltpu.CompilerParams(
            collective_id=0, has_side_effects=True, vmem_limit_bytes=60_000_000
        ),
    )(tokens, up_weight, down_weight, cotangent)
    return pl.pallas_call(
        functools.partial(put_out, len(results)),
        out_shape=tuple(jax.ShapeDtypeStruct(r.shape, r.dtype) for r in results),
        in_specs=[vmem] * len(results),
        out_specs=(any_space,) * len(results),
        scratch_shapes=[dma((3,))],
        compiler_params=pltpu.CompilerParams(vmem_limit_bytes=8_000_000),
    )(*results)


def solution(mesh):
    placed = (P(("fs", "tp"), None), P("fs", "tp"), P("tp", "fs"), P(("fs", "tp"), None))
    fs, tp = mesh.shape["fs"], mesh.shape["tp"]
    body = line_shards if (fs, tp) == (4, 8) else shards
    return jax.shard_map(
        functools.partial(body, mesh.shape["fs"], mesh.shape["tp"]),
        mesh=mesh,
        in_specs=placed,
        out_specs=(P(("fs", "tp"), None), P("fs", "tp"), P("tp", "fs")),
        check_vma=False,
    )
```

```python
import functools

import jax
import jax.numpy as jnp
from jax import lax
from jax.experimental import pallas as pl
from jax.experimental.pallas import tpu as pltpu
from jax.sharding import PartitionSpec as P

MESH = pl.DeviceIdType.MESH
BF16 = jnp.bfloat16
F32 = jnp.float32


def ring_index(p):
    q, b = p // 2, p % 2
    return 2 * q + b + (q % 2) * (1 - 2 * b)


def dot(a, b, ca, cb):
    return lax.dot_general(a, b, (((ca,), (cb,)), ((), ())), preferred_element_type=F32)


def kernel(
    nfs, nz, factor,
    tok_in, up_in, down_in, cot_in,
    dx_out, ug_out, dg_out,
    tok, cot, up, down, hid, dpre,
    dx_own, dx_send, dx_recv, dr_send, dr_recv,
    ug_own, dg_own, ug_send, ug_recv, dg_send, dg_recv,
    local_sem, zs, zr, ps, pr, ws, wr, gs, gr, xs, xr, rs, rr,
):
    fs, tp = lax.axis_index("fs"), lax.axis_index("tp")
    rows, width = tok_in.shape
    h = rows // 2
    block = 4 * h
    dl = up_in.shape[0]
    fl = up_in.shape[1]
    z, core = tp // 2, tp % 2
    pos = ring_index(fs)
    fwd = (fs, ((z + 1) % nz) * 2 + core)
    bwd = (fs, ((z + nz - 1) % nz) * 2 + core)
    mate = (fs, 2 * z + 1 - core)
    cw = (ring_index((pos + 1) % nfs), tp)
    ccw = (ring_index((pos + nfs - 1) % nfs), tp)

    def cols(o):
        return pl.ds(pl.multiple_of(o * dl, dl), dl)

    locals_ = [
        pltpu.make_async_copy(tok_in, tok.at[pl.ds(0, rows)], local_sem.at[0]),
        pltpu.make_async_copy(up_in, up.at[cols(fs)], local_sem.at[1]),
        pltpu.make_async_copy(down_in, down.at[:, cols(fs)], local_sem.at[2]),
        pltpu.make_async_copy(cot_in, cot.at[pl.ds(0, rows)], local_sem.at[3]),
    ]
    for c in locals_:
        c.start()
    barrier = pltpu.get_barrier_semaphore()
    peers = (fwd, bwd, mate, cw, ccw)
    for peer in peers:
        pl.semaphore_signal(barrier, inc=1, device_id=peer, device_id_type=MESH)
    pl.semaphore_wait(barrier, len(peers))
    for c in locals_:
        c.wait()

    sends = []

    def remote(src, dst, s, r, peer):
        c = pltpu.make_async_remote_copy(
            src_ref=src, dst_ref=dst, send_sem=s, recv_sem=r, device_id=peer, device_id_type=MESH
        )
        c.start()
        sends.append(c)
        return c

    bufs = (tok, cot)

    def z_send(k, a):
        out = []
        for d, peer in enumerate((fwd, bwd)):
            out.append(remote(
                bufs[a].at[pl.ds(k * block + d * h, h)],
                bufs[a].at[pl.ds((k + 1) * block + d * h, h)],
                zs.at[k, d, a], zr.at[k, d, a], peer,
            ))
        return out

    def mate_send(k, a):
        return remote(
            bufs[a].at[pl.ds(k * block, 2 * h)],
            bufs[a].at[pl.ds(k * block + 2 * h, 2 * h)],
            ps.at[k, a], pr.at[k, a], mate,
        )

    def w_send(k, half):
        a = ring_index((pos + nfs - k) % nfs)
        b = ring_index((pos + k) % nfs)
        n = dl // 2
        piece = up.at[pl.ds(pl.multiple_of(a * dl + half * n, n), n)]
        m = fl // 2
        other = down.at[pl.ds(half * m, m), cols(b)]
        return [
            remote(piece, piece, ws.at[k, half, 0], wr.at[k, half, 0], cw),
            remote(other, other, ws.at[k, half, 1], wr.at[k, half, 1], ccw),
        ]

    z_copy, w_copy, mate_copy = {}, {}, {}
    for a in range(2):
        z_copy[0, a] = z_send(0, a)
        w_copy[0, a] = w_send(0, a)
    for a in range(2):
        mate_copy[0, a] = mate_send(0, a)

    def hidden_block(s):
        here = pl.ds(s * block, block)
        active = jnp.maximum(dot(tok[here, :], up[...], 1, 0), 0.0)
        hid[here, :] = (active * active).astype(BF16)
        dh = dot(cot[here, :], down[...], 1, 1)
        dpre[here, :] = (2.0 * active * dh).astype(BF16)

    pair_copy = {}

    def dx_block(s):
        here = pl.ds(s * block, block)

        def tile(j, carry):
            c = cols(j)
            part = dot(dpre[here, :], up[c, :], 1, 1)
            dx_own[s, :, c] = part[: 2 * h]
            dx_send[s, :, c] = part[2 * h :].astype(BF16)
            return carry

        lax.fori_loop(0, nfs, tile, 0)
        pair_copy[s] = remote(dx_send.at[s], dx_recv.at[s], xs.at[s], xr.at[s], mate)

    x_copy = {}

    def x_step(r):
        s = r + 1 if r < nz - 1 else 0
        pair_copy[s].wait_recv()
        for d, peer in enumerate((fwd, bwd)):
            here = pl.ds(d * h, h)
            if r > 0:
                x_copy[r - 1, d].wait_recv()
            total = dx_own[s, here, :] + dx_recv[s, here, :].astype(F32)
            if r > 0:
                total = total + dr_recv[r - 1, here, :].astype(F32)
            if r < nz - 1:
                dr_send[r, here, :] = total.astype(BF16)
                x_copy[r, d] = remote(
                    dr_send.at[r, here], dr_recv.at[r, here], rs.at[r, d], rr.at[r, d], peer
                )
            else:
                dx_out[here, :] = total.astype(BF16)

    events = []
    for k in range(nfs - 1):
        for half in range(2):
            events.append(((2 * k + half + 1) * 1.5 / (nfs - 1), 1, k, half))
    for k in range(nz - 1):
        for a in range(2):
            events.append(((2 * k + a + 1) * 3.0 / (nz - 1), 0, k, a))
    events.sort()
    weights_left = 2 * (nfs - 1)
    ready = [0]

    def settle(s):
        for a in range(2):
            mate_copy[s, a].wait_recv()
        hidden_block(s)
        if s < nz - 1:
            dx_block(s)

    for _, kind, k, a in events:
        if kind == 1:
            for c in w_copy[k, a]:
                c.wait_recv()
            if k + 1 < nfs - 1:
                w_copy[k + 1, a] = w_send(k + 1, a)
            weights_left -= 1
        else:
            for c in z_copy[k, a]:
                c.wait_recv()
            if k + 1 < nz - 1:
                z_copy[k + 1, a] = z_send(k + 1, a)
            mate_copy[k + 1, a] = mate_send(k + 1, a)
            if a == 1:
                ready.append(k + 1)
        if weights_left == 0 and (kind, k) != (0, nz - 2):
            for s in ready:
                settle(s)
            ready = []
    for s in ready[:-1]:
        settle(s)
    x_step(0)
    settle(ready[-1])

    def up_term(r):
        o = ring_index((pos + nfs - r - 1) % nfs)
        return dot(tok[:, cols(o)], dpre[...], 0, 0)

    def down_term(r):
        o = ring_index((pos + r + 1) % nfs)
        return dot(hid[...], cot[:, cols(o)], 0, 0)

    g_copy = {}

    def g_send(r, half, which):
        n, m = dl // 2, fl // 2
        a, b = pl.ds(half * n, n), pl.ds(half * m, m)
        if which == 0:
            g_copy[r, half, 0] = remote(
                ug_send.at[r, a], ug_recv.at[r, a], gs.at[r, half, 0], gr.at[r, half, 0], cw
            )
        else:
            g_copy[r, half, 1] = remote(
                dg_send.at[r, b], dg_recv.at[r, b], gs.at[r, half, 1], gr.at[r, half, 1], ccw
            )

    def g_terms(r):
        ug_own[...] = up_term(r)
        dg_own[...] = down_term(r)

    def g_first():
        ug_send[0] = up_term(0).astype(BF16)
        for half in range(2):
            g_send(0, half, 0)
        dg_send[0] = down_term(0).astype(BF16)
        for half in range(2):
            g_send(0, half, 1)
        g_terms(1)

    def g_step(r, half):
        n, m = dl // 2, fl // 2
        a, b = pl.ds(half * n, n), pl.ds(half * m, m)
        g_copy[r - 1, half, 0].wait_recv()
        gu = ug_own[a, :] + ug_recv[r - 1, a, :].astype(F32)
        if r < nfs - 1:
            ug_send[r, a, :] = gu.astype(BF16)
            g_send(r, half, 0)
        else:
            ug_out[a, :] = gu * factor
        g_copy[r - 1, half, 1].wait_recv()
        gd = dg_own[b, :] + dg_recv[r - 1, b, :].astype(F32)
        if r < nfs - 1:
            dg_send[r, b, :] = gd.astype(BF16)
            g_send(r, half, 1)
        else:
            dg_out[b, :] = gd * factor

    g_first()
    dx_block(nz - 1)
    for r in range(1, max(nfs, nz)):
        if r < nfs:
            g_step(r, 0)
        if r < nz:
            x_step(r)
        if r < nfs:
            g_step(r, 1)
            if r < nfs - 1:
                g_terms(r + 1)
    for c in sends:
        c.wait_send()


def shards(nfs, ntp, tokens, up_weight, down_weight, cotangent):
    rows, width = tokens.shape
    dl, fl = up_weight.shape
    nz = ntp // 2
    whole = rows * ntp
    factor = 1.0 / (whole * nfs) ** 0.5
    dma = pltpu.SemaphoreType.DMA
    any_space = pl.BlockSpec(memory_space=pl.ANY)
    vmem = pl.BlockSpec(memory_space=pltpu.VMEM)
    return pl.pallas_call(
        functools.partial(kernel, nfs, nz, factor),
        out_shape=(
            jax.ShapeDtypeStruct((rows, width), BF16),
            jax.ShapeDtypeStruct((dl, fl), F32),
            jax.ShapeDtypeStruct((fl, dl), F32),
        ),
        in_specs=[any_space] * 4,
        out_specs=(vmem, vmem, vmem),
        scratch_shapes=[
            pltpu.VMEM((whole, width), BF16),
            pltpu.VMEM((whole, width), BF16),
            pltpu.VMEM((width, fl), BF16),
            pltpu.VMEM((fl, width), BF16),
            pltpu.VMEM((whole, fl), BF16),
            pltpu.VMEM((whole, fl), BF16),
            pltpu.VMEM((nz, rows, width), F32),
            pltpu.VMEM((nz, rows, width), BF16),
            pltpu.VMEM((nz, rows, width), BF16),
            pltpu.VMEM((nz - 1, rows, width), BF16),
            pltpu.VMEM((nz - 1, rows, width), BF16),
            pltpu.VMEM((dl, fl), F32),
            pltpu.VMEM((fl, dl), F32),
            pltpu.VMEM((nfs - 1, dl, fl), BF16),
            pltpu.VMEM((nfs - 1, dl, fl), BF16),
            pltpu.VMEM((nfs - 1, fl, dl), BF16),
            pltpu.VMEM((nfs - 1, fl, dl), BF16),
            dma((4,)),
            dma((nz - 1, 2, 2)), dma((nz - 1, 2, 2)),
            dma((nz, 2)), dma((nz, 2)),
            dma((nfs - 1, 2, 2)), dma((nfs - 1, 2, 2)),
            dma((nfs - 1, 2, 2)), dma((nfs - 1, 2, 2)),
            dma((nz,)), dma((nz,)),
            dma((nz - 1, 2)), dma((nz - 1, 2)),
        ],
        compiler_params=pltpu.CompilerParams(
            collective_id=0, has_side_effects=True, vmem_limit_bytes=67_000_000
        ),
    )(tokens, up_weight, down_weight, cotangent)


def line_kernel(
    factor, give,
    tok_in, up_in, down_in, cot_in,
    dx_out, ug_out, dg_out,
    tok, cot, up, down, up_give, down_give, hid, dpre, ug_acc, dg_acc,
    ug_send, ug_recv, dg_send, dg_recv, ug_back, dg_back, ug_home, dg_home,
    dx_own, dxm_send, dxm_recv, dxz_send, dxz_recv,
    local_sem, exs, exr, wxs, wxr, wys, wyr, ts, tr, tms, tmr,
    ms, mr, dzs, dzr, gs, gr, bs, br,
):
    fs, tp = lax.axis_index("fs"), lax.axis_index("tp")
    rows, width = tok_in.shape
    dl, fl = up_in.shape
    unit, hr, hd = 2 * rows, rows // 2, dl // 2
    x, y, z, c = fs % 2, fs // 2, tp // 2, tp % 2
    high = z // 2
    toward = 1 - 2 * high
    at_end = z % 3 == 0
    fx_, fy_, fd_ = 2 * y + 1 - x, 2 * (1 - y) + x, 2 * (1 - y) + 1 - x
    mate = (fs, 2 * z + 1 - c)
    xn, yn = (fx_, tp), (fy_, tp)
    inner = (fs, 2 * (z + toward) + c)
    outer = (fs, 2 * jnp.maximum(z - toward, 0) + c)
    beyond = (fs, 2 * (z + 2 * toward) + c)
    Q = range(4)

    def cols(o):
        return pl.ds(pl.multiple_of(o * dl, dl), dl)

    bufs = (tok, cot)

    def body(end):
        nf = fl - give if end else fl + give
        hf = nf // 2
        nown = fl - give if end else fl
        units = slice(0, nf)
        locals_ = [
            pltpu.make_async_copy(up_in.at[:, pl.ds(0, nown)], up.at[cols(fs), pl.ds(0, nown)], local_sem.at[0]),
            pltpu.make_async_copy(down_in.at[pl.ds(0, nown)], down.at[pl.ds(0, nown), cols(fs)], local_sem.at[1]),
            pltpu.make_async_copy(tok_in, tok.at[pl.ds(0, rows)], local_sem.at[2]),
            pltpu.make_async_copy(cot_in, cot.at[pl.ds(0, rows)], local_sem.at[3]),
        ]
        if end:
            locals_ += [
                pltpu.make_async_copy(up_in.at[:, pl.ds(nown, give)], up_give, local_sem.at[4]),
                pltpu.make_async_copy(down_in.at[pl.ds(nown, give)], down_give, local_sem.at[5]),
            ]
        for cp in locals_:
            cp.start()
        barrier = pltpu.get_barrier_semaphore()
        peers = (mate, xn, yn, inner, beyond) if end else (mate, xn, yn, inner, beyond, outer)
        for peer in peers:
            pl.semaphore_signal(barrier, inc=1, device_id=peer, device_id_type=MESH)
        pl.semaphore_wait(barrier, len(peers))
        for cp in locals_:
            cp.wait()

        sends = []

        def remote(src, dst, s, r, peer):
            return pltpu.make_async_remote_copy(
                src_ref=src, dst_ref=dst, send_sem=s, recv_sem=r, device_id=peer, device_id_type=MESH
            )

        def go(cp):
            cp.start()
            sends.append(cp)

        def piece(o, q):
            if q < 2:
                return up.at[pl.ds(pl.multiple_of(o * dl + q * hd, hd), hd), pl.ds(0, nown)]
            if q < 4:
                return down.at[pl.ds((q - 2) * (nown // 2), nown // 2), cols(o)]
            if q == 4:
                return up.at[cols(o), pl.ds(fl, give)]
            return down.at[pl.ds(fl, give), cols(o)]

        pieces = Q if end else range(6)
        wx = [[remote(piece(o, q), piece(o, q), wxs.at[i, q], wxr.at[i, q], xn) for q in pieces]
              for i, o in enumerate((fs, fy_))]
        wy = [[remote(piece(o, q), piece(o, q), wys.at[i, q], wyr.at[i, q], yn) for q in pieces]
              for i, o in enumerate((fs, fx_))]

        def rows_of(j, u, shift=0):
            return bufs[j % 2].at[pl.ds(u * unit + shift + (j // 2) * hr, hr)]

        def t_send(flow, j, u, v, peer):
            go(remote(rows_of(j, u), rows_of(j, v), ts.at[flow, j], tr.at[v, j], peer))

        def t_wait(u, j):
            remote(rows_of(j, u), rows_of(j, u), ts.at[0, j], tr.at[u, j], mate).wait_recv()

        tm = [[remote(rows_of(j, u), rows_of(j, u, rows), tms.at[u, j], tmr.at[u, j], mate) for j in Q]
              for u in range(4)]

        def w_got(q):
            wx[0][q].wait_recv()
            if q % 2 == 0:
                go(wy[1][q])
            wy[0][q].wait_recv()
            if q % 2:
                go(wx[1][q])

        ex = (remote(up_give, up.at[cols(fs), pl.ds(fl, give)], exs.at[0], exr.at[0], inner),
              remote(down_give, down.at[pl.ds(fl, give), cols(fs)], exs.at[1], exr.at[1], inner))

        def hidden_block(u):
            here = pl.ds(u * unit, unit)
            active = jnp.maximum(dot(tok[here, :], up[:, units], 1, 0), 0.0)
            hid[here, units] = (active * active).astype(BF16)
            dh = dot(cot[here, :], down[units, :], 1, 1)
            dpre[here, units] = (2.0 * active * dh).astype(BF16)

        dxm = [remote(dxm_send.at[u], dxm_recv.at[u], ms.at[u], mr.at[u], mate) for u in range(4)]

        def dx_block(u):
            here = pl.ds(u * unit, unit)

            def tile(j, carry):
                o = cols(j)
                part = dot(dpre[here, units], up[o, units], 1, 1)
                dx_own[u, :, o] = part[:rows]
                dxm_send[u, :, o] = part[rows:].astype(BF16)
                return carry

            lax.fori_loop(0, 4, tile, 0)
            go(dxm[u])

        def dx_sum(u):
            dxm[u].wait_recv()
            return dx_own[u] + dxm_recv[u].astype(F32)

        def z_wait(slot):
            remote(dxz_send.at[0], dxz_recv.at[slot], dzs.at[0], dzr.at[slot], mate).wait_recv()
            return dxz_recv[slot].astype(F32)

        def z_send(i, value, slot, peer):
            dxz_send[i] = value.astype(BF16)
            go(remote(dxz_send.at[i], dxz_recv.at[slot], dzs.at[i], dzr.at[slot], peer))

        def ready(u):
            for j in Q:
                tm[u][j].wait_recv()
            hidden_block(u)

        if end:
            for cp in ex:
                go(cp)
            for q in Q:
                go(wx[0][q])
                go(wy[0][q])
            for j in Q:
                t_send(0, j, 0, 1, inner)
            for j in Q:
                go(tm[0][j])
            for j in Q:
                w_got(j)
                t_wait(1, j)
                go(tm[1][j])
            for q in Q:
                (wy if q % 2 else wx)[1][q ^ 1].wait_recv()
            ready(0)
            ready(1)
            dx_block(1)
            t_wait(2, 0)
            go(tm[2][0])
            z_send(0, dx_sum(1), 0, inner)
            for j in (1, 2, 3):
                t_wait(2, j)
                go(tm[2][j])
            ready(2)
            dx_block(2)
            t_wait(3, 0)
            go(tm[3][0])
            z_send(1, dx_sum(2), 1, inner)
        else:
            for q in Q:
                go(wx[0][q])
                go(wy[0][q])
            for j in Q:
                t_send(0, j, 0, 1, outer)
            for j in (0, 1):
                t_send(1, j, 0, 3, inner)
            for j in Q:
                go(tm[0][j])
            for i in range(2):
                ex[i].wait_recv()
                go(wx[0][4 + i])
                go(wy[0][4 + i])

            def from_end(j):
                t_wait(1, j)
                t_send(2, j, 1, 2, inner)
                go(tm[1][j])

            def from_middle(j):
                t_wait(3, j)
                go(tm[3][j])

            def from_far(j):
                t_wait(2, j)
                t_send(4, j, 2, 2, outer)
                go(tm[2][j])

            from_end(0)
            w_got(0)
            from_end(1)
            from_middle(0)
            from_middle(1)
            w_got(1)
            from_end(2)
            from_far(0)
            w_got(2)
            from_end(3)
            for j in (2, 3):
                t_send(1, j, 0, 3, inner)
            from_far(1)
            w_got(3)
            w_got(4)
            w_got(5)
            from_far(2)
            from_far(3)
            for j in (0, 1):
                t_send(3, j, 3, 3, outer)

            def half_sums(u):
                here = pl.ds(u * unit, unit)
                return (ug_acc, pl.ds(u * unit, unit), units), (ug_acc, pl.ds((u + 4) * unit, unit), units), here

            def products(here, o):
                return (dot(tok[here, cols(o)], up[cols(o), units], 1, 0),
                        dot(cot[here, cols(o)], down[units, cols(o)], 1, 1))

            for u in range(3):
                for j in Q:
                    tm[u][j].wait_recv()
                (ref, a, k), (_, b, _), here = half_sums(u)
                for i, o in enumerate((fs, fx_, fy_)):
                    pre, dh = products(here, o)
                    if i:
                        pre, dh = pre + ref[a, k], dh + ref[b, k]
                    ref[a, k] = pre
                    ref[b, k] = dh
            for q in pieces:
                (wy if q % 2 else wx)[1][q ^ 1].wait_recv()
            for u in range(3):
                (ref, a, k), (_, b, _), here = half_sums(u)
                pre, dh = products(here, fd_)
                active = jnp.maximum(pre + ref[a, k], 0.0)
                hid[here, units] = (active * active).astype(BF16)
                dpre[here, units] = (2.0 * active * (dh + ref[b, k])).astype(BF16)
            for j in (2, 3):
                from_middle(j)
                t_send(3, j, 3, 3, outer)

        early = pl.ds(0, 3 * unit)
        last = pl.ds(3 * unit, unit)

        def ug_early(o, carry):
            ug_acc[cols(o), units] = dot(tok[early, cols(o)], dpre[early, units], 0, 0)
            return carry

        def dg_early(o, carry):
            dg_acc[units, cols(o)] = dot(hid[early, units], cot[early, cols(o)], 0, 0)
            return carry

        if end:
            lax.fori_loop(0, 4, ug_early, 0)
            lax.fori_loop(0, 4, dg_early, 0)
            dx_block(0)
            for j in (1, 2, 3):
                t_wait(3, j)
                go(tm[3][j])
        else:
            ug_early(fd_, 0)
            dg_early(fd_, 0)
        ready(3)

        def buf(pair, k, q):
            up_buf, down_buf = pair
            if q < 2:
                return up_buf.at[k, q, :, pl.ds(0, nf)]
            return down_buf.at[k, q - 2, pl.ds(0, hf)]

        out_bufs, in_bufs = (ug_send, dg_send), (ug_recv, dg_recv)

        def g_copy(k, q):
            over_x = k == 1 or (k == 0 and q % 2 == 0)
            return remote(buf(out_bufs, k, q), buf(in_bufs, k, q), gs.at[k, q], gr.at[k, q], xn if over_x else yn)

        g = [[g_copy(k, q) for q in Q] for k in range(3)]

        def acc_of(o, q):
            if q < 2:
                return ug_acc, pl.ds(pl.multiple_of(o * dl + q * hd, hd), hd), units
            return dg_acc, pl.ds((q - 2) * hf, hf), cols(o)

        def g_put(k, q, value):
            dst = buf(out_bufs, k, q)
            dst[...] = value.astype(BF16)
            go(g[k][q])

        def terms(o, p):
            split = end or o is fd_
            part = last if split else slice(None)
            if p == 0:
                val = dot(tok[part, cols(o)], dpre[part, units], 0, 0)
                if split:
                    val = val + ug_acc[cols(o), units]
                return val[:hd], val[hd:]
            val = dot(hid[part, units], cot[part, cols(o)], 0, 0)
            if split:
                val = val + dg_acc[units, cols(o)]
            return val[:hf], val[hf:]

        def keep(o, q, value):
            ref, a, b = acc_of(o, q)
            ref[a, b] = value

        for p in range(2):
            for h, v in enumerate(terms(fd_, p)):
                g_put(0, 2 * p + h, v)
        for p in range(2):
            even, odd = terms(fx_, p)
            g_put(1, 2 * p, even)
            keep(fx_, 2 * p + 1, odd)
            even, odd = terms(fy_, p)
            g_put(2, 2 * p + 1, odd)
            keep(fy_, 2 * p, even)
        dx_block(3 if end else 2)

        def pass_on(q):
            g[0][q].wait_recv()
            k, o = (1, fx_) if q % 2 else (2, fy_)
            ref, a, b = acc_of(o, q)
            g_put(k, q, ref[a, b] + buf(in_bufs, 0, q)[...].astype(F32))

        pass_on(0)
        pass_on(1)
        if end:
            z_send(2, dx_sum(3), 4, beyond)
        else:
            z_send(1, dx_sum(2) + z_wait(1), 3, inner)
        for p in range(2):
            for h, v in enumerate(terms(fs, p)):
                keep(fs, 2 * p + h, v)
        pass_on(2)
        pass_on(3)
        if not end:
            dx_block(3)
            dx_block(1)
            dx_block(0)
            z_send(0, dx_sum(3), 2, inner)
            z_send(2, dx_sum(1) + z_wait(3), 0, outer)

        back = (remote(ug_back, ug_home, bs.at[0], br.at[0], outer),
                remote(dg_back, dg_home, bs.at[1], br.at[1], outer))

        def finish(q):
            ref, a, b = acc_of(fs, q)
            total = ref[a, b]
            for k in (1, 2):
                g[k][q].wait_recv()
                total = total + buf(in_bufs, k, q)[...].astype(F32)
            if q < 2:
                r = pl.ds(q * hd, hd)
                ug_out[r, pl.ds(0, nown)] = total[:, :nown] * factor
                if not end:
                    ug_back[r, :] = total[:, nown:].astype(BF16)
            else:
                n = min(nown - (q - 2) * hf, hf)
                dg_out[pl.ds((q - 2) * hf, n), :] = total[:n] * factor
                if n < hf:
                    dg_back[...] = total[n:].astype(BF16)

        for q in (0, 1):
            finish(q)
        if not end:
            go(back[0])
        for q in (2, 3):
            finish(q)
        if not end:
            go(back[1])
            near = dx_sum(0) + z_wait(0) + z_wait(2)
            dx_out[...] = (near + z_wait(4)).astype(BF16)
        else:
            dx_out[...] = (dx_sum(0) + z_wait(0)).astype(BF16)
            back[0].wait_recv()
            ug_out[:, pl.ds(nown, give)] = ug_home[...].astype(F32) * factor
            back[1].wait_recv()
            dg_out[pl.ds(nown, give), :] = dg_home[...].astype(F32) * factor
        for cp in sends:
            cp.wait_send()

    pl.when(at_end)(lambda: body(True))
    pl.when(jnp.logical_not(at_end))(lambda: body(False))


def put_out(n, *refs):
    copies = [pltpu.make_async_copy(refs[i], refs[n + i], refs[2 * n].at[i]) for i in range(n)]
    for cp in copies:
        cp.start()
    for cp in copies:
        cp.wait()


def line_shards(nfs, ntp, tokens, up_weight, down_weight, cotangent):
    rows, width = tokens.shape
    dl, fl = up_weight.shape
    factor = 1.0 / (rows * ntp * nfs) ** 0.5
    mine = ntp * rows
    give = fl // 4
    most = fl + give
    hd, hf = dl // 2, most // 2
    dma = pltpu.SemaphoreType.DMA
    any_space = pl.BlockSpec(memory_space=pl.ANY)
    vmem = pl.BlockSpec(memory_space=pltpu.VMEM)
    V = pltpu.VMEM
    results = pl.pallas_call(
        functools.partial(line_kernel, factor, give),
        out_shape=(V((rows, width), BF16), V((dl, fl), F32), V((fl, dl), F32)),
        in_specs=[any_space] * 4,
        out_specs=(vmem, vmem, vmem),
        scratch_shapes=[
            V((mine, width), BF16), V((mine, width), BF16),
            V((width, most), BF16), V((most, width), BF16),
            V((dl, give), BF16), V((give, dl), BF16),
            V((mine, most), BF16), V((mine, most), BF16),
            V((width, most), F32), V((most, width), F32),
            V((3, 2, hd, most), BF16), V((3, 2, hd, most), BF16),
            V((3, 2, hf, dl), BF16), V((3, 2, hf, dl), BF16),
            V((dl, give), BF16), V((give, dl), BF16), V((dl, give), BF16), V((give, dl), BF16),
            V((4, rows, width), F32), V((4, rows, width), BF16), V((4, rows, width), BF16),
            V((3, rows, width), BF16), V((5, rows, width), BF16),
            dma((6,)), dma((2,)), dma((2,)), dma((2, 6)), dma((2, 6)), dma((2, 6)), dma((2, 6)),
            dma((5, 4)), dma((4, 4)), dma((4, 4)), dma((4, 4)),
            dma((4,)), dma((4,)), dma((3,)), dma((5,)), dma((3, 4)), dma((3, 4)), dma((2,)), dma((2,)),
        ],
        compiler_params=pltpu.CompilerParams(
            collective_id=0, has_side_effects=True, vmem_limit_bytes=60_000_000
        ),
    )(tokens, up_weight, down_weight, cotangent)
    return pl.pallas_call(
        functools.partial(put_out, len(results)),
        out_shape=tuple(jax.ShapeDtypeStruct(r.shape, r.dtype) for r in results),
        in_specs=[vmem] * len(results),
        out_specs=(any_space,) * len(results),
        scratch_shapes=[dma((3,))],
        compiler_params=pltpu.CompilerParams(vmem_limit_bytes=8_000_000),
    )(*results)


def solution(mesh):
    placed = (P(("fs", "tp"), None), P("fs", "tp"), P("tp", "fs"), P(("fs", "tp"), None))
    fs, tp = mesh.shape["fs"], mesh.shape["tp"]
    body = line_shards if (fs, tp) == (4, 8) else shards
    return jax.shard_map(
        functools.partial(body, mesh.shape["fs"], mesh.shape["tp"]),
        mesh=mesh,
        in_specs=placed,
        out_specs=(P(("fs", "tp"), None), P("fs", "tp"), P("tp", "fs")),
        check_vma=False,
    )
```

```python
import functools

import jax
import jax.numpy as jnp
from jax import lax
from jax.experimental import pallas as pl
from jax.experimental.pallas import tpu as pltpu
from jax.sharding import PartitionSpec as P

MESH = pl.DeviceIdType.MESH
BF16 = jnp.bfloat16
F32 = jnp.float32


def ring_index(p):
    q, b = p // 2, p % 2
    return 2 * q + b + (q % 2) * (1 - 2 * b)


def dot(a, b, ca, cb):
    return lax.dot_general(a, b, (((ca,), (cb,)), ((), ())), preferred_element_type=F32)


def kernel(
    nfs, nz, factor,
    tok_in, up_in, down_in, cot_in,
    dx_out, ug_out, dg_out,
    tok, cot, up, down, hid, dpre,
    dx_own, dx_send, dx_recv, dr_send, dr_recv,
    ug_own, dg_own, ug_send, ug_recv, dg_send, dg_recv,
    local_sem, zs, zr, ps, pr, ws, wr, gs, gr, xs, xr, rs, rr,
):
    fs, tp = lax.axis_index("fs"), lax.axis_index("tp")
    rows, width = tok_in.shape
    h = rows // 2
    block = 4 * h
    dl = up_in.shape[0]
    fl = up_in.shape[1]
    z, core = tp // 2, tp % 2
    pos = ring_index(fs)
    fwd = (fs, ((z + 1) % nz) * 2 + core)
    bwd = (fs, ((z + nz - 1) % nz) * 2 + core)
    mate = (fs, 2 * z + 1 - core)
    cw = (ring_index((pos + 1) % nfs), tp)
    ccw = (ring_index((pos + nfs - 1) % nfs), tp)

    def cols(o):
        return pl.ds(pl.multiple_of(o * dl, dl), dl)

    locals_ = [
        pltpu.make_async_copy(tok_in, tok.at[pl.ds(0, rows)], local_sem.at[0]),
        pltpu.make_async_copy(up_in, up.at[cols(fs)], local_sem.at[1]),
        pltpu.make_async_copy(down_in, down.at[:, cols(fs)], local_sem.at[2]),
        pltpu.make_async_copy(cot_in, cot.at[pl.ds(0, rows)], local_sem.at[3]),
    ]
    for c in locals_:
        c.start()
    barrier = pltpu.get_barrier_semaphore()
    peers = (fwd, bwd, mate, cw, ccw)
    for peer in peers:
        pl.semaphore_signal(barrier, inc=1, device_id=peer, device_id_type=MESH)
    pl.semaphore_wait(barrier, len(peers))
    for c in locals_:
        c.wait()

    sends = []

    def remote(src, dst, s, r, peer):
        c = pltpu.make_async_remote_copy(
            src_ref=src, dst_ref=dst, send_sem=s, recv_sem=r, device_id=peer, device_id_type=MESH
        )
        c.start()
        sends.append(c)
        return c

    bufs = (tok, cot)

    def z_send(k, a):
        out = []
        for d, peer in enumerate((fwd, bwd)):
            out.append(remote(
                bufs[a].at[pl.ds(k * block + d * h, h)],
                bufs[a].at[pl.ds((k + 1) * block + d * h, h)],
                zs.at[k, d, a], zr.at[k, d, a], peer,
            ))
        return out

    def mate_send(k, a):
        return remote(
            bufs[a].at[pl.ds(k * block, 2 * h)],
            bufs[a].at[pl.ds(k * block + 2 * h, 2 * h)],
            ps.at[k, a], pr.at[k, a], mate,
        )

    def w_send(k, half):
        a = ring_index((pos + nfs - k) % nfs)
        b = ring_index((pos + k) % nfs)
        n = dl // 2
        piece = up.at[pl.ds(pl.multiple_of(a * dl + half * n, n), n)]
        m = fl // 2
        other = down.at[pl.ds(half * m, m), cols(b)]
        return [
            remote(piece, piece, ws.at[k, half, 0], wr.at[k, half, 0], cw),
            remote(other, other, ws.at[k, half, 1], wr.at[k, half, 1], ccw),
        ]

    z_copy, w_copy, mate_copy = {}, {}, {}
    for a in range(2):
        z_copy[0, a] = z_send(0, a)
        w_copy[0, a] = w_send(0, a)
    for a in range(2):
        mate_copy[0, a] = mate_send(0, a)

    def hidden_block(s):
        here = pl.ds(s * block, block)
        active = jnp.maximum(dot(tok[here, :], up[...], 1, 0), 0.0)
        hid[here, :] = (active * active).astype(BF16)
        dh = dot(cot[here, :], down[...], 1, 1)
        dpre[here, :] = (2.0 * active * dh).astype(BF16)

    pair_copy = {}

    def dx_block(s):
        here = pl.ds(s * block, block)

        def tile(j, carry):
            c = cols(j)
            part = dot(dpre[here, :], up[c, :], 1, 1)
            dx_own[s, :, c] = part[: 2 * h]
            dx_send[s, :, c] = part[2 * h :].astype(BF16)
            return carry

        lax.fori_loop(0, nfs, tile, 0)
        pair_copy[s] = remote(dx_send.at[s], dx_recv.at[s], xs.at[s], xr.at[s], mate)

    x_copy = {}

    def x_step(r):
        s = r + 1 if r < nz - 1 else 0
        pair_copy[s].wait_recv()
        for d, peer in enumerate((fwd, bwd)):
            here = pl.ds(d * h, h)
            if r > 0:
                x_copy[r - 1, d].wait_recv()
            total = dx_own[s, here, :] + dx_recv[s, here, :].astype(F32)
            if r > 0:
                total = total + dr_recv[r - 1, here, :].astype(F32)
            if r < nz - 1:
                dr_send[r, here, :] = total.astype(BF16)
                x_copy[r, d] = remote(
                    dr_send.at[r, here], dr_recv.at[r, here], rs.at[r, d], rr.at[r, d], peer
                )
            else:
                dx_out[here, :] = total.astype(BF16)

    events = []
    for k in range(nfs - 1):
        for half in range(2):
            events.append(((2 * k + half + 1) * 1.5 / (nfs - 1), 1, k, half))
    for k in range(nz - 1):
        for a in range(2):
            events.append(((2 * k + a + 1) * 3.0 / (nz - 1), 0, k, a))
    events.sort()
    weights_left = 2 * (nfs - 1)
    ready = [0]

    def settle(s):
        for a in range(2):
            mate_copy[s, a].wait_recv()
        hidden_block(s)
        if s < nz - 1:
            dx_block(s)

    for _, kind, k, a in events:
        if kind == 1:
            for c in w_copy[k, a]:
                c.wait_recv()
            if k + 1 < nfs - 1:
                w_copy[k + 1, a] = w_send(k + 1, a)
            weights_left -= 1
        else:
            for c in z_copy[k, a]:
                c.wait_recv()
            if k + 1 < nz - 1:
                z_copy[k + 1, a] = z_send(k + 1, a)
            mate_copy[k + 1, a] = mate_send(k + 1, a)
            if a == 1:
                ready.append(k + 1)
        if weights_left == 0 and (kind, k) != (0, nz - 2):
            for s in ready:
                settle(s)
            ready = []
    for s in ready[:-1]:
        settle(s)
    x_step(0)
    settle(ready[-1])

    def up_term(r):
        o = ring_index((pos + nfs - r - 1) % nfs)
        return dot(tok[:, cols(o)], dpre[...], 0, 0)

    def down_term(r):
        o = ring_index((pos + r + 1) % nfs)
        return dot(hid[...], cot[:, cols(o)], 0, 0)

    g_copy = {}

    def g_send(r, half, which):
        n, m = dl // 2, fl // 2
        a, b = pl.ds(half * n, n), pl.ds(half * m, m)
        if which == 0:
            g_copy[r, half, 0] = remote(
                ug_send.at[r, a], ug_recv.at[r, a], gs.at[r, half, 0], gr.at[r, half, 0], cw
            )
        else:
            g_copy[r, half, 1] = remote(
                dg_send.at[r, b], dg_recv.at[r, b], gs.at[r, half, 1], gr.at[r, half, 1], ccw
            )

    def g_terms(r):
        ug_own[...] = up_term(r)
        dg_own[...] = down_term(r)

    def g_first():
        ug_send[0] = up_term(0).astype(BF16)
        for half in range(2):
            g_send(0, half, 0)
        dg_send[0] = down_term(0).astype(BF16)
        for half in range(2):
            g_send(0, half, 1)
        g_terms(1)

    def g_step(r, half):
        n, m = dl // 2, fl // 2
        a, b = pl.ds(half * n, n), pl.ds(half * m, m)
        g_copy[r - 1, half, 0].wait_recv()
        gu = ug_own[a, :] + ug_recv[r - 1, a, :].astype(F32)
        if r < nfs - 1:
            ug_send[r, a, :] = gu.astype(BF16)
            g_send(r, half, 0)
        else:
            ug_out[a, :] = gu * factor
        g_copy[r - 1, half, 1].wait_recv()
        gd = dg_own[b, :] + dg_recv[r - 1, b, :].astype(F32)
        if r < nfs - 1:
            dg_send[r, b, :] = gd.astype(BF16)
            g_send(r, half, 1)
        else:
            dg_out[b, :] = gd * factor

    g_first()
    dx_block(nz - 1)
    for r in range(1, max(nfs, nz)):
        if r < nfs:
            g_step(r, 0)
        if r < nz:
            x_step(r)
        if r < nfs:
            g_step(r, 1)
            if r < nfs - 1:
                g_terms(r + 1)
    for c in sends:
        c.wait_send()


def shards(nfs, ntp, tokens, up_weight, down_weight, cotangent):
    rows, width = tokens.shape
    dl, fl = up_weight.shape
    nz = ntp // 2
    whole = rows * ntp
    factor = 1.0 / (whole * nfs) ** 0.5
    dma = pltpu.SemaphoreType.DMA
    any_space = pl.BlockSpec(memory_space=pl.ANY)
    vmem = pl.BlockSpec(memory_space=pltpu.VMEM)
    return pl.pallas_call(
        functools.partial(kernel, nfs, nz, factor),
        out_shape=(
            jax.ShapeDtypeStruct((rows, width), BF16),
            jax.ShapeDtypeStruct((dl, fl), F32),
            jax.ShapeDtypeStruct((fl, dl), F32),
        ),
        in_specs=[any_space] * 4,
        out_specs=(vmem, vmem, vmem),
        scratch_shapes=[
            pltpu.VMEM((whole, width), BF16),
            pltpu.VMEM((whole, width), BF16),
            pltpu.VMEM((width, fl), BF16),
            pltpu.VMEM((fl, width), BF16),
            pltpu.VMEM((whole, fl), BF16),
            pltpu.VMEM((whole, fl), BF16),
            pltpu.VMEM((nz, rows, width), F32),
            pltpu.VMEM((nz, rows, width), BF16),
            pltpu.VMEM((nz, rows, width), BF16),
            pltpu.VMEM((nz - 1, rows, width), BF16),
            pltpu.VMEM((nz - 1, rows, width), BF16),
            pltpu.VMEM((dl, fl), F32),
            pltpu.VMEM((fl, dl), F32),
            pltpu.VMEM((nfs - 1, dl, fl), BF16),
            pltpu.VMEM((nfs - 1, dl, fl), BF16),
            pltpu.VMEM((nfs - 1, fl, dl), BF16),
            pltpu.VMEM((nfs - 1, fl, dl), BF16),
            dma((4,)),
            dma((nz - 1, 2, 2)), dma((nz - 1, 2, 2)),
            dma((nz, 2)), dma((nz, 2)),
            dma((nfs - 1, 2, 2)), dma((nfs - 1, 2, 2)),
            dma((nfs - 1, 2, 2)), dma((nfs - 1, 2, 2)),
            dma((nz,)), dma((nz,)),
            dma((nz - 1, 2)), dma((nz - 1, 2)),
        ],
        compiler_params=pltpu.CompilerParams(
            collective_id=0, has_side_effects=True, vmem_limit_bytes=67_000_000
        ),
    )(tokens, up_weight, down_weight, cotangent)


def line_kernel(
    factor, give,
    tok_in, up_in, down_in, cot_in,
    dx_out, ug_out, dg_out,
    tok, cot, up, down, up_give, down_give, hid, dpre, ug_acc, dg_acc,
    ug_send, ug_recv, dg_send, dg_recv, ug_back, dg_back, ug_home, dg_home,
    ue_send, ue_recv, de_send, de_recv, dx_own, dxm_send, dxm_recv, dxz_send, dxz_recv,
    local_sem, exs, exr, wxs, wxr, wys, wyr, ts, tr, tms, tmr,
    ms, mr, dzs, dzr, gs, gr, bs, br,
):
    fs, tp = lax.axis_index("fs"), lax.axis_index("tp")
    rows, width = tok_in.shape
    dl, fl = up_in.shape
    unit, hr, hd = 2 * rows, rows // 2, dl // 2
    x, y, z, c = fs % 2, fs // 2, tp // 2, tp % 2
    high = z // 2
    toward = 1 - 2 * high
    at_end = z % 3 == 0
    fx_, fy_, fd_ = 2 * y + 1 - x, 2 * (1 - y) + x, 2 * (1 - y) + 1 - x
    mate = (fs, 2 * z + 1 - c)
    xn, yn = (fx_, tp), (fy_, tp)
    inner = (fs, 2 * (z + toward) + c)
    outer = (fs, 2 * jnp.maximum(z - toward, 0) + c)
    beyond = (fs, 2 * (z + 2 * toward) + c)
    Q = range(4)

    def cols(o):
        return pl.ds(pl.multiple_of(o * dl, dl), dl)

    bufs = (tok, cot)

    def rows_of(j, u, shift=0):
        return bufs[j % 2].at[pl.ds(u * unit + shift + (j // 2) * rows, hr)]

    def body(end):
        nf = fl - give if end else fl + give
        nown = fl - give if end else fl
        units = slice(0, nf)
        locals_ = [
            pltpu.make_async_copy(up_in.at[:, pl.ds(0, nown)], up.at[cols(fs), pl.ds(0, nown)], local_sem.at[0]),
            pltpu.make_async_copy(down_in.at[pl.ds(0, nown)], down.at[pl.ds(0, nown), cols(fs)], local_sem.at[1]),
        ]
        for j in Q:
            mine = pl.ds((j // 2) * hr, hr)
            locals_.append(pltpu.make_async_copy((tok_in, cot_in)[j % 2].at[mine], rows_of(j, 0), local_sem.at[2 + j]))
        if end:
            locals_ += [
                pltpu.make_async_copy(up_in.at[:, pl.ds(nown, give)], up_give, local_sem.at[6]),
                pltpu.make_async_copy(down_in.at[pl.ds(nown, give)], down_give, local_sem.at[7]),
            ]
        for cp in locals_:
            cp.start()
        barrier = pltpu.get_barrier_semaphore()
        peers = (mate, xn, yn, inner) if end else (mate, xn, yn, inner, outer)
        for peer in peers:
            pl.semaphore_signal(barrier, inc=1, device_id=peer, device_id_type=MESH)
        pl.semaphore_wait(barrier, len(peers))
        for cp in locals_:
            cp.wait()

        sends = []

        def remote(src, dst, s, r, peer):
            return pltpu.make_async_remote_copy(
                src_ref=src, dst_ref=dst, send_sem=s, recv_sem=r, device_id=peer, device_id_type=MESH
            )

        def go(cp):
            cp.start()
            sends.append(cp)

        def piece(o, q):
            if q < 2:
                return up.at[pl.ds(pl.multiple_of(o * dl + q * hd, hd), hd), pl.ds(0, nown)]
            if q < 4:
                return down.at[pl.ds((q - 2) * (nown // 2), nown // 2), cols(o)]
            if q == 4:
                return up.at[cols(o), pl.ds(fl, give)]
            return down.at[pl.ds(fl, give), cols(o)]

        pieces = Q if end else range(6)
        wx = [[remote(piece(o, q), piece(o, q), wxs.at[i, q], wxr.at[i, q], xn) for q in pieces]
              for i, o in enumerate((fs, fy_))]
        wy = [[remote(piece(o, q), piece(o, q), wys.at[i, q], wyr.at[i, q], yn) for q in pieces]
              for i, o in enumerate((fs, fx_))]

        def t_send(flow, j, u, v, peer):
            go(remote(rows_of(j, u), rows_of(j, v), ts.at[flow, j], tr.at[v, j], peer))

        def t_wait(u, j):
            remote(rows_of(j, u), rows_of(j, u), ts.at[0, j], tr.at[u, j], mate).wait_recv()

        tm = [[remote(rows_of(j, u), rows_of(j, u, hr), tms.at[u, j], tmr.at[u, j], mate) for j in Q]
              for u in range(4)]

        def w_got(q):
            wx[0][q].wait_recv()
            if q % 2 == 0:
                go(wy[1][q])
            wy[0][q].wait_recv()
            if q % 2:
                go(wx[1][q])

        ex = (remote(up_give, up.at[cols(fs), pl.ds(fl, give)], exs.at[0], exr.at[0], inner),
              remote(down_give, down.at[pl.ds(fl, give), cols(fs)], exs.at[1], exr.at[1], inner))

        def hidden_block(u, here=None):
            here = pl.ds(u * unit, unit) if here is None else here
            active = jnp.maximum(dot(tok[here, :], up[:, units], 1, 0), 0.0)
            hid[here, units] = (active * active).astype(BF16)
            dh = dot(cot[here, :], down[units, :], 1, 1)
            dpre[here, units] = (2.0 * active * dh).astype(BF16)

        dxm = [remote(dxm_send.at[u], dxm_recv.at[u], ms.at[u], mr.at[u], mate) for u in range(4)]

        def dx_block(u):
            here = pl.ds(u * unit, unit)

            def tile(j, carry):
                o = cols(j)
                part = dot(dpre[here, units], up[o, units], 1, 1)
                for h in range(2):
                    half = pl.ds(h * hr, hr)
                    dx_own[u, half, o] = part[2 * h * hr : (2 * h + 1) * hr]
                    dxm_send[u, half, o] = part[(2 * h + 1) * hr : (2 * h + 2) * hr].astype(BF16)
                return carry

            lax.fori_loop(0, 4, tile, 0)
            go(dxm[u])

        def dx_sum(u):
            dxm[u].wait_recv()
            return dx_own[u] + dxm_recv[u].astype(F32)

        def z_wait(slot):
            remote(dxz_send.at[0], dxz_recv.at[slot], dzs.at[0], dzr.at[slot], mate).wait_recv()
            return dxz_recv[slot].astype(F32)

        def z_send(i, value, slot, peer):
            dxz_send[i] = value.astype(BF16)
            go(remote(dxz_send.at[i], dxz_recv.at[slot], dzs.at[i], dzr.at[slot], peer))

        def ready(u):
            for j in Q:
                tm[u][j].wait_recv()
            hidden_block(u)

        if end:
            for cp in ex:
                go(cp)
            for q in Q:
                go(wx[0][q])
                go(wy[0][q])
            for j in Q:
                t_send(0, j, 0, 1, inner)
            for j in Q:
                go(tm[0][j])
            for j in Q:
                w_got(j)
                t_wait(1, j)
                go(tm[1][j])
            for q in Q:
                (wy if q % 2 else wx)[1][q ^ 1].wait_recv()
            ready(0)
            ready(1)
            dx_block(1)
            t_wait(2, 0)
            go(tm[2][0])
            z_send(0, dx_sum(1), 0, inner)
            for j in (1, 2, 3):
                t_wait(2, j)
                go(tm[2][j])
            ready(2)
            dx_block(2)
            t_wait(3, 0)
            go(tm[3][0])
            z_send(1, dx_sum(2), 1, inner)
        else:
            for q in Q:
                go(wx[0][q])
                go(wy[0][q])
            for j in Q:
                t_send(0, j, 0, 1, outer)
            for j in (0, 1):
                t_send(1, j, 0, 3, inner)
            for j in Q:
                go(tm[0][j])
            for i in range(2):
                ex[i].wait_recv()
                go(wx[0][4 + i])
                go(wy[0][4 + i])

            def from_end(j):
                t_wait(1, j)
                t_send(2, j, 1, 2, inner)
                go(tm[1][j])

            def from_middle(j):
                t_wait(3, j)
                go(tm[3][j])

            def from_far(j):
                t_wait(2, j)
                t_send(4, j, 2, 2, outer)
                go(tm[2][j])

            from_end(0)
            w_got(0)
            from_end(1)
            from_middle(0)
            from_middle(1)
            w_got(1)
            from_end(2)
            from_far(0)
            w_got(2)
            from_end(3)
            for j in (2, 3):
                t_send(1, j, 0, 3, inner)
            from_far(1)
            w_got(3)
            w_got(4)
            w_got(5)
            from_far(2)
            from_far(3)
            for j in (0, 1):
                t_send(3, j, 3, 3, outer)

            def half_sums(u):
                here = pl.ds(u * unit, unit)
                return (ug_acc, pl.ds(u * unit, unit), units), (ug_acc, pl.ds((u + 4) * unit, unit), units), here

            def products(here, o):
                return (dot(tok[here, cols(o)], up[cols(o), units], 1, 0),
                        dot(cot[here, cols(o)], down[units, cols(o)], 1, 1))

            for u in range(3):
                for j in Q:
                    tm[u][j].wait_recv()
                (ref, a, k), (_, b, _), here = half_sums(u)
                for i, o in enumerate((fs, fx_, fy_)):
                    pre, dh = products(here, o)
                    if i:
                        pre, dh = pre + ref[a, k], dh + ref[b, k]
                    ref[a, k] = pre
                    ref[b, k] = dh
            for q in pieces:
                (wy if q % 2 else wx)[1][q ^ 1].wait_recv()
            for u in range(3):
                (ref, a, k), (_, b, _), here = half_sums(u)
                pre, dh = products(here, fd_)
                active = jnp.maximum(pre + ref[a, k], 0.0)
                hid[here, units] = (active * active).astype(BF16)
                dpre[here, units] = (2.0 * active * (dh + ref[b, k])).astype(BF16)
            for j in (2, 3):
                from_middle(j)
                t_send(3, j, 3, 3, outer)

        cut = 3 * unit + rows if end else 3 * unit
        early = pl.ds(0, cut)
        last = pl.ds(cut, 4 * unit - cut)

        def ug_early(o, carry):
            ug_acc[cols(o), units] = dot(tok[early, cols(o)], dpre[early, units], 0, 0)
            return carry

        def dg_early(o, carry):
            dg_acc[units, cols(o)] = dot(hid[early, units], cot[early, cols(o)], 0, 0)
            return carry

        if end:
            t_wait(3, 1)
            go(tm[3][1])
            dx_block(0)
            for j in (0, 1):
                tm[3][j].wait_recv()
            hidden_block(3, pl.ds(3 * unit, rows))
            lax.fori_loop(0, 4, ug_early, 0)
            t_wait(3, 2)
            go(tm[3][2])
            lax.fori_loop(0, 4, dg_early, 0)
            t_wait(3, 3)
            go(tm[3][3])
            for j in (2, 3):
                tm[3][j].wait_recv()
            hidden_block(3, last)
        else:
            ug_early(fd_, 0)
            dg_early(fd_, 0)
            ready(3)
        before = len(sends)

        gh = nown // 2

        def buf(bufs, k, q):
            if q < 2:
                return bufs[0].at[k, q, :, pl.ds(0, nown)]
            if q < 4:
                return bufs[1].at[k, q - 2, pl.ds(0, gh)]
            return bufs[q - 2].at[k]

        out_bufs, in_bufs = (ug_send, dg_send, ue_send, de_send), (ug_recv, dg_recv, ue_recv, de_recv)

        def g_copy(k, q):
            over_x = k == 1 or (k == 0 and q % 2 == 0)
            return remote(buf(out_bufs, k, q), buf(in_bufs, k, q), gs.at[k, q], gr.at[k, q], xn if over_x else yn)

        g = [[g_copy(k, q) for q in pieces] for k in range(3)]

        def acc_of(o, q):
            if q < 2:
                return ug_acc, pl.ds(pl.multiple_of(o * dl + q * hd, hd), hd), slice(0, nown)
            if q < 4:
                return dg_acc, pl.ds((q - 2) * gh, gh), cols(o)
            if q == 4:
                return ug_acc, cols(o), slice(nown, nf)
            return dg_acc, slice(nown, nf), cols(o)

        def g_put(k, q, value):
            dst = buf(out_bufs, k, q)
            dst[...] = value.astype(BF16)
            go(g[k][q])

        def terms(o, p):
            split = end or o is fd_
            part = last if split else slice(None)
            few = slice(nown, nf) if p > 1 else slice(0, nown)
            if p % 2 == 0:
                val = dot(tok[part, cols(o)], dpre[part, few], 0, 0)
                if split:
                    val = val + ug_acc[cols(o), few]
                return (val,) if p > 1 else (val[:hd], val[hd:])
            val = dot(hid[part, few], cot[part, cols(o)], 0, 0)
            if split:
                val = val + dg_acc[few, cols(o)]
            return (val,) if p > 1 else (val[:gh], val[gh:])

        def keep(o, q, value):
            ref, a, b = acc_of(o, q)
            ref[a, b] = value

        def begin(p):
            q = 2 * p if p < 2 else p + 2
            for h, v in enumerate(terms(fd_, p)):
                g_put(0, q + h, v)

        def follow(p):
            q = 2 * p if p < 2 else p + 2
            for h, v in enumerate(terms(fx_, p)):
                if (q + h) % 2 == 0:
                    g_put(1, q + h, v)
                else:
                    keep(fx_, q + h, v)
            for h, v in enumerate(terms(fy_, p)):
                if (q + h) % 2:
                    g_put(2, q + h, v)
                else:
                    keep(fy_, q + h, v)

        def own_terms(p):
            q = 2 * p if p < 2 else p + 2
            for h, v in enumerate(terms(fs, p)):
                keep(fs, q + h, v)

        def pass_on(q):
            g[0][q].wait_recv()
            k, o = (1, fx_) if q % 2 else (2, fy_)
            ref, a, b = acc_of(o, q)
            g_put(k, q, ref[a, b] + buf(in_bufs, 0, q)[...].astype(F32))

        back = (remote(ug_back, ug_home, bs.at[0], br.at[0], outer),
                remote(dg_back, dg_home, bs.at[1], br.at[1], outer))

        def summed(q):
            ref, a, b = acc_of(fs, q)
            total = ref[a, b]
            for k in (1, 2):
                g[k][q].wait_recv()
                total = total + buf(in_bufs, k, q)[...].astype(F32)
            return total

        def finish(q):
            if q < 2:
                ug_out[pl.ds(q * hd, hd), pl.ds(0, nown)] = summed(q) * factor
            else:
                dg_out[pl.ds((q - 2) * gh, gh), :] = summed(q) * factor

        if end:
            begin(0)
            begin(1)
            follow(0)
            follow(1)
            dx_block(3)
            pass_on(0)
            pass_on(1)
            own_terms(0)
            own_terms(1)
            pass_on(2)
            pass_on(3)
            z_send(2, dx_sum(3), 4, beyond)
            for cp in sends[:before]:
                cp.wait_send()
            dx_out[...] = (dx_sum(0) + z_wait(0)).astype(BF16)
            back[0].wait_recv()
            ug_out[:, pl.ds(nown, give)] = ug_home[...].astype(F32) * factor
            back[1].wait_recv()
            dg_out[pl.ds(nown, give), :] = dg_home[...].astype(F32) * factor
        else:
            begin(2)
            begin(3)
            follow(2)
            follow(3)
            dx_block(3)
            begin(0)
            begin(1)
            z_send(0, dx_sum(3), 2, inner)
            pass_on(4)
            pass_on(5)
            follow(0)
            follow(1)
            dx_block(2)
            own_terms(2)
            own_terms(3)
            pass_on(0)
            pass_on(1)
            z_send(1, dx_sum(2) + z_wait(1), 3, inner)
            own_terms(0)
            own_terms(1)
            pass_on(2)
            pass_on(3)
            dx_block(1)
            dx_block(0)
            ug_back[...] = summed(4).astype(BF16)
            dg_back[...] = summed(5).astype(BF16)
            for cp in sends[:before]:
                cp.wait_send()
            go(back[0])
            go(back[1])
            z_send(2, dx_sum(1) + z_wait(3), 0, outer)
        for q in Q:
            finish(q)
        if not end:
            near = dx_sum(0) + z_wait(0) + z_wait(2)
            dx_out[...] = (near + z_wait(4)).astype(BF16)
        del sends[:before]
        for cp in sends:
            cp.wait_send()

    pl.when(at_end)(lambda: body(True))
    pl.when(jnp.logical_not(at_end))(lambda: body(False))


def put_out(n, *refs):
    copies = [pltpu.make_async_copy(refs[i], refs[n + i], refs[2 * n].at[i]) for i in range(n)]
    for cp in copies:
        cp.start()
    for cp in copies:
        cp.wait()


def line_shards(nfs, ntp, tokens, up_weight, down_weight, cotangent):
    rows, width = tokens.shape
    dl, fl = up_weight.shape
    factor = 1.0 / (rows * ntp * nfs) ** 0.5
    mine = ntp * rows
    give = fl // 4
    most = fl + give
    hd = dl // 2
    dma = pltpu.SemaphoreType.DMA
    any_space = pl.BlockSpec(memory_space=pl.ANY)
    vmem = pl.BlockSpec(memory_space=pltpu.VMEM)
    V = pltpu.VMEM
    results = pl.pallas_call(
        functools.partial(line_kernel, factor, give),
        out_shape=(V((rows, width), BF16), V((dl, fl), F32), V((fl, dl), F32)),
        in_specs=[any_space] * 4,
        out_specs=(vmem, vmem, vmem),
        scratch_shapes=[
            V((mine, width), BF16), V((mine, width), BF16),
            V((width, most), BF16), V((most, width), BF16),
            V((dl, give), BF16), V((give, dl), BF16),
            V((mine, most), BF16), V((mine, most), BF16),
            V((width, most), F32), V((most, width), F32),
            V((3, 2, hd, fl), BF16), V((3, 2, hd, fl), BF16),
            V((3, 2, fl // 2, dl), BF16), V((3, 2, fl // 2, dl), BF16),
            V((dl, give), BF16), V((give, dl), BF16), V((dl, give), BF16), V((give, dl), BF16),
            V((3, dl, give), BF16), V((3, dl, give), BF16), V((3, give, dl), BF16), V((3, give, dl), BF16),
            V((4, rows, width), F32), V((4, rows, width), BF16), V((4, rows, width), BF16),
            V((3, rows, width), BF16), V((5, rows, width), BF16),
            dma((8,)), dma((2,)), dma((2,)), dma((2, 6)), dma((2, 6)), dma((2, 6)), dma((2, 6)),
            dma((5, 4)), dma((4, 4)), dma((4, 4)), dma((4, 4)),
            dma((4,)), dma((4,)), dma((3,)), dma((5,)), dma((3, 6)), dma((3, 6)), dma((2,)), dma((2,)),
        ],
        compiler_params=pltpu.CompilerParams(
            collective_id=0, has_side_effects=True, vmem_limit_bytes=60_000_000
        ),
    )(tokens, up_weight, down_weight, cotangent)
    return pl.pallas_call(
        functools.partial(put_out, len(results)),
        out_shape=tuple(jax.ShapeDtypeStruct(r.shape, r.dtype) for r in results),
        in_specs=[vmem] * len(results),
        out_specs=(any_space,) * len(results),
        scratch_shapes=[dma((3,))],
        compiler_params=pltpu.CompilerParams(vmem_limit_bytes=8_000_000),
    )(*results)


def solution(mesh):
    placed = (P(("fs", "tp"), None), P("fs", "tp"), P("tp", "fs"), P(("fs", "tp"), None))
    fs, tp = mesh.shape["fs"], mesh.shape["tp"]
    body = line_shards if (fs, tp) == (4, 8) else shards
    return jax.shard_map(
        functools.partial(body, mesh.shape["fs"], mesh.shape["tp"]),
        mesh=mesh,
        in_specs=placed,
        out_specs=(P(("fs", "tp"), None), P("fs", "tp"), P("tp", "fs")),
        check_vma=False,
    )
```

```python
import functools

import jax
import jax.numpy as jnp
from jax import lax
from jax.experimental import pallas as pl
from jax.experimental.pallas import tpu as pltpu
from jax.sharding import PartitionSpec as P

MESH = pl.DeviceIdType.MESH
BF16 = jnp.bfloat16
F32 = jnp.float32


def ring_index(p):
    q, b = p // 2, p % 2
    return 2 * q + b + (q % 2) * (1 - 2 * b)


def dot(a, b, ca, cb):
    return lax.dot_general(a, b, (((ca,), (cb,)), ((), ())), preferred_element_type=F32)


def kernel(
    nfs, nz, factor,
    tok_in, up_in, down_in, cot_in,
    dx_out, ug_out, dg_out,
    tok, cot, up, down, hid, dpre,
    dx_own, dx_send, dx_recv, dr_send, dr_recv,
    ug_own, dg_own, ug_send, ug_recv, dg_send, dg_recv,
    local_sem, zs, zr, ps, pr, ws, wr, gs, gr, xs, xr, rs, rr,
):
    fs, tp = lax.axis_index("fs"), lax.axis_index("tp")
    rows, width = tok_in.shape
    h = rows // 2
    block = 4 * h
    dl = up_in.shape[0]
    fl = up_in.shape[1]
    z, core = tp // 2, tp % 2
    pos = ring_index(fs)
    fwd = (fs, ((z + 1) % nz) * 2 + core)
    bwd = (fs, ((z + nz - 1) % nz) * 2 + core)
    mate = (fs, 2 * z + 1 - core)
    cw = (ring_index((pos + 1) % nfs), tp)
    ccw = (ring_index((pos + nfs - 1) % nfs), tp)

    def cols(o):
        return pl.ds(pl.multiple_of(o * dl, dl), dl)

    locals_ = [
        pltpu.make_async_copy(tok_in, tok.at[pl.ds(0, rows)], local_sem.at[0]),
        pltpu.make_async_copy(up_in, up.at[cols(fs)], local_sem.at[1]),
        pltpu.make_async_copy(down_in, down.at[:, cols(fs)], local_sem.at[2]),
        pltpu.make_async_copy(cot_in, cot.at[pl.ds(0, rows)], local_sem.at[3]),
    ]
    for c in locals_:
        c.start()
    barrier = pltpu.get_barrier_semaphore()
    peers = (fwd, bwd, mate, cw, ccw)
    for peer in peers:
        pl.semaphore_signal(barrier, inc=1, device_id=peer, device_id_type=MESH)
    pl.semaphore_wait(barrier, len(peers))
    for c in locals_:
        c.wait()

    sends = []

    def remote(src, dst, s, r, peer):
        c = pltpu.make_async_remote_copy(
            src_ref=src, dst_ref=dst, send_sem=s, recv_sem=r, device_id=peer, device_id_type=MESH
        )
        c.start()
        sends.append(c)
        return c

    bufs = (tok, cot)

    def z_send(k, a):
        out = []
        for d, peer in enumerate((fwd, bwd)):
            out.append(remote(
                bufs[a].at[pl.ds(k * block + d * h, h)],
                bufs[a].at[pl.ds((k + 1) * block + d * h, h)],
                zs.at[k, d, a], zr.at[k, d, a], peer,
            ))
        return out

    def mate_send(k, a):
        return remote(
            bufs[a].at[pl.ds(k * block, 2 * h)],
            bufs[a].at[pl.ds(k * block + 2 * h, 2 * h)],
            ps.at[k, a], pr.at[k, a], mate,
        )

    def w_send(k, half):
        a = ring_index((pos + nfs - k) % nfs)
        b = ring_index((pos + k) % nfs)
        n = dl // 2
        piece = up.at[pl.ds(pl.multiple_of(a * dl + half * n, n), n)]
        m = fl // 2
        other = down.at[pl.ds(half * m, m), cols(b)]
        return [
            remote(piece, piece, ws.at[k, half, 0], wr.at[k, half, 0], cw),
            remote(other, other, ws.at[k, half, 1], wr.at[k, half, 1], ccw),
        ]

    z_copy, w_copy, mate_copy = {}, {}, {}
    for a in range(2):
        z_copy[0, a] = z_send(0, a)
        w_copy[0, a] = w_send(0, a)
    for a in range(2):
        mate_copy[0, a] = mate_send(0, a)

    def hidden_block(s):
        here = pl.ds(s * block, block)
        active = jnp.maximum(dot(tok[here, :], up[...], 1, 0), 0.0)
        hid[here, :] = (active * active).astype(BF16)
        dh = dot(cot[here, :], down[...], 1, 1)
        dpre[here, :] = (2.0 * active * dh).astype(BF16)

    pair_copy = {}

    def dx_block(s):
        here = pl.ds(s * block, block)

        def tile(j, carry):
            c = cols(j)
            part = dot(dpre[here, :], up[c, :], 1, 1)
            dx_own[s, :, c] = part[: 2 * h]
            dx_send[s, :, c] = part[2 * h :].astype(BF16)
            return carry

        lax.fori_loop(0, nfs, tile, 0)
        pair_copy[s] = remote(dx_send.at[s], dx_recv.at[s], xs.at[s], xr.at[s], mate)

    x_copy = {}

    def x_step(r):
        s = r + 1 if r < nz - 1 else 0
        pair_copy[s].wait_recv()
        for d, peer in enumerate((fwd, bwd)):
            here = pl.ds(d * h, h)
            if r > 0:
                x_copy[r - 1, d].wait_recv()
            total = dx_own[s, here, :] + dx_recv[s, here, :].astype(F32)
            if r > 0:
                total = total + dr_recv[r - 1, here, :].astype(F32)
            if r < nz - 1:
                dr_send[r, here, :] = total.astype(BF16)
                x_copy[r, d] = remote(
                    dr_send.at[r, here], dr_recv.at[r, here], rs.at[r, d], rr.at[r, d], peer
                )
            else:
                dx_out[here, :] = total.astype(BF16)

    events = []
    for k in range(nfs - 1):
        for half in range(2):
            events.append(((2 * k + half + 1) * 1.5 / (nfs - 1), 1, k, half))
    for k in range(nz - 1):
        for a in range(2):
            events.append(((2 * k + a + 1) * 3.0 / (nz - 1), 0, k, a))
    events.sort()
    weights_left = 2 * (nfs - 1)
    ready = [0]

    def settle(s):
        for a in range(2):
            mate_copy[s, a].wait_recv()
        hidden_block(s)
        if s < nz - 1:
            dx_block(s)

    for _, kind, k, a in events:
        if kind == 1:
            for c in w_copy[k, a]:
                c.wait_recv()
            if k + 1 < nfs - 1:
                w_copy[k + 1, a] = w_send(k + 1, a)
            weights_left -= 1
        else:
            for c in z_copy[k, a]:
                c.wait_recv()
            if k + 1 < nz - 1:
                z_copy[k + 1, a] = z_send(k + 1, a)
            mate_copy[k + 1, a] = mate_send(k + 1, a)
            if a == 1:
                ready.append(k + 1)
        if weights_left == 0 and (kind, k) != (0, nz - 2):
            for s in ready:
                settle(s)
            ready = []
    for s in ready[:-1]:
        settle(s)
    x_step(0)
    settle(ready[-1])

    def up_term(r):
        o = ring_index((pos + nfs - r - 1) % nfs)
        return dot(tok[:, cols(o)], dpre[...], 0, 0)

    def down_term(r):
        o = ring_index((pos + r + 1) % nfs)
        return dot(hid[...], cot[:, cols(o)], 0, 0)

    g_copy = {}

    def g_send(r, half, which):
        n, m = dl // 2, fl // 2
        a, b = pl.ds(half * n, n), pl.ds(half * m, m)
        if which == 0:
            g_copy[r, half, 0] = remote(
                ug_send.at[r, a], ug_recv.at[r, a], gs.at[r, half, 0], gr.at[r, half, 0], cw
            )
        else:
            g_copy[r, half, 1] = remote(
                dg_send.at[r, b], dg_recv.at[r, b], gs.at[r, half, 1], gr.at[r, half, 1], ccw
            )

    def g_terms(r):
        ug_own[...] = up_term(r)
        dg_own[...] = down_term(r)

    def g_first():
        ug_send[0] = up_term(0).astype(BF16)
        for half in range(2):
            g_send(0, half, 0)
        dg_send[0] = down_term(0).astype(BF16)
        for half in range(2):
            g_send(0, half, 1)
        g_terms(1)

    def g_step(r, half):
        n, m = dl // 2, fl // 2
        a, b = pl.ds(half * n, n), pl.ds(half * m, m)
        g_copy[r - 1, half, 0].wait_recv()
        gu = ug_own[a, :] + ug_recv[r - 1, a, :].astype(F32)
        if r < nfs - 1:
            ug_send[r, a, :] = gu.astype(BF16)
            g_send(r, half, 0)
        else:
            ug_out[a, :] = gu * factor
        g_copy[r - 1, half, 1].wait_recv()
        gd = dg_own[b, :] + dg_recv[r - 1, b, :].astype(F32)
        if r < nfs - 1:
            dg_send[r, b, :] = gd.astype(BF16)
            g_send(r, half, 1)
        else:
            dg_out[b, :] = gd * factor

    g_first()
    dx_block(nz - 1)
    for r in range(1, max(nfs, nz)):
        if r < nfs:
            g_step(r, 0)
        if r < nz:
            x_step(r)
        if r < nfs:
            g_step(r, 1)
            if r < nfs - 1:
                g_terms(r + 1)
    for c in sends:
        c.wait_send()


def shards(nfs, ntp, tokens, up_weight, down_weight, cotangent):
    rows, width = tokens.shape
    dl, fl = up_weight.shape
    nz = ntp // 2
    whole = rows * ntp
    factor = 1.0 / (whole * nfs) ** 0.5
    dma = pltpu.SemaphoreType.DMA
    any_space = pl.BlockSpec(memory_space=pl.ANY)
    vmem = pl.BlockSpec(memory_space=pltpu.VMEM)
    return pl.pallas_call(
        functools.partial(kernel, nfs, nz, factor),
        out_shape=(
            jax.ShapeDtypeStruct((rows, width), BF16),
            jax.ShapeDtypeStruct((dl, fl), F32),
            jax.ShapeDtypeStruct((fl, dl), F32),
        ),
        in_specs=[any_space] * 4,
        out_specs=(vmem, vmem, vmem),
        scratch_shapes=[
            pltpu.VMEM((whole, width), BF16),
            pltpu.VMEM((whole, width), BF16),
            pltpu.VMEM((width, fl), BF16),
            pltpu.VMEM((fl, width), BF16),
            pltpu.VMEM((whole, fl), BF16),
            pltpu.VMEM((whole, fl), BF16),
            pltpu.VMEM((nz, rows, width), F32),
            pltpu.VMEM((nz, rows, width), BF16),
            pltpu.VMEM((nz, rows, width), BF16),
            pltpu.VMEM((nz - 1, rows, width), BF16),
            pltpu.VMEM((nz - 1, rows, width), BF16),
            pltpu.VMEM((dl, fl), F32),
            pltpu.VMEM((fl, dl), F32),
            pltpu.VMEM((nfs - 1, dl, fl), BF16),
            pltpu.VMEM((nfs - 1, dl, fl), BF16),
            pltpu.VMEM((nfs - 1, fl, dl), BF16),
            pltpu.VMEM((nfs - 1, fl, dl), BF16),
            dma((4,)),
            dma((nz - 1, 2, 2)), dma((nz - 1, 2, 2)),
            dma((nz, 2)), dma((nz, 2)),
            dma((nfs - 1, 2, 2)), dma((nfs - 1, 2, 2)),
            dma((nfs - 1, 2, 2)), dma((nfs - 1, 2, 2)),
            dma((nz,)), dma((nz,)),
            dma((nz - 1, 2)), dma((nz - 1, 2)),
        ],
        compiler_params=pltpu.CompilerParams(
            collective_id=0, has_side_effects=True, vmem_limit_bytes=67_000_000
        ),
    )(tokens, up_weight, down_weight, cotangent)


def line_kernel(
    factor, give,
    tok_in, up_in, down_in, cot_in,
    dx_out, ug_out, dg_out,
    tok, cot, up, down, up_give, down_give, hid, dpre, ug_acc, dg_acc,
    ug_send, ug_recv, dg_send, dg_recv, ug_back, dg_back, ug_home, dg_home,
    ue_send, ue_recv, de_send, de_recv, dx_own, dxm_send, dxm_recv, dxz_send, dxz_recv,
    local_sem, exs, exr, wxs, wxr, wys, wyr, ts, tr, tms, tmr,
    ms, mr, dzs, dzr, gs, gr, bs, br,
):
    fs, tp = lax.axis_index("fs"), lax.axis_index("tp")
    rows, width = tok_in.shape
    dl, fl = up_in.shape
    unit, hr, hd = 2 * rows, rows // 2, dl // 2
    x, y, z, c = fs % 2, fs // 2, tp // 2, tp % 2
    high = z // 2
    toward = 1 - 2 * high
    at_end = z % 3 == 0
    fx_, fy_, fd_ = 2 * y + 1 - x, 2 * (1 - y) + x, 2 * (1 - y) + 1 - x
    mate = (fs, 2 * z + 1 - c)
    xn, yn = (fx_, tp), (fy_, tp)
    inner = (fs, 2 * (z + toward) + c)
    outer = (fs, 2 * jnp.maximum(z - toward, 0) + c)
    beyond = (fs, 2 * (z + 2 * toward) + c)
    Q = range(4)

    def cols(o):
        return pl.ds(pl.multiple_of(o * dl, dl), dl)

    bufs = (tok, cot)

    def rows_of(j, u, shift=0):
        return bufs[j % 2].at[pl.ds(u * unit + shift + (j // 2) * rows, hr)]

    def body(end):
        nf = fl - give if end else fl + give
        nown = fl - give if end else fl
        units = slice(0, nf)
        locals_ = [
            pltpu.make_async_copy(up_in.at[:, pl.ds(0, nown)], up.at[cols(fs), pl.ds(0, nown)], local_sem.at[0]),
            pltpu.make_async_copy(down_in.at[pl.ds(0, nown)], down.at[pl.ds(0, nown), cols(fs)], local_sem.at[1]),
        ]
        for j in Q:
            mine = pl.ds((j // 2) * hr, hr)
            locals_.append(pltpu.make_async_copy((tok_in, cot_in)[j % 2].at[mine], rows_of(j, 0), local_sem.at[2 + j]))
        if end:
            locals_ += [
                pltpu.make_async_copy(up_in.at[:, pl.ds(nown, give)], up_give, local_sem.at[6]),
                pltpu.make_async_copy(down_in.at[pl.ds(nown, give)], down_give, local_sem.at[7]),
            ]
        for cp in locals_:
            cp.start()
        barrier = pltpu.get_barrier_semaphore()
        peers = (mate, xn, yn, inner) if end else (mate, xn, yn, inner, outer)
        for peer in peers:
            pl.semaphore_signal(barrier, inc=1, device_id=peer, device_id_type=MESH)
        pl.semaphore_wait(barrier, len(peers))
        for cp in locals_:
            cp.wait()

        def remote(src, dst, s, r, peer):
            return pltpu.make_async_remote_copy(
                src_ref=src, dst_ref=dst, send_sem=s, recv_sem=r, device_id=peer, device_id_type=MESH
            )

        def go(cp):
            cp.start()

        def sent(ref, sem):
            remote(ref, ref, sem, sem, mate).wait_send()

        def size(elements):
            return tok.at[pl.ds(0, elements // width)]

        def piece(o, q):
            if q < 2:
                return up.at[pl.ds(pl.multiple_of(o * dl + q * hd, hd), hd), pl.ds(0, nown)]
            if q < 4:
                return down.at[pl.ds((q - 2) * (nown // 2), nown // 2), cols(o)]
            if q == 4:
                return up.at[cols(o), pl.ds(fl, give)]
            return down.at[pl.ds(fl, give), cols(o)]

        pieces = Q if end else range(6)
        wx = [[remote(piece(o, q), piece(o, q), wxs.at[0], wxr.at[i, q], xn) for q in pieces]
              for i, o in enumerate((fs, fy_))]
        wy = [[remote(piece(o, q), piece(o, q), wys.at[0], wyr.at[i, q], yn) for q in pieces]
              for i, o in enumerate((fs, fx_))]

        def t_send(flow, j, u, v, peer):
            go(remote(rows_of(j, u), rows_of(j, v), ts.at[flow], tr.at[v, j], peer))

        def t_wait(u, j):
            remote(rows_of(j, u), rows_of(j, u), ts.at[0], tr.at[u, j], mate).wait_recv()

        def mate_slot(u, j):
            return 2 * u + j // 2 + (end and u == 3 and j == 3)

        tm = [[remote(rows_of(j, u), rows_of(j, u, hr), tms.at[0], tmr.at[mate_slot(u, j)], mate) for j in Q]
              for u in range(4)]

        def from_mate(u, h):
            got = pl.ds(u * unit, hr if end and u == 3 and h else rows)
            remote(tok.at[got], tok.at[got], tms.at[0], tmr.at[2 * u + h], mate).wait_recv()

        def w_got(q):
            wx[0][q].wait_recv()
            if q % 2 == 0:
                go(wy[1][q])
            wy[0][q].wait_recv()
            if q % 2:
                go(wx[1][q])

        ex = (remote(up_give, up.at[cols(fs), pl.ds(fl, give)], exs.at[0], exr.at[0], inner),
              remote(down_give, down.at[pl.ds(fl, give), cols(fs)], exs.at[1], exr.at[1], inner))

        def hidden_block(u, here=None):
            here = pl.ds(u * unit, unit) if here is None else here
            active = jnp.maximum(dot(tok[here, :], up[:, units], 1, 0), 0.0)
            hid[here, units] = (active * active).astype(BF16)
            dh = dot(cot[here, :], down[units, :], 1, 1)
            dpre[here, units] = (2.0 * active * dh).astype(BF16)

        dxm = [remote(dxm_send.at[u], dxm_recv.at[u], ms.at[0], mr.at[u], mate) for u in range(4)]

        def dx_block(u):
            here = pl.ds(u * unit, unit)

            def tile(j, carry):
                o = cols(j)
                part = dot(dpre[here, units], up[o, units], 1, 1)
                for h in range(2):
                    half = pl.ds(h * hr, hr)
                    dx_own[u, half, o] = part[2 * h * hr : (2 * h + 1) * hr]
                    dxm_send[u, half, o] = part[(2 * h + 1) * hr : (2 * h + 2) * hr].astype(BF16)
                return carry

            lax.fori_loop(0, 4, tile, 0)
            go(dxm[u])

        def dx_sum(u):
            dxm[u].wait_recv()
            return dx_own[u] + dxm_recv[u].astype(F32)

        def z_wait(slot):
            remote(dxz_send.at[0], dxz_recv.at[slot], dzs.at[0], dzr.at[slot], mate).wait_recv()
            return dxz_recv[slot].astype(F32)

        def z_send(i, value, slot, peer):
            dxz_send[i] = value.astype(BF16)
            go(remote(dxz_send.at[i], dxz_recv.at[slot], dzs.at[0], dzr.at[slot], peer))

        def ready(u):
            from_mate(u, 0)
            from_mate(u, 1)
            hidden_block(u)

        if end:
            for cp in ex:
                go(cp)
            for q in Q:
                go(wx[0][q])
                go(wy[0][q])
            for j in Q:
                t_send(0, j, 0, 1, inner)
            for j in Q:
                go(tm[0][j])
            for j in Q:
                w_got(j)
                t_wait(1, j)
                go(tm[1][j])
            for q in Q:
                (wy if q % 2 else wx)[1][q ^ 1].wait_recv()
            ready(0)
            ready(1)
            dx_block(1)
            t_wait(2, 0)
            go(tm[2][0])
            z_send(0, dx_sum(1), 0, inner)
            for j in (1, 2, 3):
                t_wait(2, j)
                go(tm[2][j])
            ready(2)
            dx_block(2)
            t_wait(3, 0)
            go(tm[3][0])
            z_send(1, dx_sum(2), 1, inner)
        else:
            for q in Q:
                go(wx[0][q])
                go(wy[0][q])
            for j in Q:
                t_send(0, j, 0, 1, outer)
            for j in (0, 1):
                t_send(1, j, 0, 3, inner)
            for j in Q:
                go(tm[0][j])
            for i in range(2):
                ex[i].wait_recv()
                go(wx[0][4 + i])
                go(wy[0][4 + i])

            def from_end(j):
                t_wait(1, j)
                t_send(2, j, 1, 2, inner)
                go(tm[1][j])

            def from_middle(j):
                t_wait(3, j)
                go(tm[3][j])

            def from_far(j):
                t_wait(2, j)
                t_send(4, j, 2, 2, outer)
                go(tm[2][j])

            from_end(0)
            w_got(0)
            from_end(1)
            from_middle(0)
            from_middle(1)
            w_got(1)
            from_end(2)
            from_far(0)
            w_got(2)
            from_end(3)
            for j in (2, 3):
                t_send(1, j, 0, 3, inner)
            from_far(1)
            w_got(3)
            w_got(4)
            w_got(5)
            from_far(2)
            from_far(3)
            for j in (0, 1):
                t_send(3, j, 3, 3, outer)

            def products(here, o):
                return (dot(tok[here, cols(o)], up[cols(o), units], 1, 0),
                        dot(cot[here, cols(o)], down[units, cols(o)], 1, 1))

            spans = [(u * unit, unit) for u in range(3)] + [(3 * unit, rows)]
            for u, (at, n) in enumerate(spans):
                here, there = pl.ds(at, n), pl.ds(4 * unit + at, n)
                from_mate(u, 0)
                if u < 3:
                    from_mate(u, 1)
                for i, o in enumerate((fs, fx_, fy_)):
                    pre, dh = products(here, o)
                    if i:
                        pre, dh = pre + ug_acc[here, units], dh + ug_acc[there, units]
                    ug_acc[here, units] = pre
                    ug_acc[there, units] = dh
            for q in pieces:
                (wy if q % 2 else wx)[1][q ^ 1].wait_recv()
            for at, n in spans:
                here, there = pl.ds(at, n), pl.ds(4 * unit + at, n)
                pre, dh = products(here, fd_)
                active = jnp.maximum(pre + ug_acc[here, units], 0.0)
                hid[here, units] = (active * active).astype(BF16)
                dpre[here, units] = (2.0 * active * (dh + ug_acc[there, units])).astype(BF16)
            for j in (2, 3):
                from_middle(j)
                t_send(3, j, 3, 3, outer)

        cut = 3 * unit + rows
        early = pl.ds(0, cut)
        last = pl.ds(cut, 4 * unit - cut)

        def ug_early(o, carry):
            ug_acc[cols(o), units] = dot(tok[early, cols(o)], dpre[early, units], 0, 0)
            return carry

        def dg_early(o, carry):
            dg_acc[units, cols(o)] = dot(hid[early, units], cot[early, cols(o)], 0, 0)
            return carry

        if end:
            t_wait(3, 1)
            go(tm[3][1])
            dx_block(0)
            from_mate(3, 0)
            hidden_block(3, pl.ds(3 * unit, rows))
            lax.fori_loop(0, 4, ug_early, 0)
            t_wait(3, 2)
            go(tm[3][2])
            lax.fori_loop(0, 4, dg_early, 0)
            from_mate(3, 1)
            spare = pl.ds(fl, rows)
            active = jnp.maximum(dot(tok[last, :], up[:, units], 1, 0), 0.0)
            hid[last, units] = (active * active).astype(BF16)
            dg_acc[spare, units] = active
            t_wait(3, 3)
            go(tm[3][3])
            from_mate(3, 2)
            dh = dot(cot[last, :], down[units, :], 1, 1)
            dpre[last, units] = (2.0 * dg_acc[spare, units] * dh).astype(BF16)
        else:
            ug_early(fd_, 0)
            dg_early(fd_, 0)
            from_mate(3, 1)
            hidden_block(3, last)

        def drain():
            w_bytes = (dl * nown * 2) * 3 // 2 + (0 if end else dl * give * 3)
            sent(size(w_bytes), wxs.at[0])
            sent(size(w_bytes), wys.at[0])
            for flow in range(1 if end else 5):
                sent(tok.at[pl.ds(0, unit)], ts.at[flow])
            sent(tok, tms.at[0])
            if end:
                for cp in ex:
                    cp.wait_send()

        gh = nown // 2

        def buf(bufs, k, q):
            if q < 2:
                return bufs[0].at[k, q, :, pl.ds(0, nown)]
            if q < 4:
                return bufs[1].at[k, q - 2, pl.ds(0, gh)]
            return bufs[q - 2].at[k]

        out_bufs, in_bufs = (ug_send, dg_send, ue_send, de_send), (ug_recv, dg_recv, ue_recv, de_recv)

        def g_copy(k, q):
            over_x = k == 1 or (k == 0 and q % 2 == 0)
            return remote(buf(out_bufs, k, q), buf(in_bufs, k, q), gs.at[0], gr.at[k, q], xn if over_x else yn)

        g = [[g_copy(k, q) for q in pieces] for k in range(3)]

        def acc_of(o, q):
            if q < 2:
                return ug_acc, pl.ds(pl.multiple_of(o * dl + q * hd, hd), hd), slice(0, nown)
            if q < 4:
                return dg_acc, pl.ds((q - 2) * gh, gh), cols(o)
            if q == 4:
                return ug_acc, cols(o), slice(nown, nf)
            return dg_acc, slice(nown, nf), cols(o)

        def g_put(k, q, value):
            dst = buf(out_bufs, k, q)
            dst[...] = value.astype(BF16)
            go(g[k][q])

        def terms(o, p):
            split = end or o is fd_
            part = last if split else slice(None)
            few = slice(nown, nf) if p > 1 else slice(0, nown)
            if p % 2 == 0:
                val = dot(tok[part, cols(o)], dpre[part, few], 0, 0)
                if split:
                    val = val + ug_acc[cols(o), few]
                return (val,) if p > 1 else (val[:hd], val[hd:])
            val = dot(hid[part, few], cot[part, cols(o)], 0, 0)
            if split:
                val = val + dg_acc[few, cols(o)]
            return (val,) if p > 1 else (val[:gh], val[gh:])

        def keep(o, q, value):
            ref, a, b = acc_of(o, q)
            ref[a, b] = value

        def begin(p):
            q = 2 * p if p < 2 else p + 2
            for h, v in enumerate(terms(fd_, p)):
                g_put(0, q + h, v)

        def follow(p):
            q = 2 * p if p < 2 else p + 2
            for h, v in enumerate(terms(fx_, p)):
                if (q + h) % 2 == 0:
                    g_put(1, q + h, v)
                else:
                    keep(fx_, q + h, v)
            for h, v in enumerate(terms(fy_, p)):
                if (q + h) % 2:
                    g_put(2, q + h, v)
                else:
                    keep(fy_, q + h, v)

        def own_terms(p):
            q = 2 * p if p < 2 else p + 2
            for h, v in enumerate(terms(fs, p)):
                keep(fs, q + h, v)

        def pass_on(q):
            g[0][q].wait_recv()
            k, o = (1, fx_) if q % 2 else (2, fy_)
            ref, a, b = acc_of(o, q)
            g_put(k, q, ref[a, b] + buf(in_bufs, 0, q)[...].astype(F32))

        back = (remote(ug_back, ug_home, bs.at[0], br.at[0], outer),
                remote(dg_back, dg_home, bs.at[1], br.at[1], outer))

        def summed(q):
            ref, a, b = acc_of(fs, q)
            total = ref[a, b]
            for k in (1, 2):
                g[k][q].wait_recv()
                total = total + buf(in_bufs, k, q)[...].astype(F32)
            return total

        def finish(q):
            if q < 2:
                ug_out[pl.ds(q * hd, hd), pl.ds(0, nown)] = summed(q) * factor
            else:
                dg_out[pl.ds((q - 2) * gh, gh), :] = summed(q) * factor

        if end:
            begin(0)
            begin(1)
            follow(0)
            follow(1)
            dx_block(3)
            pass_on(0)
            pass_on(1)
            own_terms(0)
            own_terms(1)
            pass_on(2)
            pass_on(3)
            z_send(2, dx_sum(3), 4, beyond)
            drain()
            dx_out[...] = (dx_sum(0) + z_wait(0)).astype(BF16)
            back[0].wait_recv()
            ug_out[:, pl.ds(nown, give)] = ug_home[...].astype(F32) * factor
            back[1].wait_recv()
            dg_out[pl.ds(nown, give), :] = dg_home[...].astype(F32) * factor
        else:
            begin(2)
            begin(3)
            follow(2)
            follow(3)
            dx_block(3)
            begin(0)
            begin(1)
            z_send(0, dx_sum(3), 2, inner)
            pass_on(4)
            pass_on(5)
            follow(0)
            follow(1)
            dx_block(2)
            own_terms(2)
            own_terms(3)
            pass_on(0)
            pass_on(1)
            z_send(1, dx_sum(2) + z_wait(1), 3, inner)
            own_terms(0)
            own_terms(1)
            pass_on(2)
            pass_on(3)
            dx_block(1)
            dx_block(0)
            ug_back[...] = summed(4).astype(BF16)
            dg_back[...] = summed(5).astype(BF16)
            drain()
            go(back[0])
            go(back[1])
            z_send(2, dx_sum(1) + z_wait(3), 0, outer)
        for q in Q:
            finish(q)
        if not end:
            near = dx_sum(0) + z_wait(0) + z_wait(2)
            dx_out[...] = (near + z_wait(4)).astype(BF16)
        g_bytes = 12 * hd * nown + (0 if end else 6 * dl * give)
        sent(size(g_bytes), gs.at[0])
        sent(dxm_send, ms.at[0])
        sent(dxz_send, dzs.at[0])
        if not end:
            for cp in back:
                cp.wait_send()

    pl.when(at_end)(lambda: body(True))
    pl.when(jnp.logical_not(at_end))(lambda: body(False))


def put_out(n, *refs):
    copies = [pltpu.make_async_copy(refs[i], refs[n + i], refs[2 * n].at[i]) for i in range(n)]
    for cp in copies:
        cp.start()
    for cp in copies:
        cp.wait()


def line_shards(nfs, ntp, tokens, up_weight, down_weight, cotangent):
    rows, width = tokens.shape
    dl, fl = up_weight.shape
    factor = 1.0 / (rows * ntp * nfs) ** 0.5
    mine = ntp * rows
    give = fl // 4
    most = fl + give
    hd = dl // 2
    dma = pltpu.SemaphoreType.DMA
    any_space = pl.BlockSpec(memory_space=pl.ANY)
    vmem = pl.BlockSpec(memory_space=pltpu.VMEM)
    V = pltpu.VMEM
    results = pl.pallas_call(
        functools.partial(line_kernel, factor, give),
        out_shape=(V((rows, width), BF16), V((dl, fl), F32), V((fl, dl), F32)),
        in_specs=[any_space] * 4,
        out_specs=(vmem, vmem, vmem),
        scratch_shapes=[
            V((mine, width), BF16), V((mine, width), BF16),
            V((width, most), BF16), V((most, width), BF16),
            V((dl, give), BF16), V((give, dl), BF16),
            V((mine, most), BF16), V((mine, most), BF16),
            V((width, most), F32), V((most, width), F32),
            V((3, 2, hd, fl), BF16), V((3, 2, hd, fl), BF16),
            V((3, 2, fl // 2, dl), BF16), V((3, 2, fl // 2, dl), BF16),
            V((dl, give), BF16), V((give, dl), BF16), V((dl, give), BF16), V((give, dl), BF16),
            V((3, dl, give), BF16), V((3, dl, give), BF16), V((3, give, dl), BF16), V((3, give, dl), BF16),
            V((4, rows, width), F32), V((4, rows, width), BF16), V((4, rows, width), BF16),
            V((3, rows, width), BF16), V((5, rows, width), BF16),
            dma((8,)), dma((2,)), dma((2,)), dma((1,)), dma((2, 6)), dma((1,)), dma((2, 6)),
            dma((5,)), dma((4, 4)), dma((1,)), dma((9,)),
            dma((1,)), dma((4,)), dma((1,)), dma((5,)), dma((1,)), dma((3, 6)), dma((2,)), dma((2,)),
        ],
        compiler_params=pltpu.CompilerParams(
            collective_id=0, has_side_effects=True, vmem_limit_bytes=60_000_000
        ),
    )(tokens, up_weight, down_weight, cotangent)
    return pl.pallas_call(
        functools.partial(put_out, len(results)),
        out_shape=tuple(jax.ShapeDtypeStruct(r.shape, r.dtype) for r in results),
        in_specs=[vmem] * len(results),
        out_specs=(any_space,) * len(results),
        scratch_shapes=[dma((3,))],
        compiler_params=pltpu.CompilerParams(vmem_limit_bytes=8_000_000),
    )(*results)


def solution(mesh):
    placed = (P(("fs", "tp"), None), P("fs", "tp"), P("tp", "fs"), P(("fs", "tp"), None))
    fs, tp = mesh.shape["fs"], mesh.shape["tp"]
    body = line_shards if (fs, tp) == (4, 8) else shards
    return jax.shard_map(
        functools.partial(body, mesh.shape["fs"], mesh.shape["tp"]),
        mesh=mesh,
        in_specs=placed,
        out_specs=(P(("fs", "tp"), None), P("fs", "tp"), P("tp", "fs")),
        check_vma=False,
    )
```

```python
import functools

import jax
import jax.numpy as jnp
from jax import lax
from jax.experimental import pallas as pl
from jax.experimental.pallas import tpu as pltpu
from jax.sharding import PartitionSpec as P

MESH = pl.DeviceIdType.MESH
BF16 = jnp.bfloat16
F32 = jnp.float32


def ring_index(p):
    q, b = p // 2, p % 2
    return 2 * q + b + (q % 2) * (1 - 2 * b)


def dot(a, b, ca, cb):
    return lax.dot_general(a, b, (((ca,), (cb,)), ((), ())), preferred_element_type=F32)


def kernel(
    nfs, nz, factor,
    tok_in, up_in, down_in, cot_in,
    dx_out, ug_out, dg_out,
    tok, cot, up, down, hid, dpre,
    dx_own, dx_send, dx_recv, dr_send, dr_recv,
    ug_own, dg_own, ug_send, ug_recv, dg_send, dg_recv,
    local_sem, zs, zr, ps, pr, ws, wr, gs, gr, xs, xr, rs, rr,
):
    fs, tp = lax.axis_index("fs"), lax.axis_index("tp")
    rows, width = tok_in.shape
    h = rows // 2
    block = 4 * h
    dl = up_in.shape[0]
    fl = up_in.shape[1]
    z, core = tp // 2, tp % 2
    pos = ring_index(fs)
    fwd = (fs, ((z + 1) % nz) * 2 + core)
    bwd = (fs, ((z + nz - 1) % nz) * 2 + core)
    mate = (fs, 2 * z + 1 - core)
    cw = (ring_index((pos + 1) % nfs), tp)
    ccw = (ring_index((pos + nfs - 1) % nfs), tp)

    def cols(o):
        return pl.ds(pl.multiple_of(o * dl, dl), dl)

    locals_ = [
        pltpu.make_async_copy(tok_in, tok.at[pl.ds(0, rows)], local_sem.at[0]),
        pltpu.make_async_copy(up_in, up.at[cols(fs)], local_sem.at[1]),
        pltpu.make_async_copy(down_in, down.at[:, cols(fs)], local_sem.at[2]),
        pltpu.make_async_copy(cot_in, cot.at[pl.ds(0, rows)], local_sem.at[3]),
    ]
    for c in locals_:
        c.start()
    barrier = pltpu.get_barrier_semaphore()
    peers = (fwd, bwd, mate, cw, ccw)
    for peer in peers:
        pl.semaphore_signal(barrier, inc=1, device_id=peer, device_id_type=MESH)
    pl.semaphore_wait(barrier, len(peers))
    for c in locals_:
        c.wait()

    sends = []

    def remote(src, dst, s, r, peer):
        c = pltpu.make_async_remote_copy(
            src_ref=src, dst_ref=dst, send_sem=s, recv_sem=r, device_id=peer, device_id_type=MESH
        )
        c.start()
        sends.append(c)
        return c

    bufs = (tok, cot)

    def z_send(k, a):
        out = []
        for d, peer in enumerate((fwd, bwd)):
            out.append(remote(
                bufs[a].at[pl.ds(k * block + d * h, h)],
                bufs[a].at[pl.ds((k + 1) * block + d * h, h)],
                zs.at[k, d, a], zr.at[k, d, a], peer,
            ))
        return out

    def mate_send(k, a):
        return remote(
            bufs[a].at[pl.ds(k * block, 2 * h)],
            bufs[a].at[pl.ds(k * block + 2 * h, 2 * h)],
            ps.at[k, a], pr.at[k, a], mate,
        )

    def w_send(k, half):
        a = ring_index((pos + nfs - k) % nfs)
        b = ring_index((pos + k) % nfs)
        n = dl // 2
        piece = up.at[pl.ds(pl.multiple_of(a * dl + half * n, n), n)]
        m = fl // 2
        other = down.at[pl.ds(half * m, m), cols(b)]
        return [
            remote(piece, piece, ws.at[k, half, 0], wr.at[k, half, 0], cw),
            remote(other, other, ws.at[k, half, 1], wr.at[k, half, 1], ccw),
        ]

    z_copy, w_copy, mate_copy = {}, {}, {}
    for a in range(2):
        z_copy[0, a] = z_send(0, a)
        w_copy[0, a] = w_send(0, a)
    for a in range(2):
        mate_copy[0, a] = mate_send(0, a)

    def hidden_block(s):
        here = pl.ds(s * block, block)
        active = jnp.maximum(dot(tok[here, :], up[...], 1, 0), 0.0)
        hid[here, :] = (active * active).astype(BF16)
        dh = dot(cot[here, :], down[...], 1, 1)
        dpre[here, :] = (2.0 * active * dh).astype(BF16)

    pair_copy = {}

    def dx_block(s):
        here = pl.ds(s * block, block)

        def tile(j, carry):
            c = cols(j)
            part = dot(dpre[here, :], up[c, :], 1, 1)
            dx_own[s, :, c] = part[: 2 * h]
            dx_send[s, :, c] = part[2 * h :].astype(BF16)
            return carry

        lax.fori_loop(0, nfs, tile, 0)
        pair_copy[s] = remote(dx_send.at[s], dx_recv.at[s], xs.at[s], xr.at[s], mate)

    x_copy = {}

    def x_step(r):
        s = r + 1 if r < nz - 1 else 0
        pair_copy[s].wait_recv()
        for d, peer in enumerate((fwd, bwd)):
            here = pl.ds(d * h, h)
            if r > 0:
                x_copy[r - 1, d].wait_recv()
            total = dx_own[s, here, :] + dx_recv[s, here, :].astype(F32)
            if r > 0:
                total = total + dr_recv[r - 1, here, :].astype(F32)
            if r < nz - 1:
                dr_send[r, here, :] = total.astype(BF16)
                x_copy[r, d] = remote(
                    dr_send.at[r, here], dr_recv.at[r, here], rs.at[r, d], rr.at[r, d], peer
                )
            else:
                dx_out[here, :] = total.astype(BF16)

    events = []
    for k in range(nfs - 1):
        for half in range(2):
            events.append(((2 * k + half + 1) * 1.5 / (nfs - 1), 1, k, half))
    for k in range(nz - 1):
        for a in range(2):
            events.append(((2 * k + a + 1) * 3.0 / (nz - 1), 0, k, a))
    events.sort()
    weights_left = 2 * (nfs - 1)
    ready = [0]

    def settle(s):
        for a in range(2):
            mate_copy[s, a].wait_recv()
        hidden_block(s)
        if s < nz - 1:
            dx_block(s)

    for _, kind, k, a in events:
        if kind == 1:
            for c in w_copy[k, a]:
                c.wait_recv()
            if k + 1 < nfs - 1:
                w_copy[k + 1, a] = w_send(k + 1, a)
            weights_left -= 1
        else:
            for c in z_copy[k, a]:
                c.wait_recv()
            if k + 1 < nz - 1:
                z_copy[k + 1, a] = z_send(k + 1, a)
            mate_copy[k + 1, a] = mate_send(k + 1, a)
            if a == 1:
                ready.append(k + 1)
        if weights_left == 0 and (kind, k) != (0, nz - 2):
            for s in ready:
                settle(s)
            ready = []
    for s in ready[:-1]:
        settle(s)
    x_step(0)
    settle(ready[-1])

    def up_term(r):
        o = ring_index((pos + nfs - r - 1) % nfs)
        return dot(tok[:, cols(o)], dpre[...], 0, 0)

    def down_term(r):
        o = ring_index((pos + r + 1) % nfs)
        return dot(hid[...], cot[:, cols(o)], 0, 0)

    g_copy = {}

    def g_send(r, half, which):
        n, m = dl // 2, fl // 2
        a, b = pl.ds(half * n, n), pl.ds(half * m, m)
        if which == 0:
            g_copy[r, half, 0] = remote(
                ug_send.at[r, a], ug_recv.at[r, a], gs.at[r, half, 0], gr.at[r, half, 0], cw
            )
        else:
            g_copy[r, half, 1] = remote(
                dg_send.at[r, b], dg_recv.at[r, b], gs.at[r, half, 1], gr.at[r, half, 1], ccw
            )

    def g_terms(r):
        ug_own[...] = up_term(r)
        dg_own[...] = down_term(r)

    def g_first():
        ug_send[0] = up_term(0).astype(BF16)
        for half in range(2):
            g_send(0, half, 0)
        dg_send[0] = down_term(0).astype(BF16)
        for half in range(2):
            g_send(0, half, 1)
        g_terms(1)

    def g_step(r, half):
        n, m = dl // 2, fl // 2
        a, b = pl.ds(half * n, n), pl.ds(half * m, m)
        g_copy[r - 1, half, 0].wait_recv()
        gu = ug_own[a, :] + ug_recv[r - 1, a, :].astype(F32)
        if r < nfs - 1:
            ug_send[r, a, :] = gu.astype(BF16)
            g_send(r, half, 0)
        else:
            ug_out[a, :] = gu * factor
        g_copy[r - 1, half, 1].wait_recv()
        gd = dg_own[b, :] + dg_recv[r - 1, b, :].astype(F32)
        if r < nfs - 1:
            dg_send[r, b, :] = gd.astype(BF16)
            g_send(r, half, 1)
        else:
            dg_out[b, :] = gd * factor

    g_first()
    dx_block(nz - 1)
    for r in range(1, max(nfs, nz)):
        if r < nfs:
            g_step(r, 0)
        if r < nz:
            x_step(r)
        if r < nfs:
            g_step(r, 1)
            if r < nfs - 1:
                g_terms(r + 1)
    for c in sends:
        c.wait_send()


def shards(nfs, ntp, tokens, up_weight, down_weight, cotangent):
    rows, width = tokens.shape
    dl, fl = up_weight.shape
    nz = ntp // 2
    whole = rows * ntp
    factor = 1.0 / (whole * nfs) ** 0.5
    dma = pltpu.SemaphoreType.DMA
    any_space = pl.BlockSpec(memory_space=pl.ANY)
    vmem = pl.BlockSpec(memory_space=pltpu.VMEM)
    return pl.pallas_call(
        functools.partial(kernel, nfs, nz, factor),
        out_shape=(
            jax.ShapeDtypeStruct((rows, width), BF16),
            jax.ShapeDtypeStruct((dl, fl), F32),
            jax.ShapeDtypeStruct((fl, dl), F32),
        ),
        in_specs=[any_space] * 4,
        out_specs=(vmem, vmem, vmem),
        scratch_shapes=[
            pltpu.VMEM((whole, width), BF16),
            pltpu.VMEM((whole, width), BF16),
            pltpu.VMEM((width, fl), BF16),
            pltpu.VMEM((fl, width), BF16),
            pltpu.VMEM((whole, fl), BF16),
            pltpu.VMEM((whole, fl), BF16),
            pltpu.VMEM((nz, rows, width), F32),
            pltpu.VMEM((nz, rows, width), BF16),
            pltpu.VMEM((nz, rows, width), BF16),
            pltpu.VMEM((nz - 1, rows, width), BF16),
            pltpu.VMEM((nz - 1, rows, width), BF16),
            pltpu.VMEM((dl, fl), F32),
            pltpu.VMEM((fl, dl), F32),
            pltpu.VMEM((nfs - 1, dl, fl), BF16),
            pltpu.VMEM((nfs - 1, dl, fl), BF16),
            pltpu.VMEM((nfs - 1, fl, dl), BF16),
            pltpu.VMEM((nfs - 1, fl, dl), BF16),
            dma((4,)),
            dma((nz - 1, 2, 2)), dma((nz - 1, 2, 2)),
            dma((nz, 2)), dma((nz, 2)),
            dma((nfs - 1, 2, 2)), dma((nfs - 1, 2, 2)),
            dma((nfs - 1, 2, 2)), dma((nfs - 1, 2, 2)),
            dma((nz,)), dma((nz,)),
            dma((nz - 1, 2)), dma((nz - 1, 2)),
        ],
        compiler_params=pltpu.CompilerParams(
            collective_id=0, has_side_effects=True, vmem_limit_bytes=67_000_000
        ),
    )(tokens, up_weight, down_weight, cotangent)


def line_kernel(
    factor, give,
    tok_in, up_in, down_in, cot_in,
    dx_out, ug_out, dg_out,
    tok, cot, up, down, up_give, down_give, hid, dpre, ug_acc, dg_acc,
    ug_send, ug_recv, dg_send, dg_recv, ug_back, dg_back, ug_home, dg_home,
    ue_send, ue_recv, de_send, de_recv, dx_own, dxm_send, dxm_recv, dxz_send, dxz_recv,
    local_sem, exs, exr, wxs, wxr, wys, wyr, ts, tr, tms, tmr,
    ms, mr, dzs, dzr, gs, gr, bs, br, held, hs, hr_, vs, vr,
):
    fs, tp = lax.axis_index("fs"), lax.axis_index("tp")
    rows, width = tok_in.shape
    dl, fl = up_in.shape
    unit, hr, hd = 2 * rows, rows // 2, dl // 2
    x, y, z, c = fs % 2, fs // 2, tp // 2, tp % 2
    high = z // 2
    toward = 1 - 2 * high
    at_end = z % 3 == 0
    fx_, fy_, fd_ = 2 * y + 1 - x, 2 * (1 - y) + x, 2 * (1 - y) + 1 - x
    mate = (fs, 2 * z + 1 - c)
    xn, yn = (fx_, tp), (fy_, tp)
    inner = (fs, 2 * (z + toward) + c)
    outer = (fs, 2 * jnp.maximum(z - toward, 0) + c)
    beyond = (fs, 2 * (z + 2 * toward) + c)
    Q = range(4)

    def cols(o):
        return pl.ds(pl.multiple_of(o * dl, dl), dl)

    bufs = (tok, cot)

    def rows_of(j, u, shift=0):
        return bufs[j % 2].at[pl.ds(u * unit + shift + (j // 2) * rows, hr)]

    def body(end):
        nf = fl - give if end else fl + give
        nown = fl - give if end else fl
        units = slice(0, nf)
        locals_ = [
            pltpu.make_async_copy(up_in.at[:, pl.ds(0, nown)], up.at[cols(fs), pl.ds(0, nown)], local_sem.at[0]),
            pltpu.make_async_copy(down_in.at[pl.ds(0, nown)], down.at[pl.ds(0, nown), cols(fs)], local_sem.at[1]),
        ]
        for j in Q:
            mine = pl.ds((j // 2) * hr, hr)
            locals_.append(pltpu.make_async_copy((tok_in, cot_in)[j % 2].at[mine], rows_of(j, 0), local_sem.at[2 + j]))
        if end:
            locals_ += [
                pltpu.make_async_copy(up_in.at[:, pl.ds(nown, give)], up_give, local_sem.at[6]),
                pltpu.make_async_copy(down_in.at[pl.ds(nown, give)], down_give, local_sem.at[7]),
            ]
        for cp in locals_:
            cp.start()
        barrier = pltpu.get_barrier_semaphore()
        peers = (mate, xn, yn, inner) if end else (mate, xn, yn, inner, outer)
        for peer in peers:
            pl.semaphore_signal(barrier, inc=1, device_id=peer, device_id_type=MESH)
        pl.semaphore_wait(barrier, len(peers))
        for cp in locals_:
            cp.wait()

        def remote(src, dst, s, r, peer):
            return pltpu.make_async_remote_copy(
                src_ref=src, dst_ref=dst, send_sem=s, recv_sem=r, device_id=peer, device_id_type=MESH
            )

        def go(cp):
            cp.start()

        def sent(ref, sem):
            remote(ref, ref, sem, sem, mate).wait_send()

        def size(elements):
            return tok.at[pl.ds(0, elements // width)]

        def piece(o, q):
            if q < 2:
                return up.at[pl.ds(pl.multiple_of(o * dl + q * hd, hd), hd), pl.ds(0, nown)]
            if q < 4:
                return down.at[pl.ds((q - 2) * (nown // 2), nown // 2), cols(o)]
            if q == 4:
                return up.at[cols(o), pl.ds(fl, give)]
            return down.at[pl.ds(fl, give), cols(o)]

        pieces = Q if end else range(6)
        wx = [[remote(piece(o, q), piece(o, q), wxs.at[0], wxr.at[i, q], xn) for q in pieces]
              for i, o in enumerate((fs, fy_))]
        wy = [[remote(piece(o, q), piece(o, q), wys.at[0], wyr.at[i, q], yn) for q in pieces]
              for i, o in enumerate((fs, fx_))]

        def t_send(flow, j, u, v, peer):
            go(remote(rows_of(j, u), rows_of(j, v), ts.at[flow], tr.at[v, j], peer))

        def t_wait(u, j):
            remote(rows_of(j, u), rows_of(j, u), ts.at[0], tr.at[u, j], mate).wait_recv()

        def mate_slot(u, j):
            return 2 * u + j // 2 + (end and u == 3 and j == 3)

        tm = [[remote(rows_of(j, u), rows_of(j, u, hr), tms.at[0], tmr.at[mate_slot(u, j)], mate) for j in Q]
              for u in range(4)]

        def from_mate(u, h):
            got = pl.ds(u * unit, hr if end and u == 3 and h else rows)
            remote(tok.at[got], tok.at[got], tms.at[0], tmr.at[2 * u + h], mate).wait_recv()

        def w_got(q):
            wx[0][q].wait_recv()
            if q % 2 == 0:
                go(wy[1][q])
            wy[0][q].wait_recv()
            if q % 2:
                go(wx[1][q])

        ex = (remote(up_give, up.at[cols(fs), pl.ds(fl, give)], exs.at[0], exr.at[0], inner),
              remote(down_give, down.at[pl.ds(fl, give), cols(fs)], exs.at[1], exr.at[1], inner))

        def hidden_block(u, here=None):
            here = pl.ds(u * unit, unit) if here is None else here
            active = jnp.maximum(dot(tok[here, :], up[:, units], 1, 0), 0.0)
            hid[here, units] = (active * active).astype(BF16)
            dh = dot(cot[here, :], down[units, :], 1, 1)
            dpre[here, units] = (2.0 * active * dh).astype(BF16)

        dxm = [remote(dxm_send.at[u], dxm_recv.at[u], ms.at[0], mr.at[u], mate) for u in range(4)]

        def dx_block(u):
            here = pl.ds(u * unit, unit)

            def tile(j, carry):
                o = cols(j)
                part = dot(dpre[here, units], up[o, units], 1, 1)
                for h in range(2):
                    half = pl.ds(h * hr, hr)
                    dx_own[u, half, o] = part[2 * h * hr : (2 * h + 1) * hr]
                    dxm_send[u, half, o] = part[(2 * h + 1) * hr : (2 * h + 2) * hr].astype(BF16)
                return carry

            lax.fori_loop(0, 4, tile, 0)
            go(dxm[u])

        def dx_sum(u):
            dxm[u].wait_recv()
            return dx_own[u] + dxm_recv[u].astype(F32)

        def z_wait(slot):
            remote(dxz_send.at[0], dxz_recv.at[slot], dzs.at[0], dzr.at[slot], mate).wait_recv()
            return dxz_recv[slot].astype(F32)

        def z_send(i, value, slot, peer):
            dxz_send[i] = value.astype(BF16)
            go(remote(dxz_send.at[i], dxz_recv.at[slot], dzs.at[0], dzr.at[slot], peer))

        def ready(u):
            from_mate(u, 0)
            from_mate(u, 1)
            hidden_block(u)

        if end:
            for cp in ex:
                go(cp)
            for q in Q:
                go(wx[0][q])
                go(wy[0][q])
            for j in Q:
                t_send(0, j, 0, 1, inner)
            for j in Q:
                go(tm[0][j])
            for j in Q:
                w_got(j)
                t_wait(1, j)
                go(tm[1][j])
            for q in Q:
                (wy if q % 2 else wx)[1][q ^ 1].wait_recv()
            ready(0)
            ready(1)
            dx_block(1)
            t_wait(2, 0)
            go(tm[2][0])
            z_send(0, dx_sum(1), 0, inner)
            for j in (1, 2, 3):
                t_wait(2, j)
                go(tm[2][j])
            ready(2)
            dx_block(2)
            t_wait(3, 0)
            go(tm[3][0])
            z_send(1, dx_sum(2), 1, inner)
        else:
            for q in Q:
                go(wx[0][q])
                go(wy[0][q])
            for j in Q:
                t_send(0, j, 0, 1, outer)
            for j in (0, 1):
                t_send(1, j, 0, 3, inner)
            for j in Q:
                go(tm[0][j])
            for i in range(2):
                ex[i].wait_recv()
                go(wx[0][4 + i])
                go(wy[0][4 + i])

            def from_end(j):
                t_wait(1, j)
                t_send(2, j, 1, 2, inner)
                go(tm[1][j])

            def from_middle(j):
                t_wait(3, j)
                go(tm[3][j])

            def from_far(j):
                t_wait(2, j)
                t_send(4, j, 2, 2, outer)
                go(tm[2][j])

            from_end(0)
            w_got(0)
            from_end(1)
            from_middle(0)
            from_middle(1)
            w_got(1)
            from_end(2)
            from_far(0)
            w_got(2)
            from_end(3)
            for j in (2, 3):
                t_send(1, j, 0, 3, inner)
            from_far(1)
            w_got(3)
            w_got(4)
            w_got(5)
            from_far(2)
            from_far(3)
            for j in (0, 1):
                t_send(3, j, 3, 3, outer)

            def products(here, o):
                return (dot(tok[here, cols(o)], up[cols(o), units], 1, 0),
                        dot(cot[here, cols(o)], down[units, cols(o)], 1, 1))

            spans = [(u * unit, unit) for u in range(3)] + [(3 * unit, rows)]
            for u, (at, n) in enumerate(spans):
                here, there = pl.ds(at, n), pl.ds(4 * unit + at, n)
                from_mate(u, 0)
                if u < 3:
                    from_mate(u, 1)
                for i, o in enumerate((fs, fx_, fy_)):
                    pre, dh = products(here, o)
                    if i:
                        pre, dh = pre + ug_acc[here, units], dh + ug_acc[there, units]
                    ug_acc[here, units] = pre
                    ug_acc[there, units] = dh
            for q in pieces:
                (wy if q % 2 else wx)[1][q ^ 1].wait_recv()
            for at, n in spans:
                here, there = pl.ds(at, n), pl.ds(4 * unit + at, n)
                pre, dh = products(here, fd_)
                active = jnp.maximum(pre + ug_acc[here, units], 0.0)
                hid[here, units] = (active * active).astype(BF16)
                dpre[here, units] = (2.0 * active * (dh + ug_acc[there, units])).astype(BF16)
            for j in (2, 3):
                from_middle(j)
                t_send(3, j, 3, 3, outer)

        cut = 3 * unit + rows
        early = pl.ds(0, cut)
        last = pl.ds(cut, 4 * unit - cut)

        def ug_early(o, carry):
            ug_acc[cols(o), units] = dot(tok[early, cols(o)], dpre[early, units], 0, 0)
            return carry

        def dg_early(o, carry):
            dg_acc[units, cols(o)] = dot(hid[early, units], cot[early, cols(o)], 0, 0)
            return carry

        if end:
            t_wait(3, 1)
            go(tm[3][1])
            dx_block(0)
            from_mate(3, 0)
            hidden_block(3, pl.ds(3 * unit, rows))
            lax.fori_loop(0, 4, ug_early, 0)
            t_wait(3, 2)
            go(tm[3][2])
            lax.fori_loop(0, 4, dg_early, 0)
            from_mate(3, 1)
            spare = pl.ds(fl, rows)
            active = jnp.maximum(dot(tok[last, :], up[:, units], 1, 0), 0.0)
            hid[last, units] = (active * active).astype(BF16)
            dg_acc[spare, units] = active
            t_wait(3, 3)
            go(tm[3][3])
            from_mate(3, 2)
            dh = dot(cot[last, :], down[units, :], 1, 1)
            dpre[last, units] = (2.0 * dg_acc[spare, units] * dh).astype(BF16)
        else:
            ug_early(fd_, 0)
            dg_early(fd_, 0)
            from_mate(3, 1)
            hidden_block(3, last)

        def drain():
            w_bytes = (dl * nown * 2) * 3 // 2 + (0 if end else dl * give * 3)
            sent(size(w_bytes), wxs.at[0])
            sent(size(w_bytes), wys.at[0])
            for flow in range(1 if end else 5):
                sent(tok.at[pl.ds(0, unit)], ts.at[flow])
            sent(tok, tms.at[0])
            if end:
                for cp in ex:
                    cp.wait_send()

        gh = nown // 2

        def buf(bufs, k, q):
            if q < 2:
                return bufs[0].at[k, q, :, pl.ds(0, nown)]
            if q < 4:
                return bufs[1].at[k, q - 2, pl.ds(0, gh)]
            return bufs[q - 2].at[k]

        out_bufs, in_bufs = (ug_send, dg_send, ue_send, de_send), (ug_recv, dg_recv, ue_recv, de_recv)

        detours = ((1, 2), (2, 3))
        few_rows = give // 2

        def g_copy(k, q):
            over_x = k == 1 or (k == 0 and q % 2 == 0)
            src, dst = buf(out_bufs, k, q), buf(in_bufs, k, q)
            if end and (k, q) in detours:
                most = pl.ds(0, gh - few_rows)
                src, dst = src.at[most], dst.at[most]
            return remote(src, dst, gs.at[0], gr.at[k, q], xn if over_x else yn)

        def rest_of(bufs, i):
            k, q = detours[i]
            return bufs[1].at[k, q - 2, pl.ds((fl - give) // 2 - few_rows, few_rows)]

        there = 2 * (z + toward) + c
        leave = [remote(rest_of(out_bufs, i), held.at[i], hs.at[i], hr_.at[i], ((fx_, fy_)[i], there))
                 for i in range(2)]
        arrive = [remote(held.at[i], rest_of(in_bufs, i), vs.at[i], vr.at[i], outer) for i in range(2)]

        g = [[g_copy(k, q) for q in pieces] for k in range(3)]

        def acc_of(o, q):
            if q < 2:
                return ug_acc, pl.ds(pl.multiple_of(o * dl + q * hd, hd), hd), slice(0, nown)
            if q < 4:
                return dg_acc, pl.ds((q - 2) * gh, gh), cols(o)
            if q == 4:
                return ug_acc, cols(o), slice(nown, nf)
            return dg_acc, slice(nown, nf), cols(o)

        def g_put(k, q, value):
            dst = buf(out_bufs, k, q)
            dst[...] = value.astype(BF16)
            go(g[k][q])
            if end and (k, q) in detours:
                go(leave[detours.index((k, q))])

        def terms(o, p):
            split = end or o is fd_
            part = last if split else slice(None)
            few = slice(nown, nf) if p > 1 else slice(0, nown)
            if p % 2 == 0:
                val = dot(tok[part, cols(o)], dpre[part, few], 0, 0)
                if split:
                    val = val + ug_acc[cols(o), few]
                return (val,) if p > 1 else (val[:hd], val[hd:])
            val = dot(hid[part, few], cot[part, cols(o)], 0, 0)
            if split:
                val = val + dg_acc[few, cols(o)]
            return (val,) if p > 1 else (val[:gh], val[gh:])

        def keep(o, q, value):
            ref, a, b = acc_of(o, q)
            ref[a, b] = value

        def begin(p):
            q = 2 * p if p < 2 else p + 2
            for h, v in enumerate(terms(fd_, p)):
                g_put(0, q + h, v)

        def follow(p):
            q = 2 * p if p < 2 else p + 2
            for h, v in enumerate(terms(fx_, p)):
                if (q + h) % 2 == 0:
                    g_put(1, q + h, v)
                else:
                    keep(fx_, q + h, v)
            for h, v in enumerate(terms(fy_, p)):
                if (q + h) % 2:
                    g_put(2, q + h, v)
                else:
                    keep(fy_, q + h, v)

        def own_terms(p):
            q = 2 * p if p < 2 else p + 2
            for h, v in enumerate(terms(fs, p)):
                keep(fs, q + h, v)

        def pass_on(q):
            g[0][q].wait_recv()
            k, o = (1, fx_) if q % 2 else (2, fy_)
            ref, a, b = acc_of(o, q)
            g_put(k, q, ref[a, b] + buf(in_bufs, 0, q)[...].astype(F32))

        back = (remote(ug_back, ug_home, bs.at[0], br.at[0], outer),
                remote(dg_back, dg_home, bs.at[1], br.at[1], outer))

        def summed(q):
            ref, a, b = acc_of(fs, q)
            total = ref[a, b]
            for k in (1, 2):
                g[k][q].wait_recv()
                if end and (k, q) in detours:
                    arrive[detours.index((k, q))].wait_recv()
                total = total + buf(in_bufs, k, q)[...].astype(F32)
            return total

        def finish(q):
            if q < 2:
                ug_out[pl.ds(q * hd, hd), pl.ds(0, nown)] = summed(q) * factor
            else:
                dg_out[pl.ds((q - 2) * gh, gh), :] = summed(q) * factor

        if end:
            begin(0)
            begin(1)
            follow(0)
            follow(1)
            dx_block(3)
            pass_on(0)
            pass_on(1)
            own_terms(0)
            own_terms(1)
            pass_on(2)
            pass_on(3)
            z_send(2, dx_sum(3), 4, beyond)
            drain()
            dx_out[...] = (dx_sum(0) + z_wait(0)).astype(BF16)
            back[0].wait_recv()
            ug_out[:, pl.ds(nown, give)] = ug_home[...].astype(F32) * factor
            back[1].wait_recv()
            dg_out[pl.ds(nown, give), :] = dg_home[...].astype(F32) * factor
        else:
            begin(2)
            begin(3)
            follow(2)
            follow(3)
            dx_block(3)
            begin(0)
            begin(1)
            z_send(0, dx_sum(3), 2, inner)
            pass_on(4)
            pass_on(5)
            follow(0)
            follow(1)
            dx_block(2)
            own_terms(2)
            own_terms(3)
            pass_on(0)
            pass_on(1)
            z_send(1, dx_sum(2) + z_wait(1), 3, inner)
            own_terms(0)
            own_terms(1)
            pass_on(2)
            pass_on(3)
            dx_block(1)
            dx_block(0)
            ug_back[...] = summed(4).astype(BF16)
            dg_back[...] = summed(5).astype(BF16)
            drain()
            go(back[0])
            go(back[1])
            z_send(2, dx_sum(1) + z_wait(3), 0, outer)
            for i in range(2):
                leave[i].wait_recv()
                go(arrive[i])
        for q in Q:
            finish(q)
        if not end:
            near = dx_sum(0) + z_wait(0) + z_wait(2)
            dx_out[...] = (near + z_wait(4)).astype(BF16)
        g_bytes = 12 * hd * nown + (-2 * few_rows * dl if end else 6 * dl * give)
        sent(size(g_bytes), gs.at[0])
        sent(dxm_send, ms.at[0])
        sent(dxz_send, dzs.at[0])
        for cp in leave if end else (*back, *arrive):
            cp.wait_send()

    pl.when(at_end)(lambda: body(True))
    pl.when(jnp.logical_not(at_end))(lambda: body(False))


def put_out(n, *refs):
    copies = [pltpu.make_async_copy(refs[i], refs[n + i], refs[2 * n].at[i]) for i in range(n)]
    for cp in copies:
        cp.start()
    for cp in copies:
        cp.wait()


def line_shards(nfs, ntp, tokens, up_weight, down_weight, cotangent):
    rows, width = tokens.shape
    dl, fl = up_weight.shape
    factor = 1.0 / (rows * ntp * nfs) ** 0.5
    mine = ntp * rows
    give = fl // 4
    most = fl + give
    hd = dl // 2
    dma = pltpu.SemaphoreType.DMA
    any_space = pl.BlockSpec(memory_space=pl.ANY)
    vmem = pl.BlockSpec(memory_space=pltpu.VMEM)
    V = pltpu.VMEM
    results = pl.pallas_call(
        functools.partial(line_kernel, factor, give),
        out_shape=(V((rows, width), BF16), V((dl, fl), F32), V((fl, dl), F32)),
        in_specs=[any_space] * 4,
        out_specs=(vmem, vmem, vmem),
        scratch_shapes=[
            V((mine, width), BF16), V((mine, width), BF16),
            V((width, most), BF16), V((most, width), BF16),
            V((dl, give), BF16), V((give, dl), BF16),
            V((mine, most), BF16), V((mine, most), BF16),
            V((width, most), F32), V((most, width), F32),
            V((3, 2, hd, fl), BF16), V((3, 2, hd, fl), BF16),
            V((3, 2, fl // 2, dl), BF16), V((3, 2, fl // 2, dl), BF16),
            V((dl, give), BF16), V((give, dl), BF16), V((dl, give), BF16), V((give, dl), BF16),
            V((3, dl, give), BF16), V((3, dl, give), BF16), V((3, give, dl), BF16), V((3, give, dl), BF16),
            V((4, rows, width), F32), V((4, rows, width), BF16), V((4, rows, width), BF16),
            V((3, rows, width), BF16), V((5, rows, width), BF16),
            dma((8,)), dma((2,)), dma((2,)), dma((1,)), dma((2, 6)), dma((1,)), dma((2, 6)),
            dma((5,)), dma((4, 4)), dma((1,)), dma((9,)),
            dma((1,)), dma((4,)), dma((1,)), dma((5,)), dma((1,)), dma((3, 6)), dma((2,)), dma((2,)),
            V((2, give // 2, dl), BF16), dma((2,)), dma((2,)), dma((2,)), dma((2,)),
        ],
        compiler_params=pltpu.CompilerParams(
            collective_id=0, has_side_effects=True, vmem_limit_bytes=60_000_000
        ),
    )(tokens, up_weight, down_weight, cotangent)
    return pl.pallas_call(
        functools.partial(put_out, len(results)),
        out_shape=tuple(jax.ShapeDtypeStruct(r.shape, r.dtype) for r in results),
        in_specs=[vmem] * len(results),
        out_specs=(any_space,) * len(results),
        scratch_shapes=[dma((3,))],
        compiler_params=pltpu.CompilerParams(vmem_limit_bytes=8_000_000),
    )(*results)


def solution(mesh):
    placed = (P(("fs", "tp"), None), P("fs", "tp"), P("tp", "fs"), P(("fs", "tp"), None))
    fs, tp = mesh.shape["fs"], mesh.shape["tp"]
    body = line_shards if (fs, tp) == (4, 8) else shards
    return jax.shard_map(
        functools.partial(body, mesh.shape["fs"], mesh.shape["tp"]),
        mesh=mesh,
        in_specs=placed,
        out_specs=(P(("fs", "tp"), None), P("fs", "tp"), P("tp", "fs")),
        check_vma=False,
    )
```

```python
import functools

import jax
import jax.numpy as jnp
from jax import lax
from jax.experimental import pallas as pl
from jax.experimental.pallas import tpu as pltpu
from jax.sharding import PartitionSpec as P

MESH = pl.DeviceIdType.MESH
BF16 = jnp.bfloat16
F32 = jnp.float32


def ring_index(p):
    q, b = p // 2, p % 2
    return 2 * q + b + (q % 2) * (1 - 2 * b)


def dot(a, b, ca, cb):
    return lax.dot_general(a, b, (((ca,), (cb,)), ((), ())), preferred_element_type=F32)


def kernel(
    nfs, nz, factor,
    tok_in, up_in, down_in, cot_in,
    dx_out, ug_out, dg_out,
    tok, cot, up, down, hid, dpre,
    dx_own, dx_send, dx_recv, dr_send, dr_recv,
    ug_own, dg_own, ug_send, ug_recv, dg_send, dg_recv,
    local_sem, zs, zr, ps, pr, ws, wr, gs, gr, xs, xr, rs, rr,
):
    fs, tp = lax.axis_index("fs"), lax.axis_index("tp")
    rows, width = tok_in.shape
    h = rows // 2
    block = 4 * h
    dl = up_in.shape[0]
    fl = up_in.shape[1]
    z, core = tp // 2, tp % 2
    pos = ring_index(fs)
    fwd = (fs, ((z + 1) % nz) * 2 + core)
    bwd = (fs, ((z + nz - 1) % nz) * 2 + core)
    mate = (fs, 2 * z + 1 - core)
    cw = (ring_index((pos + 1) % nfs), tp)
    ccw = (ring_index((pos + nfs - 1) % nfs), tp)

    def cols(o):
        return pl.ds(pl.multiple_of(o * dl, dl), dl)

    locals_ = [
        pltpu.make_async_copy(tok_in, tok.at[pl.ds(0, rows)], local_sem.at[0]),
        pltpu.make_async_copy(up_in, up.at[cols(fs)], local_sem.at[1]),
        pltpu.make_async_copy(down_in, down.at[:, cols(fs)], local_sem.at[2]),
        pltpu.make_async_copy(cot_in, cot.at[pl.ds(0, rows)], local_sem.at[3]),
    ]
    for c in locals_:
        c.start()
    barrier = pltpu.get_barrier_semaphore()
    peers = (fwd, bwd, mate, cw, ccw)
    for peer in peers:
        pl.semaphore_signal(barrier, inc=1, device_id=peer, device_id_type=MESH)
    pl.semaphore_wait(barrier, len(peers))
    for c in locals_:
        c.wait()

    sends = []

    def remote(src, dst, s, r, peer):
        c = pltpu.make_async_remote_copy(
            src_ref=src, dst_ref=dst, send_sem=s, recv_sem=r, device_id=peer, device_id_type=MESH
        )
        c.start()
        sends.append(c)
        return c

    bufs = (tok, cot)

    def z_send(k, a):
        out = []
        for d, peer in enumerate((fwd, bwd)):
            out.append(remote(
                bufs[a].at[pl.ds(k * block + d * h, h)],
                bufs[a].at[pl.ds((k + 1) * block + d * h, h)],
                zs.at[k, d, a], zr.at[k, d, a], peer,
            ))
        return out

    def mate_send(k, a):
        return remote(
            bufs[a].at[pl.ds(k * block, 2 * h)],
            bufs[a].at[pl.ds(k * block + 2 * h, 2 * h)],
            ps.at[k, a], pr.at[k, a], mate,
        )

    def w_send(k, half):
        a = ring_index((pos + nfs - k) % nfs)
        b = ring_index((pos + k) % nfs)
        n = dl // 2
        piece = up.at[pl.ds(pl.multiple_of(a * dl + half * n, n), n)]
        m = fl // 2
        other = down.at[pl.ds(half * m, m), cols(b)]
        return [
            remote(piece, piece, ws.at[k, half, 0], wr.at[k, half, 0], cw),
            remote(other, other, ws.at[k, half, 1], wr.at[k, half, 1], ccw),
        ]

    z_copy, w_copy, mate_copy = {}, {}, {}
    for a in range(2):
        z_copy[0, a] = z_send(0, a)
        w_copy[0, a] = w_send(0, a)
    for a in range(2):
        mate_copy[0, a] = mate_send(0, a)

    def hidden_block(s):
        here = pl.ds(s * block, block)
        active = jnp.maximum(dot(tok[here, :], up[...], 1, 0), 0.0)
        hid[here, :] = (active * active).astype(BF16)
        dh = dot(cot[here, :], down[...], 1, 1)
        dpre[here, :] = (2.0 * active * dh).astype(BF16)

    pair_copy = {}

    def dx_block(s):
        here = pl.ds(s * block, block)

        def tile(j, carry):
            c = cols(j)
            part = dot(dpre[here, :], up[c, :], 1, 1)
            dx_own[s, :, c] = part[: 2 * h]
            dx_send[s, :, c] = part[2 * h :].astype(BF16)
            return carry

        lax.fori_loop(0, nfs, tile, 0)
        pair_copy[s] = remote(dx_send.at[s], dx_recv.at[s], xs.at[s], xr.at[s], mate)

    x_copy = {}

    def x_step(r):
        s = r + 1 if r < nz - 1 else 0
        pair_copy[s].wait_recv()
        for d, peer in enumerate((fwd, bwd)):
            here = pl.ds(d * h, h)
            if r > 0:
                x_copy[r - 1, d].wait_recv()
            total = dx_own[s, here, :] + dx_recv[s, here, :].astype(F32)
            if r > 0:
                total = total + dr_recv[r - 1, here, :].astype(F32)
            if r < nz - 1:
                dr_send[r, here, :] = total.astype(BF16)
                x_copy[r, d] = remote(
                    dr_send.at[r, here], dr_recv.at[r, here], rs.at[r, d], rr.at[r, d], peer
                )
            else:
                dx_out[here, :] = total.astype(BF16)

    events = []
    for k in range(nfs - 1):
        for half in range(2):
            events.append(((2 * k + half + 1) * 1.5 / (nfs - 1), 1, k, half))
    for k in range(nz - 1):
        for a in range(2):
            events.append(((2 * k + a + 1) * 3.0 / (nz - 1), 0, k, a))
    events.sort()
    weights_left = 2 * (nfs - 1)
    ready = [0]

    def settle(s):
        for a in range(2):
            mate_copy[s, a].wait_recv()
        hidden_block(s)
        if s < nz - 1:
            dx_block(s)

    for _, kind, k, a in events:
        if kind == 1:
            for c in w_copy[k, a]:
                c.wait_recv()
            if k + 1 < nfs - 1:
                w_copy[k + 1, a] = w_send(k + 1, a)
            weights_left -= 1
        else:
            for c in z_copy[k, a]:
                c.wait_recv()
            if k + 1 < nz - 1:
                z_copy[k + 1, a] = z_send(k + 1, a)
            mate_copy[k + 1, a] = mate_send(k + 1, a)
            if a == 1:
                ready.append(k + 1)
        if weights_left == 0 and (kind, k) != (0, nz - 2):
            for s in ready:
                settle(s)
            ready = []
    for s in ready[:-1]:
        settle(s)
    x_step(0)
    settle(ready[-1])

    def up_term(r):
        o = ring_index((pos + nfs - r - 1) % nfs)
        return dot(tok[:, cols(o)], dpre[...], 0, 0)

    def down_term(r):
        o = ring_index((pos + r + 1) % nfs)
        return dot(hid[...], cot[:, cols(o)], 0, 0)

    g_copy = {}

    def g_send(r, half, which):
        n, m = dl // 2, fl // 2
        a, b = pl.ds(half * n, n), pl.ds(half * m, m)
        if which == 0:
            g_copy[r, half, 0] = remote(
                ug_send.at[r, a], ug_recv.at[r, a], gs.at[r, half, 0], gr.at[r, half, 0], cw
            )
        else:
            g_copy[r, half, 1] = remote(
                dg_send.at[r, b], dg_recv.at[r, b], gs.at[r, half, 1], gr.at[r, half, 1], ccw
            )

    def g_terms(r):
        ug_own[...] = up_term(r)
        dg_own[...] = down_term(r)

    def g_first():
        ug_send[0] = up_term(0).astype(BF16)
        for half in range(2):
            g_send(0, half, 0)
        dg_send[0] = down_term(0).astype(BF16)
        for half in range(2):
            g_send(0, half, 1)
        g_terms(1)

    def g_step(r, half):
        n, m = dl // 2, fl // 2
        a, b = pl.ds(half * n, n), pl.ds(half * m, m)
        g_copy[r - 1, half, 0].wait_recv()
        gu = ug_own[a, :] + ug_recv[r - 1, a, :].astype(F32)
        if r < nfs - 1:
            ug_send[r, a, :] = gu.astype(BF16)
            g_send(r, half, 0)
        else:
            ug_out[a, :] = gu * factor
        g_copy[r - 1, half, 1].wait_recv()
        gd = dg_own[b, :] + dg_recv[r - 1, b, :].astype(F32)
        if r < nfs - 1:
            dg_send[r, b, :] = gd.astype(BF16)
            g_send(r, half, 1)
        else:
            dg_out[b, :] = gd * factor

    g_first()
    dx_block(nz - 1)
    for r in range(1, max(nfs, nz)):
        if r < nfs:
            g_step(r, 0)
        if r < nz:
            x_step(r)
        if r < nfs:
            g_step(r, 1)
            if r < nfs - 1:
                g_terms(r + 1)
    for c in sends:
        c.wait_send()


def shards(nfs, ntp, tokens, up_weight, down_weight, cotangent):
    rows, width = tokens.shape
    dl, fl = up_weight.shape
    nz = ntp // 2
    whole = rows * ntp
    factor = 1.0 / (whole * nfs) ** 0.5
    dma = pltpu.SemaphoreType.DMA
    any_space = pl.BlockSpec(memory_space=pl.ANY)
    vmem = pl.BlockSpec(memory_space=pltpu.VMEM)
    return pl.pallas_call(
        functools.partial(kernel, nfs, nz, factor),
        out_shape=(
            jax.ShapeDtypeStruct((rows, width), BF16),
            jax.ShapeDtypeStruct((dl, fl), F32),
            jax.ShapeDtypeStruct((fl, dl), F32),
        ),
        in_specs=[any_space] * 4,
        out_specs=(vmem, vmem, vmem),
        scratch_shapes=[
            pltpu.VMEM((whole, width), BF16),
            pltpu.VMEM((whole, width), BF16),
            pltpu.VMEM((width, fl), BF16),
            pltpu.VMEM((fl, width), BF16),
            pltpu.VMEM((whole, fl), BF16),
            pltpu.VMEM((whole, fl), BF16),
            pltpu.VMEM((nz, rows, width), F32),
            pltpu.VMEM((nz, rows, width), BF16),
            pltpu.VMEM((nz, rows, width), BF16),
            pltpu.VMEM((nz - 1, rows, width), BF16),
            pltpu.VMEM((nz - 1, rows, width), BF16),
            pltpu.VMEM((dl, fl), F32),
            pltpu.VMEM((fl, dl), F32),
            pltpu.VMEM((nfs - 1, dl, fl), BF16),
            pltpu.VMEM((nfs - 1, dl, fl), BF16),
            pltpu.VMEM((nfs - 1, fl, dl), BF16),
            pltpu.VMEM((nfs - 1, fl, dl), BF16),
            dma((4,)),
            dma((nz - 1, 2, 2)), dma((nz - 1, 2, 2)),
            dma((nz, 2)), dma((nz, 2)),
            dma((nfs - 1, 2, 2)), dma((nfs - 1, 2, 2)),
            dma((nfs - 1, 2, 2)), dma((nfs - 1, 2, 2)),
            dma((nz,)), dma((nz,)),
            dma((nz - 1, 2)), dma((nz - 1, 2)),
        ],
        compiler_params=pltpu.CompilerParams(
            collective_id=0, has_side_effects=True, vmem_limit_bytes=67_000_000
        ),
    )(tokens, up_weight, down_weight, cotangent)


def line_kernel(
    factor, give,
    tok_in, up_in, down_in, cot_in,
    dx_out, ug_out, dg_out,
    tok, cot, up, down, up_give, down_give, hid, dpre, ug_acc, dg_acc,
    ug_send, ug_recv, dg_send, dg_recv, ug_back, dg_back, ug_home, dg_home,
    ue_send, ue_recv, de_send, de_recv, dx_own, dxm_send, dxm_recv, dxz_send, dxz_recv,
    local_sem, exs, exr, wxs, wxr, wys, wyr, ts, tr, tms, tmr,
    ms, mr, dzs, dzr, gs, gr, bs, br, held, hs, hr_, vs, vr,
):
    fs, tp = lax.axis_index("fs"), lax.axis_index("tp")
    rows, width = tok_in.shape
    dl, fl = up_in.shape
    unit, hr, hd = 2 * rows, rows // 2, dl // 2
    x, y, z, c = fs % 2, fs // 2, tp // 2, tp % 2
    high = z // 2
    toward = 1 - 2 * high
    at_end = z % 3 == 0
    fx_, fy_, fd_ = 2 * y + 1 - x, 2 * (1 - y) + x, 2 * (1 - y) + 1 - x
    mate = (fs, 2 * z + 1 - c)
    xn, yn = (fx_, tp), (fy_, tp)
    inner = (fs, 2 * (z + toward) + c)
    outer = (fs, 2 * jnp.maximum(z - toward, 0) + c)
    beyond = (fs, 2 * (z + 2 * toward) + c)
    Q = range(4)

    def cols(o):
        return pl.ds(pl.multiple_of(o * dl, dl), dl)

    bufs = (tok, cot)

    def rows_of(j, u, shift=0):
        return bufs[j % 2].at[pl.ds(u * unit + shift + (j // 2) * rows, hr)]

    def body(end):
        nf = fl - give if end else fl + give
        nown = fl - give if end else fl
        units = slice(0, nf)
        locals_ = [
            pltpu.make_async_copy(up_in.at[:, pl.ds(0, nown)], up.at[cols(fs), pl.ds(0, nown)], local_sem.at[0]),
            pltpu.make_async_copy(down_in.at[pl.ds(0, nown)], down.at[pl.ds(0, nown), cols(fs)], local_sem.at[0]),
        ]
        for j in Q:
            mine = pl.ds((j // 2) * hr, hr)
            locals_.append(pltpu.make_async_copy((tok_in, cot_in)[j % 2].at[mine], rows_of(j, 0), local_sem.at[0]))
        if end:
            locals_ += [
                pltpu.make_async_copy(up_in.at[:, pl.ds(nown, give)], up_give, local_sem.at[0]),
                pltpu.make_async_copy(down_in.at[pl.ds(nown, give)], down_give, local_sem.at[0]),
            ]
        for cp in locals_:
            cp.start()
        barrier = pltpu.get_barrier_semaphore()
        peers = (mate, xn, yn, inner) if end else (mate, xn, yn, inner, outer)
        for peer in peers:
            pl.semaphore_signal(barrier, inc=1, device_id=peer, device_id_type=MESH)
        pl.semaphore_wait(barrier, len(peers))
        taken = tok.at[pl.ds(0, 2 * (dl * fl + rows * width) // width)]
        pltpu.make_async_copy(taken, taken, local_sem.at[0]).wait()

        def remote(src, dst, s, r, peer):
            return pltpu.make_async_remote_copy(
                src_ref=src, dst_ref=dst, send_sem=s, recv_sem=r, device_id=peer, device_id_type=MESH
            )

        def go(cp):
            cp.start()

        def sent(ref, sem):
            remote(ref, ref, sem, sem, mate).wait_send()

        def size(elements):
            return tok.at[pl.ds(0, elements // width)]

        def piece(o, q):
            if q < 2:
                return up.at[pl.ds(pl.multiple_of(o * dl + q * hd, hd), hd), pl.ds(0, nown)]
            if q < 4:
                return down.at[pl.ds((q - 2) * (nown // 2), nown // 2), cols(o)]
            if q == 4:
                return up.at[cols(o), pl.ds(fl, give)]
            return down.at[pl.ds(fl, give), cols(o)]

        pieces = Q if end else range(6)
        wx = [[remote(piece(o, q), piece(o, q), wxs.at[0], wxr.at[6 if i else q], xn) for q in pieces]
              for i, o in enumerate((fs, fy_))]
        wy = [[remote(piece(o, q), piece(o, q), wys.at[0], wyr.at[6 if i else q], yn) for q in pieces]
              for i, o in enumerate((fs, fx_))]

        def t_send(flow, j, u, v, peer):
            go(remote(rows_of(j, u), rows_of(j, v), ts.at[flow], tr.at[v, j], peer))

        def t_wait(u, j):
            remote(rows_of(j, u), rows_of(j, u), ts.at[0], tr.at[u, j], mate).wait_recv()

        def mate_slot(u, j):
            return 2 * u + j // 2 + (end and u == 3 and j == 3)

        tm = [[remote(rows_of(j, u), rows_of(j, u, hr), tms.at[0], tmr.at[mate_slot(u, j)], mate) for j in Q]
              for u in range(4)]

        def from_mate(u, h):
            got = pl.ds(u * unit, hr if end and u == 3 and h else rows)
            remote(tok.at[got], tok.at[got], tms.at[0], tmr.at[2 * u + h], mate).wait_recv()

        def passed_on():
            ref = size(hd * nown + (nown // 2) * dl + (0 if end else give * dl))
            for sem in (wxr.at[6], wyr.at[6]):
                remote(ref, ref, sem, sem, mate).wait_recv()

        def w_got(q):
            wx[0][q].wait_recv()
            if q % 2 == 0:
                go(wy[1][q])
            wy[0][q].wait_recv()
            if q % 2:
                go(wx[1][q])

        ex = (remote(up_give, up.at[cols(fs), pl.ds(fl, give)], exs.at[0], exr.at[0], inner),
              remote(down_give, down.at[pl.ds(fl, give), cols(fs)], exs.at[1], exr.at[1], inner))

        def hidden_block(u, here=None):
            here = pl.ds(u * unit, unit) if here is None else here
            active = jnp.maximum(dot(tok[here, :], up[:, units], 1, 0), 0.0)
            hid[here, units] = (active * active).astype(BF16)
            dh = dot(cot[here, :], down[units, :], 1, 1)
            dpre[here, units] = (2.0 * active * dh).astype(BF16)

        dxm = [remote(dxm_send.at[u], dxm_recv.at[u], ms.at[0], mr.at[u], mate) for u in range(4)]

        def dx_block(u):
            here = pl.ds(u * unit, unit)

            def tile(j, carry):
                o = cols(j)
                part = dot(dpre[here, units], up[o, units], 1, 1)
                for h in range(2):
                    half = pl.ds(h * hr, hr)
                    dx_own[u, half, o] = part[2 * h * hr : (2 * h + 1) * hr]
                    dxm_send[u, half, o] = part[(2 * h + 1) * hr : (2 * h + 2) * hr].astype(BF16)
                return carry

            lax.fori_loop(0, 4, tile, 0)
            go(dxm[u])

        def dx_sum(u):
            dxm[u].wait_recv()
            return dx_own[u] + dxm_recv[u].astype(F32)

        def z_wait(slot):
            remote(dxz_send.at[0], dxz_recv.at[slot], dzs.at[0], dzr.at[slot], mate).wait_recv()
            return dxz_recv[slot].astype(F32)

        def z_send(i, value, slot, peer):
            dxz_send[i] = value.astype(BF16)
            go(remote(dxz_send.at[i], dxz_recv.at[slot], dzs.at[0], dzr.at[slot], peer))

        def ready(u):
            from_mate(u, 0)
            from_mate(u, 1)
            hidden_block(u)

        if end:
            for cp in ex:
                go(cp)
            for q in Q:
                go(wx[0][q])
                go(wy[0][q])
            for j in Q:
                t_send(0, j, 0, 1, inner)
            for j in Q:
                go(tm[0][j])
            for j in Q:
                w_got(j)
                t_wait(1, j)
                go(tm[1][j])
            passed_on()
            ready(0)
            ready(1)
            dx_block(1)
            t_wait(2, 0)
            go(tm[2][0])
            z_send(0, dx_sum(1), 0, inner)
            for j in (1, 2, 3):
                t_wait(2, j)
                go(tm[2][j])
            ready(2)
            dx_block(2)
            t_wait(3, 0)
            go(tm[3][0])
            z_send(1, dx_sum(2), 1, inner)
        else:
            for q in Q:
                go(wx[0][q])
                go(wy[0][q])
            for j in Q:
                t_send(0, j, 0, 1, outer)
            for j in (0, 1):
                t_send(1, j, 0, 3, inner)
            for j in Q:
                go(tm[0][j])
            for i in range(2):
                ex[i].wait_recv()
                go(wx[0][4 + i])
                go(wy[0][4 + i])

            def from_end(j):
                t_wait(1, j)
                t_send(2, j, 1, 2, inner)
                go(tm[1][j])

            def from_middle(j):
                t_wait(3, j)
                go(tm[3][j])

            def from_far(j):
                t_wait(2, j)
                t_send(4, j, 2, 2, outer)
                go(tm[2][j])

            from_end(0)
            w_got(0)
            from_end(1)
            from_middle(0)
            from_middle(1)
            w_got(1)
            from_end(2)
            from_far(0)
            w_got(2)
            from_end(3)
            for j in (2, 3):
                t_send(1, j, 0, 3, inner)
            from_far(1)
            w_got(3)
            w_got(4)
            w_got(5)
            from_far(2)
            from_far(3)
            for j in (0, 1):
                t_send(3, j, 3, 3, outer)

            def products(here, o):
                return (dot(tok[here, cols(o)], up[cols(o), units], 1, 0),
                        dot(cot[here, cols(o)], down[units, cols(o)], 1, 1))

            spans = [(u * unit, unit) for u in range(3)] + [(3 * unit, rows)]
            for u, (at, n) in enumerate(spans):
                here, there = pl.ds(at, n), pl.ds(4 * unit + at, n)
                from_mate(u, 0)
                if u < 3:
                    from_mate(u, 1)
                for i, o in enumerate((fs, fx_, fy_)):
                    pre, dh = products(here, o)
                    if i:
                        pre, dh = pre + ug_acc[here, units], dh + ug_acc[there, units]
                    ug_acc[here, units] = pre
                    ug_acc[there, units] = dh
            passed_on()
            for at, n in spans:
                here, there = pl.ds(at, n), pl.ds(4 * unit + at, n)
                pre, dh = products(here, fd_)
                active = jnp.maximum(pre + ug_acc[here, units], 0.0)
                hid[here, units] = (active * active).astype(BF16)
                dpre[here, units] = (2.0 * active * (dh + ug_acc[there, units])).astype(BF16)
            for j in (2, 3):
                from_middle(j)
                t_send(3, j, 3, 3, outer)

        cut = 3 * unit + rows
        early = pl.ds(0, cut)
        last = pl.ds(cut, 4 * unit - cut)

        def ug_early(o, carry):
            ug_acc[cols(o), units] = dot(tok[early, cols(o)], dpre[early, units], 0, 0)
            return carry

        def dg_early(o, carry):
            dg_acc[units, cols(o)] = dot(hid[early, units], cot[early, cols(o)], 0, 0)
            return carry

        if end:
            t_wait(3, 1)
            go(tm[3][1])
            dx_block(0)
            from_mate(3, 0)
            hidden_block(3, pl.ds(3 * unit, rows))
            lax.fori_loop(0, 4, ug_early, 0)
            t_wait(3, 2)
            go(tm[3][2])
            lax.fori_loop(0, 4, dg_early, 0)
            from_mate(3, 1)
            spare = pl.ds(fl, rows)
            active = jnp.maximum(dot(tok[last, :], up[:, units], 1, 0), 0.0)
            hid[last, units] = (active * active).astype(BF16)
            dg_acc[spare, units] = active
            t_wait(3, 3)
            go(tm[3][3])
            from_mate(3, 2)
            dh = dot(cot[last, :], down[units, :], 1, 1)
            dpre[last, units] = (2.0 * dg_acc[spare, units] * dh).astype(BF16)
        else:
            ug_early(fd_, 0)
            dg_early(fd_, 0)
            from_mate(3, 1)
            hidden_block(3, last)

        def drain():
            w_bytes = (dl * nown * 2) * 3 // 2 + (0 if end else dl * give * 3)
            sent(size(w_bytes), wxs.at[0])
            sent(size(w_bytes), wys.at[0])
            for flow in range(1 if end else 5):
                sent(tok.at[pl.ds(0, unit)], ts.at[flow])
            sent(tok, tms.at[0])
            if end:
                for cp in ex:
                    cp.wait_send()

        gh = nown // 2

        def buf(bufs, k, q):
            if q < 2:
                return bufs[0].at[k, q, :, pl.ds(0, nown)]
            if q < 4:
                return bufs[1].at[k, q - 2, pl.ds(0, gh)]
            return bufs[q - 2].at[k]

        out_bufs, in_bufs = (ug_send, dg_send, ue_send, de_send), (ug_recv, dg_recv, ue_recv, de_recv)

        detours = ((1, 2), (2, 3))
        few_rows = give // 2

        def g_copy(k, q):
            over_x = k == 1 or (k == 0 and q % 2 == 0)
            src, dst = buf(out_bufs, k, q), buf(in_bufs, k, q)
            if end and (k, q) in detours:
                most = pl.ds(0, gh - few_rows)
                src, dst = src.at[most], dst.at[most]
            return remote(src, dst, gs.at[0], gr.at[k, q], xn if over_x else yn)

        def rest_of(bufs, i):
            k, q = detours[i]
            return bufs[1].at[k, q - 2, pl.ds((fl - give) // 2 - few_rows, few_rows)]

        there = 2 * (z + toward) + c
        leave = [remote(rest_of(out_bufs, i), held.at[i], hs.at[i], hr_.at[i], ((fx_, fy_)[i], there))
                 for i in range(2)]
        arrive = [remote(held.at[i], rest_of(in_bufs, i), vs.at[i], vr.at[i], outer) for i in range(2)]

        g = [[g_copy(k, q) for q in pieces] for k in range(3)]

        def acc_of(o, q):
            if q < 2:
                return ug_acc, pl.ds(pl.multiple_of(o * dl + q * hd, hd), hd), slice(0, nown)
            if q < 4:
                return dg_acc, pl.ds((q - 2) * gh, gh), cols(o)
            if q == 4:
                return ug_acc, cols(o), slice(nown, nf)
            return dg_acc, slice(nown, nf), cols(o)

        def g_put(k, q, value):
            dst = buf(out_bufs, k, q)
            dst[...] = value.astype(BF16)
            go(g[k][q])
            if end and (k, q) in detours:
                go(leave[detours.index((k, q))])

        def terms(o, p):
            split = end or o is fd_
            part = last if split else slice(None)
            few = slice(nown, nf) if p > 1 else slice(0, nown)
            if p % 2 == 0:
                val = dot(tok[part, cols(o)], dpre[part, few], 0, 0)
                if split:
                    val = val + ug_acc[cols(o), few]
                return (val,) if p > 1 else (val[:hd], val[hd:])
            val = dot(hid[part, few], cot[part, cols(o)], 0, 0)
            if split:
                val = val + dg_acc[few, cols(o)]
            return (val,) if p > 1 else (val[:gh], val[gh:])

        def keep(o, q, value):
            ref, a, b = acc_of(o, q)
            ref[a, b] = value

        def begin(p):
            q = 2 * p if p < 2 else p + 2
            for h, v in enumerate(terms(fd_, p)):
                g_put(0, q + h, v)

        def follow(p):
            q = 2 * p if p < 2 else p + 2
            for h, v in enumerate(terms(fx_, p)):
                if (q + h) % 2 == 0:
                    g_put(1, q + h, v)
                else:
                    keep(fx_, q + h, v)
            for h, v in enumerate(terms(fy_, p)):
                if (q + h) % 2:
                    g_put(2, q + h, v)
                else:
                    keep(fy_, q + h, v)

        def own_terms(p):
            q = 2 * p if p < 2 else p + 2
            for h, v in enumerate(terms(fs, p)):
                keep(fs, q + h, v)

        def pass_on(q):
            g[0][q].wait_recv()
            k, o = (1, fx_) if q % 2 else (2, fy_)
            ref, a, b = acc_of(o, q)
            g_put(k, q, ref[a, b] + buf(in_bufs, 0, q)[...].astype(F32))

        back = (remote(ug_back, ug_home, bs.at[0], br.at[0], outer),
                remote(dg_back, dg_home, bs.at[1], br.at[1], outer))

        def summed(q):
            ref, a, b = acc_of(fs, q)
            total = ref[a, b]
            for k in (1, 2):
                g[k][q].wait_recv()
                if end and (k, q) in detours:
                    arrive[detours.index((k, q))].wait_recv()
                total = total + buf(in_bufs, k, q)[...].astype(F32)
            return total

        def finish(q):
            if q < 2:
                ug_out[pl.ds(q * hd, hd), pl.ds(0, nown)] = summed(q) * factor
            else:
                dg_out[pl.ds((q - 2) * gh, gh), :] = summed(q) * factor

        if end:
            begin(0)
            begin(1)
            follow(0)
            follow(1)
            dx_block(3)
            pass_on(0)
            pass_on(1)
            own_terms(0)
            own_terms(1)
            pass_on(2)
            pass_on(3)
            z_send(2, dx_sum(3), 4, beyond)
            drain()
            dx_out[...] = (dx_sum(0) + z_wait(0)).astype(BF16)
            back[0].wait_recv()
            ug_out[:, pl.ds(nown, give)] = ug_home[...].astype(F32) * factor
            back[1].wait_recv()
            dg_out[pl.ds(nown, give), :] = dg_home[...].astype(F32) * factor
        else:
            begin(2)
            begin(3)
            follow(2)
            follow(3)
            dx_block(3)
            begin(0)
            begin(1)
            z_send(0, dx_sum(3), 2, inner)
            pass_on(4)
            pass_on(5)
            follow(0)
            follow(1)
            dx_block(2)
            own_terms(2)
            own_terms(3)
            pass_on(0)
            pass_on(1)
            z_send(1, dx_sum(2) + z_wait(1), 3, inner)
            own_terms(0)
            own_terms(1)
            pass_on(2)
            pass_on(3)
            dx_block(1)
            dx_block(0)
            ug_back[...] = summed(4).astype(BF16)
            dg_back[...] = summed(5).astype(BF16)
            drain()
            go(back[0])
            go(back[1])
            z_send(2, dx_sum(1) + z_wait(3), 0, outer)
            for i in range(2):
                leave[i].wait_recv()
                go(arrive[i])
        for q in Q:
            finish(q)
        if not end:
            near = dx_sum(0) + z_wait(0) + z_wait(2)
            dx_out[...] = (near + z_wait(4)).astype(BF16)
        g_bytes = 12 * hd * nown + (-2 * few_rows * dl if end else 6 * dl * give)
        sent(size(g_bytes), gs.at[0])
        sent(dxm_send, ms.at[0])
        sent(dxz_send, dzs.at[0])
        for cp in leave if end else (*back, *arrive):
            cp.wait_send()

    pl.when(at_end)(lambda: body(True))
    pl.when(jnp.logical_not(at_end))(lambda: body(False))


def put_out(n, *refs):
    copies = [pltpu.make_async_copy(refs[i], refs[n + i], refs[2 * n].at[i]) for i in range(n)]
    for cp in copies:
        cp.start()
    for cp in copies:
        cp.wait()


def line_shards(nfs, ntp, tokens, up_weight, down_weight, cotangent):
    rows, width = tokens.shape
    dl, fl = up_weight.shape
    factor = 1.0 / (rows * ntp * nfs) ** 0.5
    mine = ntp * rows
    give = fl // 4
    most = fl + give
    hd = dl // 2
    dma = pltpu.SemaphoreType.DMA
    any_space = pl.BlockSpec(memory_space=pl.ANY)
    vmem = pl.BlockSpec(memory_space=pltpu.VMEM)
    V = pltpu.VMEM
    results = pl.pallas_call(
        functools.partial(line_kernel, factor, give),
        out_shape=(V((rows, width), BF16), V((dl, fl), F32), V((fl, dl), F32)),
        in_specs=[any_space] * 4,
        out_specs=(vmem, vmem, vmem),
        scratch_shapes=[
            V((mine, width), BF16), V((mine, width), BF16),
            V((width, most), BF16), V((most, width), BF16),
            V((dl, give), BF16), V((give, dl), BF16),
            V((mine, most), BF16), V((mine, most), BF16),
            V((width, most), F32), V((most, width), F32),
            V((3, 2, hd, fl), BF16), V((3, 2, hd, fl), BF16),
            V((3, 2, fl // 2, dl), BF16), V((3, 2, fl // 2, dl), BF16),
            V((dl, give), BF16), V((give, dl), BF16), V((dl, give), BF16), V((give, dl), BF16),
            V((3, dl, give), BF16), V((3, dl, give), BF16), V((3, give, dl), BF16), V((3, give, dl), BF16),
            V((4, rows, width), F32), V((4, rows, width), BF16), V((4, rows, width), BF16),
            V((3, rows, width), BF16), V((5, rows, width), BF16),
            dma((1,)), dma((2,)), dma((2,)), dma((1,)), dma((7,)), dma((1,)), dma((7,)),
            dma((5,)), dma((4, 4)), dma((1,)), dma((9,)),
            dma((1,)), dma((4,)), dma((1,)), dma((5,)), dma((1,)), dma((3, 6)), dma((2,)), dma((2,)),
            V((2, give // 2, dl), BF16), dma((2,)), dma((2,)), dma((2,)), dma((2,)),
        ],
        compiler_params=pltpu.CompilerParams(
            collective_id=0, has_side_effects=True, vmem_limit_bytes=60_000_000
        ),
    )(tokens, up_weight, down_weight, cotangent)
    return pl.pallas_call(
        functools.partial(put_out, len(results)),
        out_shape=tuple(jax.ShapeDtypeStruct(r.shape, r.dtype) for r in results),
        in_specs=[vmem] * len(results),
        out_specs=(any_space,) * len(results),
        scratch_shapes=[dma((3,))],
        compiler_params=pltpu.CompilerParams(vmem_limit_bytes=8_000_000),
    )(*results)


def solution(mesh):
    placed = (P(("fs", "tp"), None), P("fs", "tp"), P("tp", "fs"), P(("fs", "tp"), None))
    fs, tp = mesh.shape["fs"], mesh.shape["tp"]
    body = line_shards if (fs, tp) == (4, 8) else shards
    return jax.shard_map(
        functools.partial(body, mesh.shape["fs"], mesh.shape["tp"]),
        mesh=mesh,
        in_specs=placed,
        out_specs=(P(("fs", "tp"), None), P("fs", "tp"), P("tp", "fs")),
        check_vma=False,
    )
```
